256 devices in a mesh: grp: 2 (over y), sp: 16 (over z), tp: 8 (over x, core).
Axes of the slice: x: 4, y: 2, z: 16, core: 2. Of those that a mesh axis runs over, the one named last changes fastest.
The devices are a block of a 4x16x16 slice.
Arguments:
- queries: bfloat16 [24576, 1024], P(('grp', 'sp'), 'tp'), parts along dimension 0, may hold values from -8 to 8
- keys: bfloat16 [24576, 256], P(('grp', 'sp')), parts along dimension 0, may hold values from -8 to 8
- values: bfloat16 [24576, 256], P(('grp', 'sp')), parts along dimension 0, may hold values from -6 to 6
- query_gain: float32 [128], replicated, may hold values from 0.2 to 6
- key_gain: float32 [128], replicated, may hold values from 0.2 to 6
- residual: bfloat16 [24576, 2048], P(('grp', 'sp', 'tp')), parts along dimension 0, may hold values from -6 to 6
- out_weight: bfloat16 [1024, 2048], P('tp'), may hold values from -0.1875 to 0.1875
- mix_gain: float32 [2048], replicated, may hold values from 0.1 to 1.9
- ffn_gain: float32 [2048], replicated, may hold values from 0.1 to 1.9
- gate_in: bfloat16 [2048, 5632], P('sp', 'tp'), may hold values from -0.125 to 0.125
- value_in: bfloat16 [2048, 5632], P('sp', 'tp'), may hold values from -0.125 to 0.125
- conv_gate: float32 [3, 5632], P(None, 'tp'), may hold values from -3 to 3
- conv_value: float32 [3, 5632], P(None, 'tp'), may hold values from -3 to 3
- down_t: bfloat16 [2048, 5632], P('sp', 'tp'), may hold values from -0.078125 to 0.078125
Outputs:
- layer_out: bfloat16 [24576, 2048], P(('grp', 'sp', 'tp')), parts along dimension 0
The draws below stay inside these ranges and needn't reach their ends.
There are 2 independent parts, one for each index of `grp`. The reference program is written for one: setup_inputs(seed, part) draws one part's arguments, and reference() takes and returns one part's arrays. A program takes and returns all parts, laid end to end along the dimension named above; an argument that names none is the same for every part. Nothing has to cross between parts.
All inputs are finite; a program needn't handle non-finite values.
Results may differ from the reference program's by a relative error of at most 0.02.
The reference program's roundings to bfloat16 on the way count: a program that leaves them out, or rounds other values in their place, can miss the bound.
Values may be sent and summed in bfloat16 or wider, within the bound.
No kernel may reach another device: no remote copies, remote signals or barrier semaphores. Data moves between devices by JAX's collectives and lax.ppermute only.
A program may use at most 128 MiB of HBM per device.

```python
import math
import jax
import jax.numpy as jnp
from jax import lax

D = 2048
HEADS = 8
KVH = 2
HD = 128
FF = 5632
GRID_W = 64
SEQ = 12288
N_TP = 8


def shared_keys(key):
    base = jax.random.normal(jax.random.fold_in(key, 11), (SEQ, KVH * HD), jnp.float32)
    return jnp.clip(base, -8.0, 8.0)


def draw_keys(key, part):
    base = shared_keys(key)
    return base.astype(jnp.bfloat16)


def draw_queries(key, part):
    drawn = jax.random.normal(jax.random.fold_in(key, 13), (SEQ, HEADS * HD), jnp.float32)
    return jnp.clip(drawn, -8.0, 8.0).astype(jnp.bfloat16)


def gain_draw(key):
    return jnp.clip(1.0 + 0.18 * jax.random.normal(key, (HD,), jnp.float32), 0.2, 2.0)


def draw_query_gain(key, part):
    return gain_draw(jax.random.fold_in(key, 21))


def draw_key_gain(key, part):
    return gain_draw(jax.random.fold_in(key, 22))


def shard_levels(own_key, extent, shards, low, top_value):
    factor_of, own = 1.0, jax.random.fold_in(own_key, 6)
    for position, blocks in shards:
        heights = jnp.exp(jax.random.uniform(jax.random.fold_in(own, position), (blocks,), jnp.float32, low / len(shards), top_value / len(shards)))
        factor_of = factor_of * jnp.repeat(heights, extent[position] // blocks).reshape([-1 if axis == position else 1 for axis in range(len(extent))])
    return factor_of


def centred(key, shape, scale, limit, cuts=(), held_as=jnp.bfloat16):
    result = jax.random.normal(key, shape, jnp.float32) * scale
    if len(cuts) > 0:
        result = shard_levels(key, shape, cuts, -0.22, 0.18) * result
    return jnp.clip(result, min=-limit, max=limit).astype(held_as)


def setup_inputs(seed: int = 0, part: int = 0) -> dict:
    arg_keys = jax.random.split(jax.random.key(seed), 15)
    own_keys = jax.random.split(jax.random.fold_in(arg_keys[14], part), 15)
    queries = draw_queries(jax.random.fold_in(jax.random.fold_in(arg_keys[14], part), 71), part)
    keys = draw_keys(jax.random.fold_in(jax.random.fold_in(arg_keys[14], part), 71), part)
    values = centred(own_keys[2], (SEQ, KVH * HD), 1.0, 6.0, ((0, 16),))
    query_gain = draw_query_gain(jax.random.fold_in(arg_keys[14], 71), part)
    key_gain = draw_key_gain(jax.random.fold_in(arg_keys[14], 71), part)
    residual = centred(own_keys[5], (SEQ, D), 1.0, 6.0, ((0, 128),))
    out_weight = centred(arg_keys[6], (HEADS * HD, D), (HEADS * HD) ** -0.5, 0.1875, ((0, 8),))
    mix_gain = jnp.clip(1.0 + 0.18 * jax.random.normal(arg_keys[7], (D,), jnp.float32), 0.1, 1.9)
    ffn_gain = jnp.clip(1.0 + 0.18 * jax.random.normal(arg_keys[8], (D,), jnp.float32), 0.1, 1.9)
    gate_in = centred(arg_keys[9], (D, FF), D ** -0.5, 0.125, ((0, 16), (1, 8)))
    value_in = centred(arg_keys[10], (D, FF), D ** -0.5, 0.125, ((0, 16), (1, 8)))
    conv_gate = centred(arg_keys[11], (3, FF), 0.577, 3.0, ((1, 8),), jnp.float32)
    conv_value = centred(arg_keys[12], (3, FF), 0.577, 3.0, ((1, 8),), jnp.float32)
    down_t = centred(arg_keys[13], (D, FF), FF ** -0.5, 0.078125, ((0, 16), (1, 8)))
    return dict(queries=queries, keys=keys, values=values, query_gain=query_gain, key_gain=key_gain, residual=residual, out_weight=out_weight, mix_gain=mix_gain, ffn_gain=ffn_gain, gate_in=gate_in, value_in=value_in, conv_gate=conv_gate, conv_value=conv_value, down_t=down_t)


EPSILON = 1e-06
THETA = 10000.0

def rotary_tables():
    quarter = HD // 4
    inverse = THETA ** (-(2.0 * jnp.arange(quarter, dtype=jnp.float32)) / (HD // 2))
    positions = jnp.arange(SEQ, dtype=jnp.int32)
    grid_row = (positions // GRID_W - SEQ // GRID_W // 2).astype(jnp.float32)
    grid_col = (positions % GRID_W - GRID_W // 2).astype(jnp.float32)
    row_angle = grid_row[:, None] * inverse[None, :]
    col_angle = grid_col[:, None] * inverse[None, :]
    angle = jnp.concatenate([row_angle, row_angle, col_angle, col_angle], axis=-1)
    return (jnp.cos(angle), jnp.sin(angle))

def rotate_quarters(vector):
    first, second, third, fourth = jnp.split(vector, 4, axis=-1)
    return jnp.concatenate([-second, first, -fourth, third], axis=-1)

def prepare_heads(raw, gain, cos_table, sin_table, factor):
    floats = raw.astype(jnp.float32)
    normed = floats * lax.rsqrt(lax.optimization_barrier(jnp.mean(floats * floats, axis=-1, keepdims=True)) + EPSILON) * gain
    turned = normed * cos_table + rotate_quarters(normed) * sin_table
    return (turned * factor).astype(jnp.bfloat16)

def rms_rows(stream, gain):
    floats = stream.astype(jnp.float32)
    return floats * lax.rsqrt(lax.optimization_barrier(jnp.mean(floats * floats, axis=-1, keepdims=True)) + EPSILON) * gain

def reference(queries, keys, values, query_gain, key_gain, residual, out_weight, mix_gain, ffn_gain, gate_in, value_in, conv_gate, conv_value, down_t):
    group = HEADS // KVH
    cos_table, sin_table = rotary_tables()
    query_rot = prepare_heads(queries.reshape(SEQ, HEADS, HD), query_gain, cos_table[:, None, :], sin_table[:, None, :], HD ** (-0.5))
    key_rot = prepare_heads(keys.reshape(SEQ, KVH, HD), key_gain, cos_table[:, None, :], sin_table[:, None, :], 1.0)
    key_float = key_rot.astype(jnp.float32)
    value_float = values.reshape(SEQ, KVH, HD).astype(jnp.float32)
    block = math.gcd(SEQ, 512)
    query_blocks = query_rot.reshape(SEQ // block, block, KVH, group, HD)

    def attend_block(query_block):
        scores = jnp.einsum('qhgd,khd->hgqk', query_block.astype(jnp.float32), key_float)
        highest = lax.optimization_barrier(jnp.max(scores, axis=-1, keepdims=True))
        weights = jnp.exp(scores - highest)
        denom = lax.optimization_barrier(jnp.sum(weights, axis=-1, keepdims=True))
        rounded = weights.astype(jnp.bfloat16).astype(jnp.float32)
        summed = jnp.einsum('hgqk,khd->qhgd', rounded, value_float)
        denom_t = jnp.transpose(denom, (2, 0, 1, 3))
        return (summed / denom_t).astype(jnp.bfloat16)
    attended = lax.map(attend_block, query_blocks).reshape(SEQ, HEADS * HD)
    head_cols = HEADS * HD // N_TP
    mix = jnp.zeros((SEQ, D), jnp.float32)
    for group_index in range(N_TP):
        lower = group_index * head_cols
        partial_mix = jnp.dot(attended[:, lower:lower + head_cols], out_weight[lower:lower + head_cols], preferred_element_type=jnp.float32).astype(jnp.bfloat16)
        partial_mix = lax.optimization_barrier(partial_mix)
        mix = mix + partial_mix.astype(jnp.float32)
    mix_normed = rms_rows(mix, mix_gain)
    stream = (residual.astype(jnp.float32) + mix_normed).astype(jnp.bfloat16)
    normed = rms_rows(stream, ffn_gain).astype(jnp.bfloat16)
    gate_up = jnp.dot(normed, gate_in, preferred_element_type=jnp.float32).astype(jnp.bfloat16)
    value_up = jnp.dot(normed, value_in, preferred_element_type=jnp.float32).astype(jnp.bfloat16)

    def depthwise(upward, taps):
        padded = jnp.pad(upward.astype(jnp.float32), ((1, 1), (0, 0)))
        return taps[0] * padded[:-2] + taps[1] * padded[1:-1] + taps[2] * padded[2:]
    gate_mixed = depthwise(gate_up, conv_gate)
    value_mixed = depthwise(value_up, conv_value)
    hidden = (jax.nn.gelu(gate_mixed, approximate=True) * value_mixed).astype(jnp.bfloat16)
    unit_cols = FF // N_TP
    ffn_out = jnp.zeros((SEQ, D), jnp.float32)
    for group_index in range(N_TP):
        lower = group_index * unit_cols
        partial_down = jnp.dot(hidden[:, lower:lower + unit_cols], down_t[:, lower:lower + unit_cols].T, preferred_element_type=jnp.float32).astype(jnp.bfloat16)
        partial_down = lax.optimization_barrier(partial_down)
        ffn_out = ffn_out + partial_down.astype(jnp.float32)
    return (stream.astype(jnp.float32) + ffn_out).astype(jnp.bfloat16)
```

```python
import functools
import numpy as np
import jax
import jax.numpy as jnp
from jax import lax
from jax.experimental import pallas as pl
from jax.experimental.pallas import tpu as pltpu
from jax.sharding import PartitionSpec as P

HEADS = 8
KVH = 2
GRID_W = 64
EPSILON = 1e-06
THETA = 10000.0
F32 = jnp.float32
BF16 = jnp.bfloat16
NT = (((1,), (1,)), ((), ()))


def rotary_parts(seq_total, head_dim):
    quarter = head_dim // 4
    inverse = THETA ** (-(2.0 * np.arange(quarter, dtype=np.float32)) / np.float32(head_dim // 2))
    inverse = inverse.astype(np.float32)
    rows = seq_total // GRID_W
    row_angle = (np.arange(rows) - rows // 2).astype(np.float32)[:, None] * inverse
    col_angle = (np.arange(GRID_W) - GRID_W // 2).astype(np.float32)[:, None] * inverse

    def lanes(angle, first):
        zero = np.zeros_like(angle)
        cos, sin = np.cos(angle.astype(np.float64)), np.sin(angle.astype(np.float64))
        cos, sin = [cos, cos], [-sin, sin]
        pad = [zero, zero]
        parts = (cos + pad if first else pad + cos) + (sin + pad if first else pad + sin)
        return np.concatenate(parts, axis=-1).astype(np.float32)

    return lanes(row_angle, True), lanes(col_angle, False)


def turned(raw, gain, cos, sin, factor):
    x = raw.astype(F32)
    head_dim = x.shape[-1]
    quarter = head_dim // 4
    normed = x * lax.rsqrt(jnp.mean(x * x, axis=-1, keepdims=True) + EPSILON) * gain
    lane = lax.broadcasted_iota(jnp.int32, x.shape, 1)
    other = jnp.where(
        (lane & quarter) == 0,
        pltpu.roll(normed, head_dim - quarter, 1),
        pltpu.roll(normed, quarter, 1),
    )
    return ((normed * cos + other * sin) * factor).astype(BF16)


def key_kernel(at_ref, k_ref, v_ref, down_ref, gain_ref, row_ref, col_ref, out_ref):
    part, hd = k_ref.shape
    count = part // GRID_W
    for i in range(count):
        rows = pl.ds(i * GRID_W, GRID_W)
        table = row_ref[0, pl.ds(at_ref[0] * count + i, 1), :] + col_ref[...]
        out_ref[rows, :] = turned(k_ref[rows, :], gain_ref[...], table[:, :hd], table[:, hd:], 1.0)
    out_ref[pl.ds(part, part), :] = v_ref[...]
    out_ref[pl.ds(2 * part, down_ref.shape[0]), :] = down_ref[...]


def query_kernel(toks, *refs):
    raws, (gain_ref, row_ref, col_ref, out_ref) = refs[:-4], refs[-4:]
    hd = raws[0].shape[1]
    blocks = raws[0].shape[0] // GRID_W
    for i in range(blocks):
        table = row_ref[0, pl.ds(i, 1), :] + col_ref[...]
        for k, raw in enumerate(raws):
            q = turned(
                raw[pl.ds(i * GRID_W, GRID_W), :], gain_ref[...], table[:, :hd], table[:, hd:], hd ** (-0.5)
            )
            at = 0
            while at < GRID_W:
                owner, inside = divmod(i * GRID_W + at, toks)
                size = min(toks - inside, GRID_W - at)
                out_ref[owner, pl.ds(k * toks + inside, size), :] = q[at : at + size]
                at += size


def as_row(col, eye):
    return jnp.sum(jnp.where(eye, col, 0.0), axis=0, keepdims=True)


def as_col(row, eye):
    return jnp.sum(jnp.where(eye, row, 0.0), axis=1, keepdims=True)


def square_eye(n):
    return lax.broadcasted_iota(jnp.int32, (n, n), 0) == lax.broadcasted_iota(jnp.int32, (n, n), 1)


def attend_kernel(shards, first, last, *refs):
    q_ref, refs = refs[0], refs[1:]
    kv, refs = refs[:shards], refs[shards:]
    if not first:
        carry_ref, refs = refs[0], refs[1:]
    out_ref = refs[0]
    rows, hd = q_ref.shape[1:]
    part = kv[0].shape[0] // 2
    half = hd // 2
    keys = jnp.concatenate([r[pl.ds(0, part), :] for r in kv], axis=0)
    vals = jnp.concatenate([r[pl.ds(part, part), :] for r in kv], axis=0)
    s = lax.dot_general(q_ref[0], keys, NT, preferred_element_type=F32)
    m = jnp.max(s, axis=1, keepdims=True)
    if not first:
        m_old = carry_ref[0, pl.ds(rows, rows), 0:1]
        den_old = carry_ref[0, pl.ds(rows, rows), half : half + 1]
        m = jnp.maximum(m, m_old)
    p = jnp.exp(s - m)
    den = jnp.sum(p, axis=1, keepdims=True)
    acc = jnp.dot(p.astype(BF16), vals, preferred_element_type=F32)
    if not first:
        fade = jnp.exp(m_old - m)
        den = den + den_old * fade
        acc = acc + carry_ref[0, pl.ds(0, rows), :] * fade
    if not last:
        out_ref[0, pl.ds(0, rows), :] = acc
        lane = lax.broadcasted_iota(jnp.int32, (rows, hd), 1)
        out_ref[0, pl.ds(rows, rows), :] = jnp.where(lane < half, m, den)
        return
    out_ref[0, pl.ds(0, rows), :] = (acc / den).astype(BF16)
    eye = square_eye(hd)
    lse = m + jnp.log(den)
    stats = [as_row(lse[b * hd : (b + 1) * hd], eye) for b in range(rows // hd)]
    tail = out_ref.shape[1] - rows
    left = jnp.concatenate(stats + [jnp.zeros((8 - len(stats), hd), F32)], axis=0)
    high = left.astype(BF16).astype(F32)
    left = left - high
    mid = left.astype(BF16).astype(F32)
    out_ref[0, pl.ds(rows, tail), :] = jnp.concatenate(
        [high, mid, left - mid, jnp.zeros((tail - 24, hd), F32)], axis=0
    ).astype(BF16)


def normalised(x, gain):
    return x * lax.rsqrt(jnp.mean(x * x, axis=-1, keepdims=True) + EPSILON) * gain


def mix_kernel(group, pieces, at_ref, in_ref, res_ref, mg_ref, fg_ref, *refs):
    parts, refs = refs[:pieces], refs[pieces:]
    stream_ref, normed_ref, head_ref, att_ref, w_ref, sem = refs
    copies = []
    for i, part in enumerate(parts):
        size = part.shape[0]
        start = pl.multiple_of(at_ref[i], size)
        copies.append(pltpu.make_async_copy(part, w_ref.at[pl.ds(start, size), :], sem.at[i]))
    for c in copies:
        c.start()
    sources = in_ref.shape[0]
    hd = in_ref.shape[2]
    toks = res_ref.shape[0]
    rows = group * toks
    splits = sources // KVH
    eye = square_eye(hd)
    for kv in range(KVH):
        lse = []
        for j in range(splits):
            t = in_ref[kv * splits + j, pl.ds(rows, in_ref.shape[1] - rows), :].astype(F32)
            t = t[0:8] + t[8:16] + t[16:24]
            lse.append(t)
        cols = []
        for j in range(splits):
            blocks = [as_col(lse[j][b : b + 1], eye) for b in range(rows // hd)]
            cols.append(jnp.concatenate(blocks, axis=0))
        for h in range(group):
            mine = [cols[j][(h ^ j) * toks : (h ^ j) * toks + toks] for j in range(splits)]
            top = functools.reduce(jnp.maximum, mine)
            w = [jnp.exp(x - top) for x in mine]
            total = functools.reduce(jnp.add, w)
            acc = None
            for j in range(splits):
                o = in_ref[kv * splits + j, pl.ds((h ^ j) * toks, toks), :].astype(F32)
                term = (w[j] / total) * o
                acc = term if acc is None else acc + term
            c = (kv * group + h) * hd
            att_ref[:, c : c + hd] = acc.astype(BF16)
    for c in copies:
        c.wait()
    mix = jnp.dot(att_ref[...], w_ref[...], preferred_element_type=F32)
    stream = (res_ref[...].astype(F32) + normalised(mix, mg_ref[...])).astype(BF16)
    stream_ref[...] = stream
    normed_ref[...] = normalised(stream.astype(F32), fg_ref[...]).astype(BF16)


def gelu(v):
    return 0.5 * v * (1.0 + jnp.tanh(0.7978845608028654 * (v + 0.044715 * v * v * v)))


def ffn_kernel(pieces, shards, at_ref, halo_ref, taps_ref, gv_ref, *refs):
    toks_in, refs = refs[:pieces], refs[pieces:]
    downs, refs = refs[:shards], refs[shards:]
    keep_ref, send_ref, x_ref, w_ref, d_ref, h_ref, p_ref, sem_x, sem_w, sem_d, sem_o = refs
    main = x_ref.shape[0] - halo_ref.shape[0]
    units = h_ref.shape[1]
    lanes = gv_ref.shape[2]
    skip = downs[0].shape[0] - units

    def token_copy(i):
        size = toks_in[i].shape[0]
        start = pl.multiple_of(at_ref[i], 16)
        return pltpu.make_async_copy(toks_in[i], x_ref.at[pl.ds(start, size), :], sem_x.at[i])

    def weight_copy(i):
        return pltpu.make_async_copy(gv_ref.at[i], w_ref.at[:, pl.ds(i * lanes, lanes)], sem_w.at[i])

    def down_copy(i):
        start = pl.multiple_of(at_ref[pieces + i], lanes)
        return pltpu.make_async_copy(
            downs[i].at[pl.ds(skip, units), :], d_ref.at[:, pl.ds(start, lanes)], sem_d.at[i]
        )

    for i in range(pieces):
        token_copy(i).start()
    for i in range(shards):
        weight_copy(i).start()
    for i in range(shards):
        down_copy(i).start()
    x_ref[pl.ds(main, halo_ref.shape[0]), :] = halo_ref[...]
    for i in range(pieces):
        token_copy(i).wait()
    for i in range(shards):
        weight_copy(i).wait()

    def up_block(start, size):
        w = jnp.concatenate(
            [w_ref[pl.ds(start, size), :], w_ref[pl.ds(units + start, size), :]], axis=0
        )
        up = lax.dot_general(x_ref[...], w, NT, preferred_element_type=F32)
        up = up.astype(BF16).astype(F32)
        now = up[:main]
        row = lax.broadcasted_iota(jnp.int32, now.shape, 0)
        before = jnp.where(row == 0, up[main : main + 1], pltpu.roll(now, 1, 0))
        after = jnp.where(row == main - 1, up[main + 1 : main + 2], pltpu.roll(now, main - 1, 0))
        return now, before, after

    block = 128
    full = units // block
    for b in range(full + (1 if units % block else 0)):
        size = min(block, units - b * block)
        now, before, after = up_block(b * block, size)
        taps = taps_ref[b]
        mixed = taps[0:1, : 2 * size] * before + taps[1:2, : 2 * size] * now + taps[2:3, : 2 * size] * after
        h_ref[:, b * block : b * block + size] = (gelu(mixed[:, :size]) * mixed[:, size:]).astype(BF16)

    for i in range(shards):
        down_copy(i).wait()
    for n in range(d_ref.shape[1] // 256):
        cols = slice(n * 256, n * 256 + 256)
        p_ref[:, cols] = jnp.dot(h_ref[...], d_ref[:, cols], preferred_element_type=F32).astype(BF16)
    count, own = keep_ref.shape[0], keep_ref.shape[1]
    outs = []
    for k in range(count):
        for o, ref in enumerate((keep_ref, send_ref)):
            start = pl.multiple_of(at_ref[pieces + shards + 2 * k + o], 16)
            outs.append(
                pltpu.make_async_copy(p_ref.at[pl.ds(start, own), :], ref.at[k], sem_o.at[2 * k + o])
            )
    for c in outs:
        c.start()
    for c in outs:
        c.wait()


def vmem(limit=56 << 20):
    return pltpu.CompilerParams(vmem_limit_bytes=limit)


def body(
    queries,
    keys,
    values,
    query_gain,
    key_gain,
    residual,
    out_weight,
    mix_gain,
    ffn_gain,
    gate_in,
    value_in,
    conv_gate,
    conv_value,
    down_t,
):
    tok = queries.shape[0]
    hd = query_gain.shape[0]
    n_sp, n_tp = lax.axis_size("sp"), lax.axis_size("tp")
    n_x = n_tp // 2
    group = HEADS // KVH
    splits = n_tp // KVH
    part = tok // splits
    own = tok // n_tp
    model = residual.shape[1]
    units = gate_in.shape[1]
    tp, sp = lax.axis_index("tp"), lax.axis_index("sp")
    kv_head, piece = tp // splits, tp % splits
    x, core = tp // 2, tp % 2

    def send(array, change):
        return lax.ppermute(array, "tp", [(i, change(i)) for i in range(n_tp)])

    def other_core(array):
        return send(array, lambda i: i ^ 1)

    def up_x(array):
        return send(array, lambda i: (i + 2) % n_tp)

    def down_x(array):
        return send(array, lambda i: (i - 2) % n_tp)

    def far_x(array):
        return send(array, lambda i: (i + n_x) % n_tp)

    def gathered(mine):
        size = mine.shape[0]
        half = size // 2
        a = up_x(mine)
        b = down_x(mine)
        near = other_core(mine)
        c = up_x(a[:half])
        d = down_x(b[half:])
        low, high = ((x + n_x - 1) % n_x) * 2, ((x + 1) % n_x) * 2
        far = (tp + n_x) % n_tp
        found = [(mine, tp * size), (near, (tp ^ 1) * size)]
        for array, base in ((a, low), (b, high)):
            found.append((array, (base + core) * size))
            found.append((other_core(array), (base + 1 - core) * size))
        for array, shift in ((c, 0), (d, half)):
            found.append((array, far * size + shift))
            found.append((other_core(array), (far ^ 1) * size + shift))
        return [f[0] for f in found], [f[1] for f in found]

    row_np, col_np = rotary_parts(tok * n_sp, hd)
    row_np = row_np.reshape(n_sp, tok // GRID_W, 2 * hd)
    rows_all, cols_all = jnp.asarray(row_np), jnp.asarray(col_np)
    at = jnp.stack([piece, kv_head, sp]).astype(jnp.int32)
    packed_rows = 2 * part + units
    packed = pl.pallas_call(
        key_kernel,
        out_shape=jax.ShapeDtypeStruct((packed_rows, hd), BF16),
        grid_spec=pltpu.PrefetchScalarGridSpec(
            num_scalar_prefetch=1,
            grid=(1,),
            in_specs=[
                pl.BlockSpec((part, hd), lambda i, a: (a[0], a[1])),
                pl.BlockSpec((part, hd), lambda i, a: (a[0], a[1])),
                pl.BlockSpec((units, hd), lambda i, a: (0, 0)),
                pl.BlockSpec((1, hd), lambda i, a: (0, 0)),
                pl.BlockSpec((1,) + row_np.shape[1:], lambda i, a: (a[2], 0, 0)),
                pl.BlockSpec(col_np.shape, lambda i, a: (0, 0)),
            ],
            out_specs=pl.BlockSpec((packed_rows, hd), lambda i, a: (0, 0)),
        ),
        name="key_prep",
    )(at, keys, values, down_t.T, key_gain[None], rows_all, cols_all)
    right = [(i, (i + 1) % n_sp) for i in range(n_sp)]
    left = [(i, (i - 1) % n_sp) for i in range(n_sp)]
    shards, sources = [packed], [sp]
    a = b = packed
    for s in range(1, n_sp // 2 + 1):
        a = lax.ppermute(a, "sp", right)
        shards.append(a)
        sources.append((sp + n_sp - s) % n_sp)
        if len(shards) < n_sp:
            b = lax.ppermute(b, "sp", left)
            shards.append(b)
            sources.append((sp + s) % n_sp)

    gate_rows = lax.all_gather(jnp.concatenate([gate_in.T, value_in.T], axis=0), "sp", axis=0, tiled=False)

    raw = [queries, other_core(queries)]
    pair = send(queries, lambda i: i ^ 2)
    raw += [pair, other_core(pair)]
    rows = group * own
    turned_q = pl.pallas_call(
        lambda at_ref, *refs: query_kernel(own, *refs),
        out_shape=jax.ShapeDtypeStruct((n_tp, rows, hd), BF16),
        grid_spec=pltpu.PrefetchScalarGridSpec(
            num_scalar_prefetch=1,
            grid=(1,),
            in_specs=[pl.BlockSpec((tok, hd), lambda i, a: (0, 0))] * group
            + [
                pl.BlockSpec((1, hd), lambda i, a: (0, 0)),
                pl.BlockSpec((1,) + row_np.shape[1:], lambda i, a: (a[2], 0, 0)),
                pl.BlockSpec(col_np.shape, lambda i, a: (0, 0)),
            ],
            out_specs=pl.BlockSpec((n_tp, rows, hd), lambda i, a: (0, 0, 0)),
        ),
        name="query_prep",
    )(at, *raw, query_gain[None], rows_all, cols_all)

    out_pieces, out_at = gathered(out_weight)

    tail = 32
    step = 4
    calls = n_sp // step
    carry = None
    for c in range(calls):
        last = c == calls - 1
        here = shards[c * step : (c + 1) * step]
        shape = (n_tp, rows + tail, hd) if last else (n_tp, 2 * rows, hd)
        operands = [turned_q] + here + ([] if carry is None else [carry])
        specs = [pl.BlockSpec((1, rows, hd), lambda i: (i, 0, 0))]
        specs += [pl.BlockSpec((2 * part, hd), lambda i: (0, 0))] * step
        if carry is not None:
            specs.append(pl.BlockSpec((1, 2 * rows, hd), lambda i: (i, 0, 0)))
        carry = pl.pallas_call(
            functools.partial(attend_kernel, step, c == 0, last),
            out_shape=jax.ShapeDtypeStruct(shape, BF16 if last else F32),
            grid=(n_tp,),
            in_specs=specs,
            out_specs=pl.BlockSpec((1,) + shape[1:], lambda i: (i, 0, 0)),
            compiler_params=vmem(),
            cost_estimate=pl.CostEstimate(
                flops=8 * group * tok * part * step * hd,
                bytes_accessed=8 << 20,
                transcendentals=group * tok * part * step,
            ),
            name="attend%d" % c,
        )(*operands)
    seen = lax.all_to_all(carry, "tp", split_axis=0, concat_axis=0, tiled=True)
    anywhere = pl.BlockSpec(memory_space=pl.ANY)
    whole = pl.BlockSpec(memory_space=pltpu.VMEM)
    stream, normed = pl.pallas_call(
        functools.partial(mix_kernel, group, len(out_pieces)),
        out_shape=[jax.ShapeDtypeStruct((own, model), BF16)] * 2,
        in_specs=[pl.BlockSpec(memory_space=pltpu.SMEM)] + [whole] * 4 + [anywhere] * len(out_pieces),
        scratch_shapes=[
            pltpu.VMEM((rows, hd), F32),
            pltpu.VMEM((own, HEADS * hd), BF16),
            pltpu.VMEM((HEADS * hd, model), BF16),
            pltpu.SemaphoreType.DMA((len(out_pieces),)),
        ],
        compiler_params=vmem(),
        cost_estimate=pl.CostEstimate(
            flops=2 * own * HEADS * hd * model, bytes_accessed=6 << 20, transcendentals=0
        ),
        name="mix",
    )(jnp.stack(out_at).astype(jnp.int32), seen, residual, mix_gain[None], ffn_gain[None], *out_pieces)

    token_pieces, token_at = gathered(normed)
    first = last_row = None
    for p, r in zip(token_pieces, token_at):
        f = jnp.where(r == 0, p[:1], 0)
        e = jnp.where(r + p.shape[0] == tok, p[-1:], 0)
        first = f if first is None else first + f
        last_row = e if last_row is None else last_row + e
    before = lax.ppermute(last_row, "sp", [(i, i + 1) for i in range(n_sp - 1)])
    after = lax.ppermute(first, "sp", [(i + 1, i) for i in range(n_sp - 1)])
    halo = jnp.concatenate([before, after, jnp.zeros((14, model), BF16)], axis=0)
    blocks = -(-units // 128)
    taps = []
    for t in range(blocks):
        lo, hi = t * 128, min(units, t * 128 + 128)
        both = jnp.concatenate([conv_gate[:, lo:hi], conv_value[:, lo:hi]], axis=1)
        taps.append(jnp.pad(both, ((0, 5), (0, 256 - both.shape[1]))))
    taps = jnp.stack(taps)
    slots = []
    for k in range(n_x):
        to = ((x + k) % n_x) * 2
        slots += [(to + core) * own, (to + 1 - core) * own]
    where = jnp.stack(token_at + [s * hd for s in sources] + slots).astype(jnp.int32)
    keep, away = pl.pallas_call(
        functools.partial(ffn_kernel, len(token_pieces), n_sp),
        out_shape=[jax.ShapeDtypeStruct((n_x, own, model), BF16)] * 2,
        in_specs=[pl.BlockSpec(memory_space=pltpu.SMEM), whole, whole]
        + [anywhere] * (1 + len(token_pieces) + n_sp),
        out_specs=[anywhere, anywhere],
        scratch_shapes=[
            pltpu.VMEM((tok + 16, model), BF16),
            pltpu.VMEM((2 * units, model), BF16),
            pltpu.VMEM((units, model), BF16),
            pltpu.VMEM((tok, units), BF16),
            pltpu.VMEM((tok, model), BF16),
            pltpu.SemaphoreType.DMA((len(token_pieces),)),
            pltpu.SemaphoreType.DMA((n_sp,)),
            pltpu.SemaphoreType.DMA((n_sp,)),
            pltpu.SemaphoreType.DMA((2 * n_x,)),
        ],
        compiler_params=vmem(),
        cost_estimate=pl.CostEstimate(
            flops=6 * tok * units * model, bytes_accessed=16 << 20, transcendentals=tok * units
        ),
        name="ffn",
    )(where, halo, taps, gate_rows, *token_pieces, *shards)
    near = other_core(away)
    total = [keep[k].astype(F32) + near[k].astype(F32) for k in range(n_x)]
    one = up_x(total[1].astype(BF16))
    two = far_x(total[2].astype(BF16))
    three = down_x(total[3].astype(BF16))
    out = total[0] + one.astype(F32) + two.astype(F32) + three.astype(F32)
    return (stream.astype(F32) + out).astype(BF16)


def solution(mesh):
    return jax.shard_map(
        body,
        mesh=mesh,
        in_specs=(
            P(("grp", "sp"), "tp"),
            P(("grp", "sp"), None),
            P(("grp", "sp"), None),
            P(),
            P(),
            P(("grp", "sp", "tp"), None),
            P("tp", None),
            P(),
            P(),
            P("sp", "tp"),
            P("sp", "tp"),
            P(None, "tp"),
            P(None, "tp"),
            P("sp", "tp"),
        ),
        out_specs=P(("grp", "sp", "tp"), None),
        check_vma=False,
    )
```

```python
import functools
import numpy as np
import jax
import jax.numpy as jnp
from jax import lax
from jax.experimental import pallas as pl
from jax.experimental.pallas import tpu as pltpu
from jax.sharding import PartitionSpec as P

HEADS = 8
KVH = 2
GRID_W = 64
EPSILON = 1e-06
THETA = 10000.0
F32 = jnp.float32
BF16 = jnp.bfloat16
NT = (((1,), (1,)), ((), ()))


def rotary_parts(seq_total, head_dim):
    quarter = head_dim // 4
    inverse = THETA ** (-(2.0 * np.arange(quarter, dtype=np.float32)) / np.float32(head_dim // 2))
    inverse = inverse.astype(np.float32)
    rows = seq_total // GRID_W
    row_angle = (np.arange(rows) - rows // 2).astype(np.float32)[:, None] * inverse
    col_angle = (np.arange(GRID_W) - GRID_W // 2).astype(np.float32)[:, None] * inverse

    def lanes(angle, first):
        zero = np.zeros_like(angle)
        cos, sin = np.cos(angle.astype(np.float64)), np.sin(angle.astype(np.float64))
        cos, sin = [cos, cos], [-sin, sin]
        pad = [zero, zero]
        parts = (cos + pad if first else pad + cos) + (sin + pad if first else pad + sin)
        return np.concatenate(parts, axis=-1).astype(np.float32)

    return lanes(row_angle, True), lanes(col_angle, False)


def turned(raw, gain, cos, sin, factor):
    x = raw.astype(F32)
    head_dim = x.shape[-1]
    quarter = head_dim // 4
    normed = x * lax.rsqrt(jnp.mean(x * x, axis=-1, keepdims=True) + EPSILON) * gain
    lane = lax.broadcasted_iota(jnp.int32, x.shape, 1)
    other = jnp.where(
        (lane & quarter) == 0,
        pltpu.roll(normed, head_dim - quarter, 1),
        pltpu.roll(normed, quarter, 1),
    )
    return ((normed * cos + other * sin) * factor).astype(BF16)


def key_kernel(at_ref, k_ref, v_ref, down_ref, gain_ref, row_ref, col_ref, out_ref):
    part, hd = k_ref.shape
    count = part // GRID_W
    for i in range(count):
        rows = pl.ds(i * GRID_W, GRID_W)
        table = row_ref[0, pl.ds(at_ref[0] * count + i, 1), :] + col_ref[...]
        out_ref[rows, :] = turned(k_ref[rows, :], gain_ref[...], table[:, :hd], table[:, hd:], 1.0)
    out_ref[pl.ds(part, part), :] = v_ref[...]
    out_ref[pl.ds(2 * part, down_ref.shape[0]), :] = down_ref[...]


def query_kernel(toks, *refs):
    raws, (gain_ref, row_ref, col_ref, out_ref) = refs[:-4], refs[-4:]
    hd = raws[0].shape[1]
    blocks = raws[0].shape[0] // GRID_W
    for i in range(blocks):
        table = row_ref[0, pl.ds(i, 1), :] + col_ref[...]
        for k, raw in enumerate(raws):
            q = turned(
                raw[pl.ds(i * GRID_W, GRID_W), :], gain_ref[...], table[:, :hd], table[:, hd:], hd ** (-0.5)
            )
            at = 0
            while at < GRID_W:
                owner, inside = divmod(i * GRID_W + at, toks)
                size = min(toks - inside, GRID_W - at)
                out_ref[owner, pl.ds(k * toks + inside, size), :] = q[at : at + size]
                at += size


def as_row(col, eye):
    return jnp.sum(jnp.where(eye, col, 0.0), axis=0, keepdims=True)


def as_col(row, eye):
    return jnp.sum(jnp.where(eye, row, 0.0), axis=1, keepdims=True)


def square_eye(n):
    return lax.broadcasted_iota(jnp.int32, (n, n), 0) == lax.broadcasted_iota(jnp.int32, (n, n), 1)


def attend_kernel(shards, first, last, *refs):
    q_ref, refs = refs[0], refs[1:]
    kv, refs = refs[:shards], refs[shards:]
    if not first:
        carry_ref, refs = refs[0], refs[1:]
    out_ref = refs[0]
    rows, hd = q_ref.shape[1:]
    part = kv[0].shape[0] // 2
    half = hd // 2
    keys = jnp.concatenate([r[pl.ds(0, part), :] for r in kv], axis=0)
    vals = jnp.concatenate([r[pl.ds(part, part), :] for r in kv], axis=0)
    s = lax.dot_general(q_ref[0], keys, NT, preferred_element_type=F32)
    m = jnp.max(s, axis=1, keepdims=True)
    if not first:
        m_old = carry_ref[0, pl.ds(rows, rows), 0:1]
        den_old = carry_ref[0, pl.ds(rows, rows), half : half + 1]
        m = jnp.maximum(m, m_old)
    p = jnp.exp(s - m)
    den = jnp.sum(p, axis=1, keepdims=True)
    acc = jnp.dot(p.astype(BF16), vals, preferred_element_type=F32)
    if not first:
        fade = jnp.exp(m_old - m)
        den = den + den_old * fade
        acc = acc + carry_ref[0, pl.ds(0, rows), :] * fade
    if not last:
        out_ref[0, pl.ds(0, rows), :] = acc
        lane = lax.broadcasted_iota(jnp.int32, (rows, hd), 1)
        out_ref[0, pl.ds(rows, rows), :] = jnp.where(lane < half, m, den)
        return
    out_ref[0, pl.ds(0, rows), :] = (acc / den).astype(BF16)
    eye = square_eye(hd)
    lse = m + jnp.log(den)
    stats = [as_row(lse[b * hd : (b + 1) * hd], eye) for b in range(rows // hd)]
    tail = out_ref.shape[1] - rows
    left = jnp.concatenate(stats + [jnp.zeros((8 - len(stats), hd), F32)], axis=0)
    high = left.astype(BF16).astype(F32)
    left = left - high
    mid = left.astype(BF16).astype(F32)
    out_ref[0, pl.ds(rows, tail), :] = jnp.concatenate(
        [high, mid, left - mid, jnp.zeros((tail - 24, hd), F32)], axis=0
    ).astype(BF16)


def normalised(x, gain):
    return x * lax.rsqrt(jnp.mean(x * x, axis=-1, keepdims=True) + EPSILON) * gain


def mix_kernel(group, pieces, at_ref, in_ref, res_ref, mg_ref, fg_ref, *refs):
    parts, refs = refs[:pieces], refs[pieces:]
    stream_ref, normed_ref, head_ref, att_ref, w_ref, sem = refs
    copies = []
    for i, part in enumerate(parts):
        size = part.shape[0]
        start = pl.multiple_of(at_ref[i], size)
        copies.append(pltpu.make_async_copy(part, w_ref.at[pl.ds(start, size), :], sem.at[i]))
    for c in copies:
        c.start()
    sources = in_ref.shape[0]
    hd = in_ref.shape[2]
    toks = res_ref.shape[0]
    rows = group * toks
    splits = sources // KVH
    eye = square_eye(hd)
    for kv in range(KVH):
        lse = []
        for j in range(splits):
            t = in_ref[kv * splits + j, pl.ds(rows, in_ref.shape[1] - rows), :].astype(F32)
            t = t[0:8] + t[8:16] + t[16:24]
            lse.append(t)
        cols = []
        for j in range(splits):
            blocks = [as_col(lse[j][b : b + 1], eye) for b in range(rows // hd)]
            cols.append(jnp.concatenate(blocks, axis=0))
        for h in range(group):
            mine = [cols[j][(h ^ j) * toks : (h ^ j) * toks + toks] for j in range(splits)]
            top = functools.reduce(jnp.maximum, mine)
            w = [jnp.exp(x - top) for x in mine]
            total = functools.reduce(jnp.add, w)
            acc = None
            for j in range(splits):
                o = in_ref[kv * splits + j, pl.ds((h ^ j) * toks, toks), :].astype(F32)
                term = (w[j] / total) * o
                acc = term if acc is None else acc + term
            c = (kv * group + h) * hd
            att_ref[:, c : c + hd] = acc.astype(BF16)
    for c in copies:
        c.wait()
    mix = jnp.dot(att_ref[...], w_ref[...], preferred_element_type=F32)
    stream = (res_ref[...].astype(F32) + normalised(mix, mg_ref[...])).astype(BF16)
    stream_ref[...] = stream
    normed_ref[...] = normalised(stream.astype(F32), fg_ref[...]).astype(BF16)


def gelu(v):
    return 0.5 * v * (1.0 + jnp.tanh(0.7978845608028654 * (v + 0.044715 * v * v * v)))


def ffn_kernel(pieces, shards, at_ref, halo_ref, taps_ref, gv_ref, *refs):
    toks_in, refs = refs[:pieces], refs[pieces:]
    downs, refs = refs[:shards], refs[shards:]
    keep_ref, send_ref, x_ref, w_ref, d_ref, h_ref, p_ref, sem_x, sem_w, sem_d, sem_o = refs
    main = x_ref.shape[0] - halo_ref.shape[0]
    units = h_ref.shape[1]
    lanes = gv_ref.shape[2]
    skip = downs[0].shape[0] - units

    def token_copy(i):
        size = toks_in[i].shape[0]
        start = pl.multiple_of(at_ref[i], 16)
        return pltpu.make_async_copy(toks_in[i], x_ref.at[pl.ds(start, size), :], sem_x.at[i])

    def weight_copy(i):
        return pltpu.make_async_copy(gv_ref.at[i], w_ref.at[:, pl.ds(i * lanes, lanes)], sem_w.at[i])

    def down_copy(i):
        start = pl.multiple_of(at_ref[pieces + i], lanes)
        return pltpu.make_async_copy(
            downs[i].at[pl.ds(skip, units), :], d_ref.at[:, pl.ds(start, lanes)], sem_d.at[i]
        )

    for i in range(pieces):
        token_copy(i).start()
    for i in range(shards):
        weight_copy(i).start()
    for i in range(shards):
        down_copy(i).start()
    x_ref[pl.ds(main, halo_ref.shape[0]), :] = halo_ref[...]
    for i in range(pieces):
        token_copy(i).wait()
    for i in range(shards):
        weight_copy(i).wait()

    def up_block(b, size):
        start = pl.multiple_of(b * block, block)
        w = jnp.concatenate(
            [w_ref[pl.ds(start, size), :], w_ref[pl.ds(units + start, size), :]], axis=0
        )
        up = lax.dot_general(x_ref[...], w, NT, preferred_element_type=F32)
        up = up.astype(BF16).astype(F32)
        now = up[:main]
        row = lax.broadcasted_iota(jnp.int32, now.shape, 0)
        before = jnp.where(row == 0, up[main : main + 1], pltpu.roll(now, 1, 0))
        after = jnp.where(row == main - 1, up[main + 1 : main + 2], pltpu.roll(now, main - 1, 0))
        taps = taps_ref[b]
        mixed = taps[0:1, : 2 * size] * before + taps[1:2, : 2 * size] * now + taps[2:3, : 2 * size] * after
        return (gelu(mixed[:, :size]) * mixed[:, size:]).astype(BF16)

    block = 128
    full = units // block

    def full_block(b, unused):
        h_ref[:, pl.ds(pl.multiple_of(b * block, block), block)] = up_block(b, block)
        return unused

    lax.fori_loop(0, full, full_block, 0)
    if units % block:
        h_ref[:, full * block :] = up_block(full, units % block)

    for i in range(shards):
        down_copy(i).wait()

    def down_block(n, unused):
        cols = pl.ds(pl.multiple_of(n * 256, 256), 256)
        p_ref[:, cols] = jnp.dot(h_ref[...], d_ref[:, cols], preferred_element_type=F32).astype(BF16)
        return unused

    lax.fori_loop(0, d_ref.shape[1] // 256, down_block, 0)
    count, own = keep_ref.shape[0], keep_ref.shape[1]
    outs = []
    for k in range(count):
        for o, ref in enumerate((keep_ref, send_ref)):
            start = pl.multiple_of(at_ref[pieces + shards + 2 * k + o], 16)
            outs.append(
                pltpu.make_async_copy(p_ref.at[pl.ds(start, own), :], ref.at[k], sem_o.at[2 * k + o])
            )
    for c in outs:
        c.start()
    for c in outs:
        c.wait()


def vmem(limit=56 << 20):
    return pltpu.CompilerParams(vmem_limit_bytes=limit)


def body(
    queries,
    keys,
    values,
    query_gain,
    key_gain,
    residual,
    out_weight,
    mix_gain,
    ffn_gain,
    gate_in,
    value_in,
    conv_gate,
    conv_value,
    down_t,
):
    tok = queries.shape[0]
    hd = query_gain.shape[0]
    n_sp, n_tp = lax.axis_size("sp"), lax.axis_size("tp")
    n_x = n_tp // 2
    group = HEADS // KVH
    splits = n_tp // KVH
    part = tok // splits
    own = tok // n_tp
    model = residual.shape[1]
    units = gate_in.shape[1]
    tp, sp = lax.axis_index("tp"), lax.axis_index("sp")
    kv_head, piece = tp // splits, tp % splits
    x, core = tp // 2, tp % 2

    def send(array, change):
        return lax.ppermute(array, "tp", [(i, change(i)) for i in range(n_tp)])

    def other_core(array):
        return send(array, lambda i: i ^ 1)

    def up_x(array):
        return send(array, lambda i: (i + 2) % n_tp)

    def down_x(array):
        return send(array, lambda i: (i - 2) % n_tp)

    def far_x(array):
        return send(array, lambda i: (i + n_x) % n_tp)

    def gathered(mine):
        size = mine.shape[0]
        half = size // 2
        a = up_x(mine)
        b = down_x(mine)
        near = other_core(mine)
        c = up_x(a[:half])
        d = down_x(b[half:])
        low, high = ((x + n_x - 1) % n_x) * 2, ((x + 1) % n_x) * 2
        far = (tp + n_x) % n_tp
        found = [(mine, tp * size), (near, (tp ^ 1) * size)]
        for array, base in ((a, low), (b, high)):
            found.append((array, (base + core) * size))
            found.append((other_core(array), (base + 1 - core) * size))
        for array, shift in ((c, 0), (d, half)):
            found.append((array, far * size + shift))
            found.append((other_core(array), (far ^ 1) * size + shift))
        return [f[0] for f in found], [f[1] for f in found]

    row_np, col_np = rotary_parts(tok * n_sp, hd)
    row_np = row_np.reshape(n_sp, tok // GRID_W, 2 * hd)
    rows_all, cols_all = jnp.asarray(row_np), jnp.asarray(col_np)
    at = jnp.stack([piece, kv_head, sp]).astype(jnp.int32)
    packed_rows = 2 * part + units
    packed = pl.pallas_call(
        key_kernel,
        out_shape=jax.ShapeDtypeStruct((packed_rows, hd), BF16),
        grid_spec=pltpu.PrefetchScalarGridSpec(
            num_scalar_prefetch=1,
            grid=(1,),
            in_specs=[
                pl.BlockSpec((part, hd), lambda i, a: (a[0], a[1])),
                pl.BlockSpec((part, hd), lambda i, a: (a[0], a[1])),
                pl.BlockSpec((units, hd), lambda i, a: (0, 0)),
                pl.BlockSpec((1, hd), lambda i, a: (0, 0)),
                pl.BlockSpec((1,) + row_np.shape[1:], lambda i, a: (a[2], 0, 0)),
                pl.BlockSpec(col_np.shape, lambda i, a: (0, 0)),
            ],
            out_specs=pl.BlockSpec((packed_rows, hd), lambda i, a: (0, 0)),
        ),
        name="key_prep",
    )(at, keys, values, down_t.T, key_gain[None], rows_all, cols_all)
    gate_rows = lax.all_gather(jnp.concatenate([gate_in.T, value_in.T], axis=0), "sp", axis=0, tiled=False)

    raw = [queries, other_core(queries)]
    pair = send(queries, lambda i: i ^ 2)
    raw += [pair, other_core(pair)]
    rows = group * own
    turned_q = pl.pallas_call(
        lambda at_ref, *refs: query_kernel(own, *refs),
        out_shape=jax.ShapeDtypeStruct((n_tp, rows, hd), BF16),
        grid_spec=pltpu.PrefetchScalarGridSpec(
            num_scalar_prefetch=1,
            grid=(1,),
            in_specs=[pl.BlockSpec((tok, hd), lambda i, a: (0, 0))] * group
            + [
                pl.BlockSpec((1, hd), lambda i, a: (0, 0)),
                pl.BlockSpec((1,) + row_np.shape[1:], lambda i, a: (a[2], 0, 0)),
                pl.BlockSpec(col_np.shape, lambda i, a: (0, 0)),
            ],
            out_specs=pl.BlockSpec((n_tp, rows, hd), lambda i, a: (0, 0, 0)),
        ),
        name="query_prep",
    )(at, *raw, query_gain[None], rows_all, cols_all)

    out_pieces, out_at = gathered(out_weight)

    right = [(i, (i + 1) % n_sp) for i in range(n_sp)]
    left = [(i, (i - 1) % n_sp) for i in range(n_sp)]
    tail = 32
    step = 4
    calls = n_sp // step

    def attend(c, here, carry):
        last = c == calls - 1
        shape = (n_tp, rows + tail, hd) if last else (n_tp, 2 * rows, hd)
        operands = [turned_q] + here + ([] if carry is None else [carry])
        specs = [pl.BlockSpec((1, rows, hd), lambda i: (i, 0, 0))]
        specs += [pl.BlockSpec((2 * part, hd), lambda i: (0, 0))] * step
        if carry is not None:
            specs.append(pl.BlockSpec((1, 2 * rows, hd), lambda i: (i, 0, 0)))
        return pl.pallas_call(
            functools.partial(attend_kernel, step, c == 0, last),
            out_shape=jax.ShapeDtypeStruct(shape, BF16 if last else F32),
            grid=(n_tp,),
            in_specs=specs,
            out_specs=pl.BlockSpec((1,) + shape[1:], lambda i: (i, 0, 0)),
            compiler_params=vmem(),
            cost_estimate=pl.CostEstimate(
                flops=8 * group * tok * part * step * hd,
                bytes_accessed=8 << 20,
                transcendentals=group * tok * part * step,
            ),
            name="attend%d" % c,
        )(*operands)

    shards, sources = [packed], [sp]
    a = b = packed
    carry = None
    done = 0
    for s in range(1, n_sp // 2 + 1):
        a = lax.ppermute(a, "sp", right)
        shards.append(a)
        sources.append((sp + n_sp - s) % n_sp)
        if len(shards) < n_sp:
            b = lax.ppermute(b, "sp", left)
            shards.append(b)
            sources.append((sp + s) % n_sp)
        if s % 2 == 0:
            if carry is None:
                a, b, turned_q = lax.optimization_barrier((a, b, turned_q))
            else:
                a, b, carry = lax.optimization_barrier((a, b, carry))
            if s == n_sp // 2:
                carry, *out_pieces = lax.optimization_barrier((carry, *out_pieces))
            carry = attend(done, shards[done * step : (done + 1) * step], carry)
            done += 1

    seen = lax.all_to_all(carry, "tp", split_axis=0, concat_axis=0, tiled=True)
    anywhere = pl.BlockSpec(memory_space=pl.ANY)
    whole = pl.BlockSpec(memory_space=pltpu.VMEM)
    stream, normed = pl.pallas_call(
        functools.partial(mix_kernel, group, len(out_pieces)),
        out_shape=[jax.ShapeDtypeStruct((own, model), BF16)] * 2,
        in_specs=[pl.BlockSpec(memory_space=pltpu.SMEM)] + [whole] * 4 + [anywhere] * len(out_pieces),
        scratch_shapes=[
            pltpu.VMEM((rows, hd), F32),
            pltpu.VMEM((own, HEADS * hd), BF16),
            pltpu.VMEM((HEADS * hd, model), BF16),
            pltpu.SemaphoreType.DMA((len(out_pieces),)),
        ],
        compiler_params=vmem(),
        cost_estimate=pl.CostEstimate(
            flops=2 * own * HEADS * hd * model, bytes_accessed=6 << 20, transcendentals=0
        ),
        name="mix",
    )(jnp.stack(out_at).astype(jnp.int32), seen, residual, mix_gain[None], ffn_gain[None], *out_pieces)

    token_pieces, token_at = gathered(normed)
    first = last_row = None
    for p, r in zip(token_pieces, token_at):
        f = jnp.where(r == 0, p[:1], 0)
        e = jnp.where(r + p.shape[0] == tok, p[-1:], 0)
        first = f if first is None else first + f
        last_row = e if last_row is None else last_row + e
    before = lax.ppermute(last_row, "sp", [(i, i + 1) for i in range(n_sp - 1)])
    after = lax.ppermute(first, "sp", [(i + 1, i) for i in range(n_sp - 1)])
    halo = jnp.concatenate([before, after, jnp.zeros((14, model), BF16)], axis=0)
    blocks = -(-units // 128)
    taps = []
    for t in range(blocks):
        lo, hi = t * 128, min(units, t * 128 + 128)
        both = jnp.concatenate([conv_gate[:, lo:hi], conv_value[:, lo:hi]], axis=1)
        taps.append(jnp.pad(both, ((0, 5), (0, 256 - both.shape[1]))))
    taps = jnp.stack(taps)
    slots = []
    for k in range(n_x):
        to = ((x + k) % n_x) * 2
        slots += [(to + core) * own, (to + 1 - core) * own]
    where = jnp.stack(token_at + [s * hd for s in sources] + slots).astype(jnp.int32)
    keep, away = pl.pallas_call(
        functools.partial(ffn_kernel, len(token_pieces), n_sp),
        out_shape=[jax.ShapeDtypeStruct((n_x, own, model), BF16)] * 2,
        in_specs=[pl.BlockSpec(memory_space=pltpu.SMEM), whole, whole]
        + [anywhere] * (1 + len(token_pieces) + n_sp),
        out_specs=[anywhere, anywhere],
        scratch_shapes=[
            pltpu.VMEM((tok + 16, model), BF16),
            pltpu.VMEM((2 * units, model), BF16),
            pltpu.VMEM((units, model), BF16),
            pltpu.VMEM((tok, units), BF16),
            pltpu.VMEM((tok, model), BF16),
            pltpu.SemaphoreType.DMA((len(token_pieces),)),
            pltpu.SemaphoreType.DMA((n_sp,)),
            pltpu.SemaphoreType.DMA((n_sp,)),
            pltpu.SemaphoreType.DMA((2 * n_x,)),
        ],
        compiler_params=vmem(),
        cost_estimate=pl.CostEstimate(
            flops=6 * tok * units * model, bytes_accessed=16 << 20, transcendentals=tok * units
        ),
        name="ffn",
    )(where, halo, taps, gate_rows, *token_pieces, *shards)
    near = other_core(away)
    total = [keep[k].astype(F32) + near[k].astype(F32) for k in range(n_x)]
    one = up_x(total[1].astype(BF16))
    two = far_x(total[2].astype(BF16))
    three = down_x(total[3].astype(BF16))
    out = total[0] + one.astype(F32) + two.astype(F32) + three.astype(F32)
    return (stream.astype(F32) + out).astype(BF16)


def solution(mesh):
    return jax.shard_map(
        body,
        mesh=mesh,
        in_specs=(
            P(("grp", "sp"), "tp"),
            P(("grp", "sp"), None),
            P(("grp", "sp"), None),
            P(),
            P(),
            P(("grp", "sp", "tp"), None),
            P("tp", None),
            P(),
            P(),
            P("sp", "tp"),
            P("sp", "tp"),
            P(None, "tp"),
            P(None, "tp"),
            P("sp", "tp"),
        ),
        out_specs=P(("grp", "sp", "tp"), None),
        check_vma=False,
    )
```

```python
import functools
import numpy as np
import jax
import jax.numpy as jnp
from jax import lax
from jax.experimental import pallas as pl
from jax.experimental.pallas import tpu as pltpu
from jax.sharding import PartitionSpec as P

HEADS = 8
KVH = 2
GRID_W = 64
EPSILON = 1e-06
THETA = 10000.0
F32 = jnp.float32
BF16 = jnp.bfloat16
NT = (((1,), (1,)), ((), ()))


def rotary_parts(seq_total, head_dim):
    quarter = head_dim // 4
    inverse = THETA ** (-(2.0 * np.arange(quarter, dtype=np.float32)) / np.float32(head_dim // 2))
    inverse = inverse.astype(np.float32)
    rows = seq_total // GRID_W
    row_angle = (np.arange(rows) - rows // 2).astype(np.float32)[:, None] * inverse
    col_angle = (np.arange(GRID_W) - GRID_W // 2).astype(np.float32)[:, None] * inverse

    def lanes(angle, first):
        zero = np.zeros_like(angle)
        cos, sin = np.cos(angle.astype(np.float64)), np.sin(angle.astype(np.float64))
        cos, sin = [cos, cos], [-sin, sin]
        pad = [zero, zero]
        parts = (cos + pad if first else pad + cos) + (sin + pad if first else pad + sin)
        return np.concatenate(parts, axis=-1).astype(np.float32)

    return lanes(row_angle, True), lanes(col_angle, False)


def turned(raw, gain, cos, sin, factor):
    x = raw.astype(F32)
    head_dim = x.shape[-1]
    quarter = head_dim // 4
    normed = x * lax.rsqrt(jnp.mean(x * x, axis=-1, keepdims=True) + EPSILON) * gain
    lane = lax.broadcasted_iota(jnp.int32, x.shape, 1)
    other = jnp.where(
        (lane & quarter) == 0,
        pltpu.roll(normed, head_dim - quarter, 1),
        pltpu.roll(normed, quarter, 1),
    )
    return ((normed * cos + other * sin) * factor).astype(BF16)


def key_kernel(at_ref, k_ref, v_ref, gain_ref, row_ref, col_ref, out_ref):
    part, hd = k_ref.shape
    count = part // GRID_W
    for i in range(count):
        rows = pl.ds(i * GRID_W, GRID_W)
        table = row_ref[0, pl.ds(at_ref[0] * count + i, 1), :] + col_ref[...]
        out_ref[rows, :] = turned(k_ref[rows, :], gain_ref[...], table[:, :hd], table[:, hd:], 1.0)
    out_ref[pl.ds(part, part), :] = v_ref[...]


def query_kernel(toks, *refs):
    raws, (gain_ref, row_ref, col_ref, out_ref) = refs[:-4], refs[-4:]
    hd = raws[0].shape[1]
    blocks = raws[0].shape[0] // GRID_W
    for i in range(blocks):
        table = row_ref[0, pl.ds(i, 1), :] + col_ref[...]
        for k, raw in enumerate(raws):
            q = turned(
                raw[pl.ds(i * GRID_W, GRID_W), :], gain_ref[...], table[:, :hd], table[:, hd:], hd ** (-0.5)
            )
            at = 0
            while at < GRID_W:
                owner, inside = divmod(i * GRID_W + at, toks)
                size = min(toks - inside, GRID_W - at)
                out_ref[owner, pl.ds(k * toks + inside, size), :] = q[at : at + size]
                at += size


def as_row(col, eye):
    return jnp.sum(jnp.where(eye, col, 0.0), axis=0, keepdims=True)


def as_col(row, eye):
    return jnp.sum(jnp.where(eye, row, 0.0), axis=1, keepdims=True)


def square_eye(n):
    return lax.broadcasted_iota(jnp.int32, (n, n), 0) == lax.broadcasted_iota(jnp.int32, (n, n), 1)


def attend_kernel(shards, *refs):
    q_ref, kv, out_ref = refs[0], refs[1 : 1 + shards], refs[1 + shards]
    rows, hd = q_ref.shape[1:]
    part = kv[0].shape[0] // 2
    keys = jnp.concatenate([r[pl.ds(0, part), :] for r in kv], axis=0)
    vals = jnp.concatenate([r[pl.ds(part, part), :] for r in kv], axis=0)
    s = lax.dot_general(q_ref[0], keys, NT, preferred_element_type=F32)
    m = jnp.max(s, axis=1, keepdims=True)
    p = jnp.exp(s - m)
    den = jnp.sum(p, axis=1, keepdims=True)
    acc = jnp.dot(p.astype(BF16), vals, preferred_element_type=F32)
    out_ref[0, pl.ds(0, rows), :] = (acc / den).astype(BF16)
    eye = square_eye(hd)
    lse = m + jnp.log(den)
    stats = [as_row(lse[b * hd : (b + 1) * hd], eye) for b in range(rows // hd)]
    tail = out_ref.shape[1] - rows
    left = jnp.concatenate(stats + [jnp.zeros((8 - len(stats), hd), F32)], axis=0)
    high = left.astype(BF16).astype(F32)
    left = left - high
    mid = left.astype(BF16).astype(F32)
    out_ref[0, pl.ds(rows, tail), :] = jnp.concatenate(
        [high, mid, left - mid, jnp.zeros((tail - 24, hd), F32)], axis=0
    ).astype(BF16)


def normalised(x, gain):
    return x * lax.rsqrt(jnp.mean(x * x, axis=-1, keepdims=True) + EPSILON) * gain


def mix_kernel(group, pieces, at_ref, in_ref, res_ref, mg_ref, fg_ref, *refs):
    parts, refs = refs[:pieces], refs[pieces:]
    stream_ref, normed_ref, head_ref, att_ref, w_ref, sem = refs
    copies = []
    for i, part in enumerate(parts):
        size = part.shape[0]
        start = pl.multiple_of(at_ref[i], size)
        copies.append(pltpu.make_async_copy(part, w_ref.at[pl.ds(start, size), :], sem.at[i]))
    for c in copies:
        c.start()
    sources = in_ref.shape[0]
    hd = in_ref.shape[2]
    toks = res_ref.shape[0]
    rows = group * toks
    splits = sources // KVH
    eye = square_eye(hd)
    for kv in range(KVH):
        lse = []
        for j in range(splits):
            t = in_ref[kv * splits + j, pl.ds(rows, in_ref.shape[1] - rows), :].astype(F32)
            t = t[0:8] + t[8:16] + t[16:24]
            lse.append(t)
        cols = []
        for j in range(splits):
            blocks = [as_col(lse[j][b : b + 1], eye) for b in range(rows // hd)]
            cols.append(jnp.concatenate(blocks, axis=0))
        for h in range(group):
            mine = [cols[j][(h ^ j) * toks : (h ^ j) * toks + toks] for j in range(splits)]
            top = functools.reduce(jnp.maximum, mine)
            w = [jnp.exp(x - top) for x in mine]
            total = functools.reduce(jnp.add, w)
            acc = None
            for j in range(splits):
                o = in_ref[kv * splits + j, pl.ds((h ^ j) * toks, toks), :].astype(F32)
                term = (w[j] / total) * o
                acc = term if acc is None else acc + term
            c = (kv * group + h) * hd
            att_ref[:, c : c + hd] = acc.astype(BF16)
    for c in copies:
        c.wait()
    mix = jnp.dot(att_ref[...], w_ref[...], preferred_element_type=F32)
    stream = (res_ref[...].astype(F32) + normalised(mix, mg_ref[...])).astype(BF16)
    stream_ref[...] = stream
    normed_ref[...] = normalised(stream.astype(F32), fg_ref[...]).astype(BF16)


def gelu(v):
    return 0.5 * v * (1.0 + jnp.tanh(0.7978845608028654 * (v + 0.044715 * v * v * v)))


def ffn_kernel(pieces, at_ref, halo_ref, taps_ref, all_ref, *refs):
    toks_in, refs = refs[:pieces], refs[pieces:]
    keep_ref, send_ref, x_ref, g_ref, v_ref, d_ref, even_ref, odd_ref, h_ref, p_ref = refs[:10]
    sem_x, sem_g, sem_v, sem_d, sem_o = refs[10:]
    main = x_ref.shape[0] - halo_ref.shape[0]
    units = d_ref.shape[1]
    shards = d_ref.shape[0]
    block = taps_ref.shape[2] // 2
    blocks = taps_ref.shape[0]

    def token_copy(i):
        size = toks_in[i].shape[0]
        start = pl.multiple_of(at_ref[i], 16)
        return pltpu.make_async_copy(toks_in[i], x_ref.at[pl.ds(start, size), :], sem_x.at[i])

    def rows_copy(b, base, ref, sem):
        start = pl.multiple_of(b * block, block)
        return pltpu.make_async_copy(
            all_ref.at[:, pl.ds(base + start, block), :], ref.at[:, pl.ds(start, block), :], sem.at[b]
        )

    def gate_copy(b):
        return rows_copy(b, 0, g_ref, sem_g)

    def value_copy(b):
        return rows_copy(b, units, v_ref, sem_v)

    down = pltpu.make_async_copy(all_ref.at[:, pl.ds(2 * units, units), :], d_ref, sem_d)
    for i in range(pieces):
        token_copy(i).start()
    for b in range(blocks):
        gate_copy(b).start()
        value_copy(b).start()
    down.start()
    x_ref[pl.ds(main, halo_ref.shape[0]), :] = halo_ref[...]
    for i in range(pieces):
        token_copy(i).wait()

    def arrive(b):
        gate_copy(b).wait()
        value_copy(b).wait()

    def up(b, out_ref):
        rows = pl.ds(b * block, block)
        w = [
            jnp.concatenate([ref[s, rows, :] for s in range(shards)], axis=1) for ref in (g_ref, v_ref)
        ]
        w = jnp.concatenate(w, axis=0)
        y = lax.dot_general(x_ref[...], w, NT, preferred_element_type=F32)
        out_ref[...] = y.astype(BF16).astype(F32)

    def finish(b, in_ref):
        now = in_ref[pl.ds(0, main), :]
        row = lax.broadcasted_iota(jnp.int32, now.shape, 0)
        before = jnp.where(row == 0, in_ref[main : main + 1, :], pltpu.roll(now, 1, 0))
        after = jnp.where(row == main - 1, in_ref[main + 1 : main + 2, :], pltpu.roll(now, main - 1, 0))
        taps = taps_ref[b]
        mixed = taps[0:1] * before + taps[1:2] * now + taps[2:3] * after
        h_ref[:, pl.ds(b * block, block)] = (gelu(mixed[:, :block]) * mixed[:, block:]).astype(BF16)

    arrive(0)
    up(0, even_ref)

    def pair(i, unused):
        b = pl.multiple_of(2 * i, 2)
        arrive(b + 1)
        arrive(b + 2)
        up(b + 1, odd_ref)
        finish(b, even_ref)
        up(b + 2, even_ref)
        finish(b + 1, odd_ref)
        return unused

    lax.fori_loop(0, blocks // 2 - 1, pair, 0)
    arrive(blocks - 1)
    up(blocks - 1, odd_ref)
    finish(blocks - 2, even_ref)
    finish(blocks - 1, odd_ref)
    down.wait()

    def down_block(n, unused):
        w = jnp.concatenate([d_ref[2 * n], d_ref[2 * n + 1]], axis=1)
        y = jnp.dot(h_ref[:, :units], w, preferred_element_type=F32)
        p_ref[:, pl.ds(pl.multiple_of(n * 256, 256), 256)] = y.astype(BF16)
        return unused

    lax.fori_loop(0, shards // 2, down_block, 0)
    count, own = keep_ref.shape[0], keep_ref.shape[1]
    outs = []
    for k in range(count):
        for o, ref in enumerate((keep_ref, send_ref)):
            start = pl.multiple_of(at_ref[pieces + 2 * k + o], 16)
            outs.append(
                pltpu.make_async_copy(p_ref.at[pl.ds(start, own), :], ref.at[k], sem_o.at[2 * k + o])
            )
    for c in outs:
        c.start()
    for c in outs:
        c.wait()


def vmem(limit=56 << 20):
    return pltpu.CompilerParams(vmem_limit_bytes=limit)


def body(
    queries,
    keys,
    values,
    query_gain,
    key_gain,
    residual,
    out_weight,
    mix_gain,
    ffn_gain,
    gate_in,
    value_in,
    conv_gate,
    conv_value,
    down_t,
):
    tok = queries.shape[0]
    hd = query_gain.shape[0]
    n_sp, n_tp = lax.axis_size("sp"), lax.axis_size("tp")
    n_x = n_tp // 2
    group = HEADS // KVH
    splits = n_tp // KVH
    part = tok // splits
    own = tok // n_tp
    model = residual.shape[1]
    units = gate_in.shape[1]
    tp, sp = lax.axis_index("tp"), lax.axis_index("sp")
    kv_head, piece = tp // splits, tp % splits
    x, core = tp // 2, tp % 2

    def send(array, change):
        return lax.ppermute(array, "tp", [(i, change(i)) for i in range(n_tp)])

    def other_core(array):
        return send(array, lambda i: i ^ 1)

    def up_x(array):
        return send(array, lambda i: (i + 2) % n_tp)

    def down_x(array):
        return send(array, lambda i: (i - 2) % n_tp)

    def far_x(array):
        return send(array, lambda i: (i + n_x) % n_tp)

    def gathered(mine):
        size = mine.shape[0]
        half = size // 2
        a = up_x(mine)
        b = down_x(mine)
        near = other_core(mine)
        c = up_x(a[:half])
        d = down_x(b[half:])
        low, high = ((x + n_x - 1) % n_x) * 2, ((x + 1) % n_x) * 2
        far = (tp + n_x) % n_tp
        found = [(mine, tp * size), (near, (tp ^ 1) * size)]
        for array, base in ((a, low), (b, high)):
            found.append((array, (base + core) * size))
            found.append((other_core(array), (base + 1 - core) * size))
        for array, shift in ((c, 0), (d, half)):
            found.append((array, far * size + shift))
            found.append((other_core(array), (far ^ 1) * size + shift))
        return [f[0] for f in found], [f[1] for f in found]

    row_np, col_np = rotary_parts(tok * n_sp, hd)
    row_np = row_np.reshape(n_sp, tok // GRID_W, 2 * hd)
    rows_all, cols_all = jnp.asarray(row_np), jnp.asarray(col_np)
    at = jnp.stack([piece, kv_head, sp]).astype(jnp.int32)
    packed_rows = 2 * part
    packed = pl.pallas_call(
        key_kernel,
        out_shape=jax.ShapeDtypeStruct((packed_rows, hd), BF16),
        grid_spec=pltpu.PrefetchScalarGridSpec(
            num_scalar_prefetch=1,
            grid=(1,),
            in_specs=[
                pl.BlockSpec((part, hd), lambda i, a: (a[0], a[1])),
                pl.BlockSpec((part, hd), lambda i, a: (a[0], a[1])),
                pl.BlockSpec((1, hd), lambda i, a: (0, 0)),
                pl.BlockSpec((1,) + row_np.shape[1:], lambda i, a: (a[2], 0, 0)),
                pl.BlockSpec(col_np.shape, lambda i, a: (0, 0)),
            ],
            out_specs=pl.BlockSpec((packed_rows, hd), lambda i, a: (0, 0)),
        ),
        name="key_prep",
    )(at, keys, values, key_gain[None], rows_all, cols_all)
    gate_rows = lax.all_gather(
        jnp.concatenate([gate_in.T, value_in.T, down_t.T], axis=0), "sp", axis=0, tiled=False
    )

    raw = [queries, other_core(queries)]
    pair = send(queries, lambda i: i ^ 2)
    raw += [pair, other_core(pair)]
    rows = group * own
    turned_q = pl.pallas_call(
        lambda at_ref, *refs: query_kernel(own, *refs),
        out_shape=jax.ShapeDtypeStruct((n_tp, rows, hd), BF16),
        grid_spec=pltpu.PrefetchScalarGridSpec(
            num_scalar_prefetch=1,
            grid=(1,),
            in_specs=[pl.BlockSpec((tok, hd), lambda i, a: (0, 0))] * group
            + [
                pl.BlockSpec((1, hd), lambda i, a: (0, 0)),
                pl.BlockSpec((1,) + row_np.shape[1:], lambda i, a: (a[2], 0, 0)),
                pl.BlockSpec(col_np.shape, lambda i, a: (0, 0)),
            ],
            out_specs=pl.BlockSpec((n_tp, rows, hd), lambda i, a: (0, 0, 0)),
        ),
        name="query_prep",
    )(at, *raw, query_gain[None], rows_all, cols_all)

    out_pieces, out_at = gathered(out_weight)

    packed, queries, out_weight = lax.optimization_barrier((packed, queries, out_weight))
    right = [(i, (i + 1) % n_sp) for i in range(n_sp)]
    left = [(i, (i - 1) % n_sp) for i in range(n_sp)]
    tail = 32
    shards = [packed]
    a = b = packed
    for s in range(1, n_sp // 2 + 1):
        a = lax.ppermute(a, "sp", right)
        shards.append(a)
        if len(shards) < n_sp:
            b = lax.ppermute(b, "sp", left)
            shards.append(b)
        if s == n_sp // 4:
            a, b, turned_q = lax.optimization_barrier((a, b, turned_q))
    a, *out_pieces = lax.optimization_barrier((a, *out_pieces))
    carry = pl.pallas_call(
        functools.partial(attend_kernel, n_sp),
        out_shape=jax.ShapeDtypeStruct((n_tp, rows + tail, hd), BF16),
        grid=(n_tp,),
        in_specs=[pl.BlockSpec((1, rows, hd), lambda i: (i, 0, 0))]
        + [pl.BlockSpec((2 * part, hd), lambda i: (0, 0))] * n_sp,
        out_specs=pl.BlockSpec((1, rows + tail, hd), lambda i: (i, 0, 0)),
        compiler_params=vmem(),
        cost_estimate=pl.CostEstimate(
            flops=8 * group * tok * part * n_sp * hd,
            bytes_accessed=8 << 20,
            transcendentals=group * tok * part * n_sp,
        ),
        name="attend",
    )(turned_q, *shards[:-1], a)
    seen = lax.all_to_all(carry, "tp", split_axis=0, concat_axis=0, tiled=True)
    anywhere = pl.BlockSpec(memory_space=pl.ANY)
    whole = pl.BlockSpec(memory_space=pltpu.VMEM)
    stream, normed = pl.pallas_call(
        functools.partial(mix_kernel, group, len(out_pieces)),
        out_shape=[jax.ShapeDtypeStruct((own, model), BF16)] * 2,
        in_specs=[pl.BlockSpec(memory_space=pltpu.SMEM)] + [whole] * 4 + [anywhere] * len(out_pieces),
        scratch_shapes=[
            pltpu.VMEM((rows, hd), F32),
            pltpu.VMEM((own, HEADS * hd), BF16),
            pltpu.VMEM((HEADS * hd, model), BF16),
            pltpu.SemaphoreType.DMA((len(out_pieces),)),
        ],
        compiler_params=vmem(),
        cost_estimate=pl.CostEstimate(
            flops=2 * own * HEADS * hd * model, bytes_accessed=6 << 20, transcendentals=0
        ),
        name="mix",
    )(jnp.stack(out_at).astype(jnp.int32), seen, residual, mix_gain[None], ffn_gain[None], *out_pieces)

    token_pieces, token_at = gathered(normed)
    first = last_row = None
    for p, r in zip(token_pieces, token_at):
        f = jnp.where(r == 0, p[:1], 0)
        e = jnp.where(r + p.shape[0] == tok, p[-1:], 0)
        first = f if first is None else first + f
        last_row = e if last_row is None else last_row + e
    before = lax.ppermute(last_row, "sp", [(i, i + 1) for i in range(n_sp - 1)])
    after = lax.ppermute(first, "sp", [(i + 1, i) for i in range(n_sp - 1)])
    halo = jnp.concatenate([before, after, jnp.zeros((14, model), BF16)], axis=0)
    block = 128
    blocks = -(-units // block)

    def by_block(taps):
        wide = jnp.pad(taps, ((0, 5), (0, blocks * block - units)))
        return jnp.transpose(wide.reshape(8, blocks, block), (1, 0, 2))

    taps = jnp.concatenate([by_block(conv_gate), by_block(conv_value)], axis=2)
    slots = []
    for k in range(n_x):
        to = ((x + k) % n_x) * 2
        slots += [(to + core) * own, (to + 1 - core) * own]
    where = jnp.stack(token_at + slots).astype(jnp.int32)
    keep, away = pl.pallas_call(
        functools.partial(ffn_kernel, len(token_pieces)),
        out_shape=[jax.ShapeDtypeStruct((n_x, own, model), BF16)] * 2,
        in_specs=[pl.BlockSpec(memory_space=pltpu.SMEM), whole, whole]
        + [anywhere] * (1 + len(token_pieces)),
        out_specs=[anywhere, anywhere],
        scratch_shapes=[
            pltpu.VMEM((tok + 16, model), BF16),
            pltpu.VMEM((n_sp, blocks * block, hd), BF16),
            pltpu.VMEM((n_sp, blocks * block, hd), BF16),
            pltpu.VMEM((n_sp, units, hd), BF16),
            pltpu.VMEM((tok + 16, 2 * block), F32),
            pltpu.VMEM((tok + 16, 2 * block), F32),
            pltpu.VMEM((tok, blocks * block), BF16),
            pltpu.VMEM((tok, model), BF16),
            pltpu.SemaphoreType.DMA((len(token_pieces),)),
            pltpu.SemaphoreType.DMA((blocks,)),
            pltpu.SemaphoreType.DMA((blocks,)),
            pltpu.SemaphoreType.DMA,
            pltpu.SemaphoreType.DMA((2 * n_x,)),
        ],
        compiler_params=vmem(),
        cost_estimate=pl.CostEstimate(
            flops=6 * tok * units * model, bytes_accessed=16 << 20, transcendentals=tok * units
        ),
        name="ffn",
    )(where, halo, taps, gate_rows, *token_pieces)
    near = other_core(away)
    total = [keep[k].astype(F32) + near[k].astype(F32) for k in range(n_x)]
    one = up_x(total[1].astype(BF16))
    two = far_x(total[2].astype(BF16))
    three = down_x(total[3].astype(BF16))
    out = total[0] + one.astype(F32) + two.astype(F32) + three.astype(F32)
    return (stream.astype(F32) + out).astype(BF16)


def solution(mesh):
    return jax.shard_map(
        body,
        mesh=mesh,
        in_specs=(
            P(("grp", "sp"), "tp"),
            P(("grp", "sp"), None),
            P(("grp", "sp"), None),
            P(),
            P(),
            P(("grp", "sp", "tp"), None),
            P("tp", None),
            P(),
            P(),
            P("sp", "tp"),
            P("sp", "tp"),
            P(None, "tp"),
            P(None, "tp"),
            P("sp", "tp"),
        ),
        out_specs=P(("grp", "sp", "tp"), None),
        check_vma=False,
    )
```

```python
import functools
import numpy as np
import jax
import jax.numpy as jnp
from jax import lax
from jax.experimental import pallas as pl
from jax.experimental.pallas import tpu as pltpu
from jax.sharding import PartitionSpec as P

HEADS = 8
KVH = 2
GRID_W = 64
EPSILON = 1e-06
THETA = 10000.0
F32 = jnp.float32
BF16 = jnp.bfloat16
NT = (((1,), (1,)), ((), ()))


def rotary_parts(seq_total, head_dim):
    quarter = head_dim // 4
    inverse = THETA ** (-(2.0 * np.arange(quarter, dtype=np.float32)) / np.float32(head_dim // 2))
    inverse = inverse.astype(np.float32)
    rows = seq_total // GRID_W
    row_angle = (np.arange(rows) - rows // 2).astype(np.float32)[:, None] * inverse
    col_angle = (np.arange(GRID_W) - GRID_W // 2).astype(np.float32)[:, None] * inverse

    def lanes(angle, first):
        zero = np.zeros_like(angle)
        cos, sin = np.cos(angle.astype(np.float64)), np.sin(angle.astype(np.float64))
        cos, sin = [cos, cos], [-sin, sin]
        pad = [zero, zero]
        parts = (cos + pad if first else pad + cos) + (sin + pad if first else pad + sin)
        return np.concatenate(parts, axis=-1).astype(np.float32)

    return lanes(row_angle, True), lanes(col_angle, False)


def turned(raw, gain, cos, sin, factor):
    x = raw.astype(F32)
    head_dim = x.shape[-1]
    quarter = head_dim // 4
    normed = x * lax.rsqrt(jnp.mean(x * x, axis=-1, keepdims=True) + EPSILON) * gain
    lane = lax.broadcasted_iota(jnp.int32, x.shape, 1)
    other = jnp.where(
        (lane & quarter) == 0,
        pltpu.roll(normed, head_dim - quarter, 1),
        pltpu.roll(normed, quarter, 1),
    )
    return ((normed * cos + other * sin) * factor).astype(BF16)


def key_kernel(at_ref, k_ref, v_ref, gain_ref, row_ref, col_ref, out_ref):
    part, hd = k_ref.shape
    count = part // GRID_W
    for i in range(count):
        rows = pl.ds(i * GRID_W, GRID_W)
        table = row_ref[0, pl.ds(at_ref[0] * count + i, 1), :] + col_ref[...]
        out_ref[rows, :] = turned(k_ref[rows, :], gain_ref[...], table[:, :hd], table[:, hd:], 1.0)
    out_ref[pl.ds(part, part), :] = v_ref[...]


def query_kernel(at_ref, raw_ref, gain_ref, row_ref, col_ref, out_ref):
    hd = raw_ref.shape[1]
    for i in range(raw_ref.shape[0] // GRID_W):
        table = row_ref[0, pl.ds(i, 1), :] + col_ref[...]
        rows = pl.ds(i * GRID_W, GRID_W)
        out_ref[rows, :] = turned(
            raw_ref[rows, :], gain_ref[...], table[:, :hd], table[:, hd:], hd ** (-0.5)
        )


def as_row(col, eye):
    return jnp.sum(jnp.where(eye, col, 0.0), axis=0, keepdims=True)


def as_col(row, eye):
    return jnp.sum(jnp.where(eye, row, 0.0), axis=1, keepdims=True)


def square_eye(n):
    return lax.broadcasted_iota(jnp.int32, (n, n), 0) == lax.broadcasted_iota(jnp.int32, (n, n), 1)


def stats_rows(col, eye, tail):
    hd = eye.shape[0]
    rows = [as_row(col[b * hd : (b + 1) * hd], eye) for b in range(col.shape[0] // hd)]
    left = jnp.concatenate(rows + [jnp.zeros((8 - len(rows), hd), F32)], axis=0)
    high = left.astype(BF16).astype(F32)
    left = left - high
    mid = left.astype(BF16).astype(F32)
    return jnp.concatenate([high, mid, left - mid, jnp.zeros((tail - 24, hd), F32)], axis=0).astype(BF16)


def stats_col(block, eye, count):
    block = block.astype(F32)
    block = block[0:8] + block[8:16] + block[16:24]
    return jnp.concatenate([as_col(block[b : b + 1], eye) for b in range(count)], axis=0)


def attend_kernel(shards, heads, own, at_ref, *refs):
    q_in, refs = refs[:heads], refs[heads:]
    kv, refs = refs[:shards], refs[shards:]
    outs, (q_ref, sem) = refs[:2], refs[2:]
    core, slot0 = at_ref[3], at_ref[0]
    step = pl.program_id(0)
    hd = q_ref.shape[2]
    rows = heads * own
    part = kv[0].shape[0] // 2

    @pl.when(step == 0)
    def _():
        copies = []
        for k in range(heads):
            copies.append(pltpu.make_async_copy(q_in[k], q_ref.at[slot0 ^ k], sem.at[k]))
        for c in copies:
            c.start()
        for c in copies:
            c.wait()

    keys = jnp.concatenate([r[pl.ds(0, part), :] for r in kv], axis=0)
    vals = jnp.concatenate([r[pl.ds(part, part), :] for r in kv], axis=0)
    eye = square_eye(hd)
    tail = outs[0].shape[1] - rows
    todo = [(p, h) for p in range(2) for h in range(0, heads, 2)]

    def score(p, h):
        start = pl.multiple_of((2 * step + (core ^ p)) * own, 32)
        q = jnp.concatenate([q_ref[h + i, pl.ds(start, own), :] for i in range(2)], axis=0)
        return lax.dot_general(q, keys, NT, preferred_element_type=F32)

    lse = [[], []]
    ahead = score(*todo[0])
    for i, (p, h) in enumerate(todo):
        s = ahead
        if i + 1 < len(todo):
            ahead = score(*todo[i + 1])
        m = jnp.max(s, axis=1, keepdims=True)
        e = jnp.exp(s - m)
        den = jnp.sum(e, axis=1, keepdims=True)
        acc = jnp.dot(e.astype(BF16), vals, preferred_element_type=F32)
        outs[p][0, pl.ds(h * own, 2 * own), :] = (acc / den).astype(BF16)
        lse[p].append(m + jnp.log(den))
    for p in range(2):
        outs[p][0, pl.ds(rows, tail), :] = stats_rows(jnp.concatenate(lse[p], axis=0), eye, tail)


def merge_kernel(rows, a_ref, b_ref, *out_refs):
    hd = a_ref.shape[2]
    tail = a_ref.shape[1] - rows
    eye = square_eye(hd)
    for k, out_ref in enumerate(out_refs):
        la = stats_col(a_ref[k, pl.ds(rows, tail), :], eye, rows // hd)
        lb = stats_col(b_ref[k, pl.ds(rows, tail), :], eye, rows // hd)
        top = jnp.maximum(la, lb)
        wa, wb = jnp.exp(la - top), jnp.exp(lb - top)
        total = wa + wb
        a = a_ref[k, pl.ds(0, rows), :].astype(F32)
        b = b_ref[k, pl.ds(0, rows), :].astype(F32)
        out_ref[pl.ds(0, rows), :] = (a * (wa / total) + b * (wb / total)).astype(BF16)
        out_ref[pl.ds(rows, tail), :] = stats_rows(top + jnp.log(total), eye, tail)


def normalised(x, gain):
    return x * lax.rsqrt(jnp.mean(x * x, axis=-1, keepdims=True) + EPSILON) * gain


def mix_kernel(group, chips, pieces, at_ref, res_ref, mg_ref, fg_ref, *refs):
    seen, refs = refs[:chips], refs[chips:]
    parts, refs = refs[:pieces], refs[pieces:]
    stream_ref, normed_ref, in_ref, att_ref, w_ref, sem_in, sem = refs
    arrive = []
    for i, one in enumerate(seen):
        arrive.append(pltpu.make_async_copy(one, in_ref.at[at_ref[pieces + i]], sem_in.at[i]))
    copies = []
    for i, part in enumerate(parts):
        size = part.shape[0]
        start = pl.multiple_of(at_ref[i], size)
        copies.append(pltpu.make_async_copy(part, w_ref.at[pl.ds(start, size), :], sem.at[i]))
    for c in arrive + copies:
        c.start()
    for c in arrive:
        c.wait()
    hd = in_ref.shape[2]
    toks = res_ref.shape[0]
    rows = group * toks
    tail = in_ref.shape[1] - rows
    splits = chips // KVH
    eye = square_eye(hd)
    for kv in range(KVH):
        cols = [stats_col(in_ref[kv * splits + j, pl.ds(rows, tail), :], eye, rows // hd) for j in range(splits)]
        top = functools.reduce(jnp.maximum, cols)
        w = [jnp.exp(x - top) for x in cols]
        total = functools.reduce(jnp.add, w)
        acc = None
        for j in range(splits):
            term = (w[j] / total) * in_ref[kv * splits + j, pl.ds(0, rows), :].astype(F32)
            acc = term if acc is None else acc + term
        acc = acc.astype(BF16)
        for h in range(group):
            c = (kv * group + h) * hd
            att_ref[:, c : c + hd] = acc[h * toks : (h + 1) * toks]
    for c in copies:
        c.wait()
    mix = jnp.dot(att_ref[...], w_ref[...], preferred_element_type=F32)
    stream = (res_ref[...].astype(F32) + normalised(mix, mg_ref[...])).astype(BF16)
    stream_ref[...] = stream
    normed_ref[...] = normalised(stream.astype(F32), fg_ref[...]).astype(BF16)


def gelu(v):
    return 0.5 * v * (1.0 + jnp.tanh(0.7978845608028654 * (v + 0.044715 * v * v * v)))


def ffn_kernel(pieces, at_ref, halo_ref, taps_ref, all_ref, *refs):
    toks_in, refs = refs[:pieces], refs[pieces:]
    keep_ref, send_ref, x_ref, g_ref, v_ref, d_ref, even_ref, odd_ref, h_ref, p_ref = refs[:10]
    sem_x, sem_g, sem_v, sem_d, sem_o = refs[10:]
    main = x_ref.shape[0] - halo_ref.shape[0]
    units = d_ref.shape[1]
    shards = d_ref.shape[0]
    block = taps_ref.shape[2] // 2
    blocks = taps_ref.shape[0]

    def token_copy(i):
        size = toks_in[i].shape[0]
        start = pl.multiple_of(at_ref[i], 16)
        return pltpu.make_async_copy(toks_in[i], x_ref.at[pl.ds(start, size), :], sem_x.at[i])

    def rows_copy(b, base, ref, sem):
        start = pl.multiple_of(b * block, block)
        return pltpu.make_async_copy(
            all_ref.at[:, pl.ds(base + start, block), :], ref.at[:, pl.ds(start, block), :], sem.at[b]
        )

    def gate_copy(b):
        return rows_copy(b, 0, g_ref, sem_g)

    def value_copy(b):
        return rows_copy(b, units, v_ref, sem_v)

    down = pltpu.make_async_copy(all_ref.at[:, pl.ds(2 * units, units), :], d_ref, sem_d)
    for i in range(pieces):
        token_copy(i).start()
    for b in range(blocks):
        gate_copy(b).start()
        value_copy(b).start()
    down.start()
    x_ref[pl.ds(main, halo_ref.shape[0]), :] = halo_ref[...]
    for i in range(pieces):
        token_copy(i).wait()

    def arrive(b):
        gate_copy(b).wait()
        value_copy(b).wait()

    def up(b, out_ref):
        rows = pl.ds(b * block, block)
        w = [
            jnp.concatenate([ref[s, rows, :] for s in range(shards)], axis=1) for ref in (g_ref, v_ref)
        ]
        w = jnp.concatenate(w, axis=0)
        y = lax.dot_general(x_ref[...], w, NT, preferred_element_type=F32)
        out_ref[...] = y.astype(BF16).astype(F32)

    def finish(b, in_ref):
        now = in_ref[pl.ds(0, main), :]
        row = lax.broadcasted_iota(jnp.int32, now.shape, 0)
        before = jnp.where(row == 0, in_ref[main : main + 1, :], pltpu.roll(now, 1, 0))
        after = jnp.where(row == main - 1, in_ref[main + 1 : main + 2, :], pltpu.roll(now, main - 1, 0))
        taps = taps_ref[b]
        mixed = taps[0:1] * before + taps[1:2] * now + taps[2:3] * after
        h_ref[:, pl.ds(b * block, block)] = (gelu(mixed[:, :block]) * mixed[:, block:]).astype(BF16)

    arrive(0)
    up(0, even_ref)

    def pair(i, unused):
        b = pl.multiple_of(2 * i, 2)
        arrive(b + 1)
        arrive(b + 2)
        up(b + 1, odd_ref)
        finish(b, even_ref)
        up(b + 2, even_ref)
        finish(b + 1, odd_ref)
        return unused

    lax.fori_loop(0, blocks // 2 - 1, pair, 0)
    arrive(blocks - 1)
    up(blocks - 1, odd_ref)
    finish(blocks - 2, even_ref)
    finish(blocks - 1, odd_ref)
    down.wait()

    def down_block(n, unused):
        w = jnp.concatenate([d_ref[2 * n], d_ref[2 * n + 1]], axis=1)
        y = jnp.dot(h_ref[:, :units], w, preferred_element_type=F32)
        p_ref[:, pl.ds(pl.multiple_of(n * 256, 256), 256)] = y.astype(BF16)
        return unused

    lax.fori_loop(0, shards // 2, down_block, 0)
    count, own = keep_ref.shape[0], keep_ref.shape[1]
    outs = []
    for k in range(count):
        for o, ref in enumerate((keep_ref, send_ref)):
            start = pl.multiple_of(at_ref[pieces + 2 * k + o], 16)
            outs.append(
                pltpu.make_async_copy(p_ref.at[pl.ds(start, own), :], ref.at[k], sem_o.at[2 * k + o])
            )
    for c in outs:
        c.start()
    for c in outs:
        c.wait()


def vmem(limit=56 << 20):
    return pltpu.CompilerParams(vmem_limit_bytes=limit)


def body(
    queries,
    keys,
    values,
    query_gain,
    key_gain,
    residual,
    out_weight,
    mix_gain,
    ffn_gain,
    gate_in,
    value_in,
    conv_gate,
    conv_value,
    down_t,
):
    tok = queries.shape[0]
    hd = query_gain.shape[0]
    n_sp, n_tp = lax.axis_size("sp"), lax.axis_size("tp")
    n_x = n_tp // 2
    group = HEADS // KVH
    splits = n_tp // KVH
    part = tok // splits
    own = tok // n_tp
    model = residual.shape[1]
    units = gate_in.shape[1]
    tp, sp = lax.axis_index("tp"), lax.axis_index("sp")
    kv_head, piece = tp // splits, tp % splits
    x, core = tp // 2, tp % 2

    def send(array, change):
        return lax.ppermute(array, "tp", [(i, change(i)) for i in range(n_tp)])

    def other_core(array):
        return send(array, lambda i: i ^ 1)

    def up_x(array):
        return send(array, lambda i: (i + 2) % n_tp)

    def down_x(array):
        return send(array, lambda i: (i - 2) % n_tp)

    def far_x(array):
        return send(array, lambda i: (i + n_x) % n_tp)

    def gathered(mine, direct=False):
        size = mine.shape[0]
        half = size // 2
        a = up_x(mine)
        b = down_x(mine)
        near = other_core(mine)
        if direct:
            pieces = [(mine, tp), (near, tp ^ 1)]
            far = far_x(mine)
            for array, shift in ((a, n_x - 1), (b, 1), (far, n_x // 2)):
                base = ((x + shift) % n_x) * 2
                across = other_core(array)
                pieces += [(array, base + core), (across, base + 1 - core)]
            return [p[0] for p in pieces], [p[1] * size for p in pieces]
        c = up_x(a[:half])
        d = down_x(b[half:])
        low, high = ((x + n_x - 1) % n_x) * 2, ((x + 1) % n_x) * 2
        far = (tp + n_x) % n_tp
        found = [(mine, tp * size), (near, (tp ^ 1) * size)]
        for array, base in ((a, low), (b, high)):
            found.append((array, (base + core) * size))
            found.append((other_core(array), (base + 1 - core) * size))
        for array, shift in ((c, 0), (d, half)):
            found.append((array, far * size + shift))
            found.append((other_core(array), (far ^ 1) * size + shift))
        return [f[0] for f in found], [f[1] for f in found]

    row_np, col_np = rotary_parts(tok * n_sp, hd)
    row_np = row_np.reshape(n_sp, tok // GRID_W, 2 * hd)
    rows_all, cols_all = jnp.asarray(row_np), jnp.asarray(col_np)
    at = jnp.stack([piece, kv_head, sp, core, x]).astype(jnp.int32)
    packed_rows = 2 * part
    packed = pl.pallas_call(
        key_kernel,
        out_shape=jax.ShapeDtypeStruct((packed_rows, hd), BF16),
        grid_spec=pltpu.PrefetchScalarGridSpec(
            num_scalar_prefetch=1,
            grid=(1,),
            in_specs=[
                pl.BlockSpec((part, hd), lambda i, a: (a[0], a[1])),
                pl.BlockSpec((part, hd), lambda i, a: (a[0], a[1])),
                pl.BlockSpec((1, hd), lambda i, a: (0, 0)),
                pl.BlockSpec((1,) + row_np.shape[1:], lambda i, a: (a[2], 0, 0)),
                pl.BlockSpec(col_np.shape, lambda i, a: (0, 0)),
            ],
            out_specs=pl.BlockSpec((packed_rows, hd), lambda i, a: (0, 0)),
        ),
        name="key_prep",
    )(at, keys, values, key_gain[None], rows_all, cols_all)
    weights = jnp.concatenate([gate_in.T, value_in.T, down_t.T], axis=0)
    gate_rows = lax.all_gather(weights, "sp", axis=0, tiled=False)

    mine = pl.pallas_call(
        query_kernel,
        out_shape=jax.ShapeDtypeStruct((tok, hd), BF16),
        grid_spec=pltpu.PrefetchScalarGridSpec(
            num_scalar_prefetch=1,
            grid=(1,),
            in_specs=[
                pl.BlockSpec((tok, hd), lambda i, a: (0, 0)),
                pl.BlockSpec((1, hd), lambda i, a: (0, 0)),
                pl.BlockSpec((1,) + row_np.shape[1:], lambda i, a: (a[2], 0, 0)),
                pl.BlockSpec(col_np.shape, lambda i, a: (0, 0)),
            ],
            out_specs=pl.BlockSpec((tok, hd), lambda i, a: (0, 0)),
        ),
        name="query_prep",
    )(at, queries, query_gain[None], rows_all, cols_all)
    pair = send(mine, lambda i: i ^ 2)
    turned_q = [mine, other_core(mine), pair, other_core(pair)]
    rows = group * own

    out_pieces, out_at = gathered(out_weight, direct=True)

    packed, queries, out_weight = lax.optimization_barrier((packed, queries, out_weight))
    right = [(i, (i + 1) % n_sp) for i in range(n_sp)]
    left = [(i, (i - 1) % n_sp) for i in range(n_sp)]
    tail = 32
    shards = [packed]
    a = b = packed
    for s in range(1, n_sp // 2 + 1):
        a = lax.ppermute(a, "sp", right)
        shards.append(a)
        if len(shards) < n_sp:
            b = lax.ppermute(b, "sp", left)
            shards.append(b)
        if s == n_sp // 4:
            a, b, *turned_q = lax.optimization_barrier((a, b, *turned_q))
    a, *out_pieces = lax.optimization_barrier((a, *out_pieces))
    anywhere = pl.BlockSpec(memory_space=pl.ANY)
    keep, away = pl.pallas_call(
        functools.partial(attend_kernel, n_sp, group, own),
        out_shape=[jax.ShapeDtypeStruct((n_x, rows + tail, hd), BF16)] * 2,
        grid_spec=pltpu.PrefetchScalarGridSpec(
            num_scalar_prefetch=1,
            grid=(n_x,),
            in_specs=[anywhere] * group + [pl.BlockSpec((2 * part, hd), lambda i, a: (0, 0))] * n_sp,
            out_specs=[pl.BlockSpec((1, rows + tail, hd), lambda i, a: (lax.rem(i + n_x - a[4], n_x), 0, 0))] * 2,
            scratch_shapes=[pltpu.VMEM((group, tok, hd), BF16), pltpu.SemaphoreType.DMA((group,))],
        ),
        compiler_params=vmem(),
        cost_estimate=pl.CostEstimate(
            flops=8 * group * tok * part * n_sp * hd,
            bytes_accessed=8 << 20,
            transcendentals=group * tok * part * n_sp,
        ),
        name="attend",
    )(at, *turned_q, *shards[:-1], a)
    merged = pl.pallas_call(
        functools.partial(merge_kernel, rows),
        out_shape=[jax.ShapeDtypeStruct((rows + tail, hd), BF16)] * n_x,
        compiler_params=vmem(),
        name="merge",
    )(keep, other_core(away))
    seen = [merged[0], up_x(merged[1]), far_x(merged[2]), down_x(merged[3])]
    seen_at = [(x + n_x - k) % n_x for k in range(n_x)]
    whole = pl.BlockSpec(memory_space=pltpu.VMEM)
    stream, normed = pl.pallas_call(
        functools.partial(mix_kernel, group, n_x, len(out_pieces)),
        out_shape=[jax.ShapeDtypeStruct((own, model), BF16)] * 2,
        in_specs=[pl.BlockSpec(memory_space=pltpu.SMEM)] + [whole] * 3 + [anywhere] * (n_x + len(out_pieces)),
        scratch_shapes=[
            pltpu.VMEM((n_x, rows + tail, hd), BF16),
            pltpu.VMEM((own, HEADS * hd), BF16),
            pltpu.VMEM((HEADS * hd, model), BF16),
            pltpu.SemaphoreType.DMA((n_x,)),
            pltpu.SemaphoreType.DMA((len(out_pieces),)),
        ],
        compiler_params=vmem(),
        cost_estimate=pl.CostEstimate(
            flops=2 * own * HEADS * hd * model, bytes_accessed=6 << 20, transcendentals=0
        ),
        name="mix",
    )(
        jnp.stack(out_at + seen_at).astype(jnp.int32),
        residual,
        mix_gain[None],
        ffn_gain[None],
        *seen,
        *out_pieces,
    )

    token_pieces, token_at = gathered(normed)
    first = last_row = None
    for p, r in zip(token_pieces, token_at):
        f = jnp.where(r == 0, p[:1], 0)
        e = jnp.where(r + p.shape[0] == tok, p[-1:], 0)
        first = f if first is None else first + f
        last_row = e if last_row is None else last_row + e
    before = lax.ppermute(last_row, "sp", [(i, i + 1) for i in range(n_sp - 1)])
    after = lax.ppermute(first, "sp", [(i + 1, i) for i in range(n_sp - 1)])
    halo = jnp.concatenate([before, after, jnp.zeros((14, model), BF16)], axis=0)
    block = 128
    blocks = -(-units // block)

    def by_block(taps):
        wide = jnp.pad(taps, ((0, 5), (0, blocks * block - units)))
        return jnp.transpose(wide.reshape(8, blocks, block), (1, 0, 2))

    taps = jnp.concatenate([by_block(conv_gate), by_block(conv_value)], axis=2)
    slots = []
    for k in range(n_x):
        to = ((x + k) % n_x) * 2
        slots += [(to + core) * own, (to + 1 - core) * own]
    where = jnp.stack(token_at + slots).astype(jnp.int32)
    keep, away = pl.pallas_call(
        functools.partial(ffn_kernel, len(token_pieces)),
        out_shape=[jax.ShapeDtypeStruct((n_x, own, model), BF16)] * 2,
        in_specs=[pl.BlockSpec(memory_space=pltpu.SMEM), whole, whole]
        + [anywhere] * (1 + len(token_pieces)),
        out_specs=[anywhere, anywhere],
        scratch_shapes=[
            pltpu.VMEM((tok + 16, model), BF16),
            pltpu.VMEM((n_sp, blocks * block, hd), BF16),
            pltpu.VMEM((n_sp, blocks * block, hd), BF16),
            pltpu.VMEM((n_sp, units, hd), BF16),
            pltpu.VMEM((tok + 16, 2 * block), F32),
            pltpu.VMEM((tok + 16, 2 * block), F32),
            pltpu.VMEM((tok, blocks * block), BF16),
            pltpu.VMEM((tok, model), BF16),
            pltpu.SemaphoreType.DMA((len(token_pieces),)),
            pltpu.SemaphoreType.DMA((blocks,)),
            pltpu.SemaphoreType.DMA((blocks,)),
            pltpu.SemaphoreType.DMA,
            pltpu.SemaphoreType.DMA((2 * n_x,)),
        ],
        compiler_params=vmem(),
        cost_estimate=pl.CostEstimate(
            flops=6 * tok * units * model, bytes_accessed=16 << 20, transcendentals=tok * units
        ),
        name="ffn",
    )(where, halo, taps, gate_rows, *token_pieces)
    near = other_core(away)
    total = [keep[k].astype(F32) + near[k].astype(F32) for k in range(n_x)]
    one = up_x(total[1].astype(BF16))
    two = far_x(total[2].astype(BF16))
    three = down_x(total[3].astype(BF16))
    out = total[0] + one.astype(F32) + two.astype(F32) + three.astype(F32)
    return (stream.astype(F32) + out).astype(BF16)


def solution(mesh):
    return jax.shard_map(
        body,
        mesh=mesh,
        in_specs=(
            P(("grp", "sp"), "tp"),
            P(("grp", "sp"), None),
            P(("grp", "sp"), None),
            P(),
            P(),
            P(("grp", "sp", "tp"), None),
            P("tp", None),
            P(),
            P(),
            P("sp", "tp"),
            P("sp", "tp"),
            P(None, "tp"),
            P(None, "tp"),
            P("sp", "tp"),
        ),
        out_specs=P(("grp", "sp", "tp"), None),
        check_vma=False,
    )
```

```python
import functools
import numpy as np
import jax
import jax.numpy as jnp
from jax import lax
from jax.experimental import pallas as pl
from jax.experimental.pallas import tpu as pltpu
from jax.sharding import PartitionSpec as P

HEADS = 8
KVH = 2
GRID_W = 64
EPSILON = 1e-06
THETA = 10000.0
F32 = jnp.float32
BF16 = jnp.bfloat16
NT = (((1,), (1,)), ((), ()))


def rotary_parts(seq_total, head_dim):
    quarter = head_dim // 4
    inverse = THETA ** (-(2.0 * np.arange(quarter, dtype=np.float32)) / np.float32(head_dim // 2))
    inverse = inverse.astype(np.float32)
    rows = seq_total // GRID_W
    row_angle = (np.arange(rows) - rows // 2).astype(np.float32)[:, None] * inverse
    col_angle = (np.arange(GRID_W) - GRID_W // 2).astype(np.float32)[:, None] * inverse

    def lanes(angle, first):
        zero = np.zeros_like(angle)
        cos, sin = np.cos(angle.astype(np.float64)), np.sin(angle.astype(np.float64))
        cos, sin = [cos, cos], [-sin, sin]
        pad = [zero, zero]
        parts = (cos + pad if first else pad + cos) + (sin + pad if first else pad + sin)
        return np.concatenate(parts, axis=-1).astype(np.float32)

    return lanes(row_angle, True), lanes(col_angle, False)


def turned(raw, gain, cos, sin, factor):
    x = raw.astype(F32)
    head_dim = x.shape[-1]
    quarter = head_dim // 4
    normed = x * lax.rsqrt(jnp.mean(x * x, axis=-1, keepdims=True) + EPSILON) * gain
    lane = lax.broadcasted_iota(jnp.int32, x.shape, 1)
    other = jnp.where(
        (lane & quarter) == 0,
        pltpu.roll(normed, head_dim - quarter, 1),
        pltpu.roll(normed, quarter, 1),
    )
    return ((normed * cos + other * sin) * factor).astype(BF16)


def key_kernel(at_ref, k_ref, v_ref, gain_ref, row_ref, col_ref, out_ref):
    part, hd = k_ref.shape
    count = part // GRID_W
    for i in range(count):
        rows = pl.ds(i * GRID_W, GRID_W)
        table = row_ref[0, pl.ds(at_ref[0] * count + i, 1), :] + col_ref[...]
        out_ref[rows, :] = turned(k_ref[rows, :], gain_ref[...], table[:, :hd], table[:, hd:], 1.0)
    out_ref[pl.ds(part, part), :] = v_ref[...]


def query_kernel(at_ref, raw_ref, gain_ref, row_ref, col_ref, out_ref):
    hd = raw_ref.shape[1]
    for i in range(raw_ref.shape[0] // GRID_W):
        table = row_ref[0, pl.ds(i, 1), :] + col_ref[...]
        rows = pl.ds(i * GRID_W, GRID_W)
        out_ref[rows, :] = turned(
            raw_ref[rows, :], gain_ref[...], table[:, :hd], table[:, hd:], hd ** (-0.5)
        )


def as_row(col, eye):
    return jnp.sum(jnp.where(eye, col, 0.0), axis=0, keepdims=True)


def as_col(row, eye):
    return jnp.sum(jnp.where(eye, row, 0.0), axis=1, keepdims=True)


def square_eye(n):
    return lax.broadcasted_iota(jnp.int32, (n, n), 0) == lax.broadcasted_iota(jnp.int32, (n, n), 1)


def stats_rows(col, eye, tail):
    hd = eye.shape[0]
    rows = [as_row(col[b * hd : (b + 1) * hd], eye) for b in range(col.shape[0] // hd)]
    left = jnp.concatenate(rows + [jnp.zeros((8 - len(rows), hd), F32)], axis=0)
    high = left.astype(BF16).astype(F32)
    left = left - high
    mid = left.astype(BF16).astype(F32)
    return jnp.concatenate([high, mid, left - mid, jnp.zeros((tail - 24, hd), F32)], axis=0).astype(BF16)


def stats_col(block, eye, count):
    block = block.astype(F32)
    block = block[0:8] + block[8:16] + block[16:24]
    return jnp.concatenate([as_col(block[b : b + 1], eye) for b in range(count)], axis=0)


def attend_kernel(shards, heads, own, at_ref, *refs):
    q_in, refs = refs[:heads], refs[heads:]
    kv, refs = refs[:shards], refs[shards:]
    outs, (q_ref, sem) = refs[:2], refs[2:]
    core, slot0 = at_ref[3], at_ref[0]
    step = pl.program_id(0)
    hd = q_ref.shape[2]
    rows = heads * own
    part = kv[0].shape[0] // 2

    @pl.when(step == 0)
    def _():
        copies = []
        for k in range(heads):
            copies.append(pltpu.make_async_copy(q_in[k], q_ref.at[slot0 ^ k], sem.at[k]))
        for c in copies:
            c.start()
        for c in copies:
            c.wait()

    keys = jnp.concatenate([r[pl.ds(0, part), :] for r in kv], axis=0)
    vals = jnp.concatenate([r[pl.ds(part, part), :] for r in kv], axis=0)
    eye = square_eye(hd)
    tail = outs[0].shape[1] - rows
    todo = [(p, h) for p in range(2) for h in range(0, heads, 2)]

    def score(p, h):
        start = pl.multiple_of((2 * step + (core ^ p)) * own, 32)
        q = jnp.concatenate([q_ref[h + i, pl.ds(start, own), :] for i in range(2)], axis=0)
        return lax.dot_general(q, keys, NT, preferred_element_type=F32)

    lse = [[], []]
    ahead = score(*todo[0])
    for i, (p, h) in enumerate(todo):
        s = ahead
        if i + 1 < len(todo):
            ahead = score(*todo[i + 1])
        m = jnp.max(s, axis=1, keepdims=True)
        e = jnp.exp(s - m)
        den = jnp.sum(e, axis=1, keepdims=True)
        acc = jnp.dot(e.astype(BF16), vals, preferred_element_type=F32)
        outs[p][0, pl.ds(h * own, 2 * own), :] = (acc / den).astype(BF16)
        lse[p].append(m + jnp.log(den))
    for p in range(2):
        outs[p][0, pl.ds(rows, tail), :] = stats_rows(jnp.concatenate(lse[p], axis=0), eye, tail)


def merge_kernel(rows, a_ref, b_ref, *out_refs):
    hd = a_ref.shape[2]
    tail = a_ref.shape[1] - rows
    eye = square_eye(hd)
    for k, out_ref in enumerate(out_refs):
        la = stats_col(a_ref[k, pl.ds(rows, tail), :], eye, rows // hd)
        lb = stats_col(b_ref[k, pl.ds(rows, tail), :], eye, rows // hd)
        top = jnp.maximum(la, lb)
        wa, wb = jnp.exp(la - top), jnp.exp(lb - top)
        total = wa + wb
        a = a_ref[k, pl.ds(0, rows), :].astype(F32)
        b = b_ref[k, pl.ds(0, rows), :].astype(F32)
        out_ref[pl.ds(0, rows), :] = (a * (wa / total) + b * (wb / total)).astype(BF16)
        out_ref[pl.ds(rows, tail), :] = stats_rows(top + jnp.log(total), eye, tail)


def normalised(x, gain):
    return x * lax.rsqrt(jnp.mean(x * x, axis=-1, keepdims=True) + EPSILON) * gain


def mix_kernel(group, chips, pieces, at_ref, res_ref, mg_ref, fg_ref, *refs):
    seen, refs = refs[:chips], refs[chips:]
    parts, refs = refs[:pieces], refs[pieces:]
    stream_ref, normed_ref, in_ref, att_ref, w_ref, sem_in, sem = refs
    arrive = []
    for i, one in enumerate(seen):
        arrive.append(pltpu.make_async_copy(one, in_ref.at[at_ref[pieces + i]], sem_in.at[i]))
    copies = []
    for i, part in enumerate(parts):
        size = part.shape[0]
        start = pl.multiple_of(at_ref[i], size)
        copies.append(pltpu.make_async_copy(part, w_ref.at[pl.ds(start, size), :], sem.at[i]))
    for c in arrive + copies:
        c.start()
    for c in arrive:
        c.wait()
    hd = in_ref.shape[2]
    toks = res_ref.shape[0]
    rows = group * toks
    tail = in_ref.shape[1] - rows
    splits = chips // KVH
    eye = square_eye(hd)
    for kv in range(KVH):
        cols = [stats_col(in_ref[kv * splits + j, pl.ds(rows, tail), :], eye, rows // hd) for j in range(splits)]
        top = functools.reduce(jnp.maximum, cols)
        w = [jnp.exp(x - top) for x in cols]
        total = functools.reduce(jnp.add, w)
        acc = None
        for j in range(splits):
            term = (w[j] / total) * in_ref[kv * splits + j, pl.ds(0, rows), :].astype(F32)
            acc = term if acc is None else acc + term
        acc = acc.astype(BF16)
        for h in range(group):
            c = (kv * group + h) * hd
            att_ref[:, c : c + hd] = acc[h * toks : (h + 1) * toks]
    for c in copies:
        c.wait()
    mix = jnp.dot(att_ref[...], w_ref[...], preferred_element_type=F32)
    stream = (res_ref[...].astype(F32) + normalised(mix, mg_ref[...])).astype(BF16)
    stream_ref[...] = stream
    normed_ref[...] = normalised(stream.astype(F32), fg_ref[...]).astype(BF16)


def gelu(v):
    return 0.5 * v * (1.0 + jnp.tanh(0.7978845608028654 * (v + 0.044715 * v * v * v)))


def ffn_kernel(pieces, at_ref, halo_ref, taps_ref, all_ref, *refs):
    toks_in, refs = refs[:pieces], refs[pieces:]
    keep_ref, send_ref, x_ref, g_ref, v_ref, d_ref, even_ref, odd_ref, h_ref, p_ref = refs[:10]
    sem_x, sem_g, sem_v, sem_d, sem_o = refs[10:]
    main = x_ref.shape[0] - halo_ref.shape[0]
    units = d_ref.shape[1]
    shards = d_ref.shape[0]
    block = taps_ref.shape[2] // 2
    blocks = taps_ref.shape[0]

    def token_copy(i):
        size = toks_in[i].shape[0]
        start = pl.multiple_of(at_ref[i], 16)
        return pltpu.make_async_copy(toks_in[i], x_ref.at[pl.ds(start, size), :], sem_x.at[i])

    def rows_copy(b, base, ref, sem):
        start = pl.multiple_of(b * block, block)
        return pltpu.make_async_copy(
            all_ref.at[:, pl.ds(base + start, block), :], ref.at[:, pl.ds(start, block), :], sem.at[b]
        )

    def gate_copy(b):
        return rows_copy(b, 0, g_ref, sem_g)

    def value_copy(b):
        return rows_copy(b, units, v_ref, sem_v)

    down = pltpu.make_async_copy(all_ref.at[:, pl.ds(2 * units, units), :], d_ref, sem_d)
    for i in range(pieces):
        token_copy(i).start()
    for b in range(blocks):
        gate_copy(b).start()
        value_copy(b).start()
    down.start()
    x_ref[pl.ds(main, halo_ref.shape[0]), :] = halo_ref[...]
    for i in range(pieces):
        token_copy(i).wait()

    def arrive(b):
        gate_copy(b).wait()
        value_copy(b).wait()

    def up(b, out_ref):
        rows = pl.ds(b * block, block)
        w = [
            jnp.concatenate([ref[s, rows, :] for s in range(shards)], axis=1) for ref in (g_ref, v_ref)
        ]
        w = jnp.concatenate(w, axis=0)
        y = lax.dot_general(x_ref[...], w, NT, preferred_element_type=F32)
        out_ref[...] = y.astype(BF16).astype(F32)

    def finish(b, in_ref):
        now = in_ref[pl.ds(0, main), :]
        row = lax.broadcasted_iota(jnp.int32, now.shape, 0)
        before = jnp.where(row == 0, in_ref[main : main + 1, :], pltpu.roll(now, 1, 0))
        after = jnp.where(row == main - 1, in_ref[main + 1 : main + 2, :], pltpu.roll(now, main - 1, 0))
        taps = taps_ref[b]
        mixed = taps[0:1] * before + taps[1:2] * now + taps[2:3] * after
        h_ref[:, pl.ds(b * block, block)] = (gelu(mixed[:, :block]) * mixed[:, block:]).astype(BF16)

    arrive(0)
    up(0, even_ref)

    def pair(i, unused):
        b = pl.multiple_of(2 * i, 2)
        arrive(b + 1)
        arrive(b + 2)
        up(b + 1, odd_ref)
        finish(b, even_ref)
        up(b + 2, even_ref)
        finish(b + 1, odd_ref)
        return unused

    lax.fori_loop(0, blocks // 2 - 1, pair, 0)
    arrive(blocks - 1)
    up(blocks - 1, odd_ref)
    finish(blocks - 2, even_ref)
    finish(blocks - 1, odd_ref)
    down.wait()

    def down_block(n, unused):
        w = jnp.concatenate([d_ref[2 * n], d_ref[2 * n + 1]], axis=1)
        y = jnp.dot(h_ref[:, :units], w, preferred_element_type=F32)
        p_ref[:, pl.ds(pl.multiple_of(n * 256, 256), 256)] = y.astype(BF16)
        return unused

    lax.fori_loop(0, shards // 2, down_block, 0)
    count, own = keep_ref.shape[0], keep_ref.shape[1]
    outs = []
    for k in range(count):
        for o, ref in enumerate((keep_ref, send_ref)):
            start = pl.multiple_of(at_ref[pieces + 2 * k + o], 16)
            outs.append(
                pltpu.make_async_copy(p_ref.at[pl.ds(start, own), :], ref.at[k], sem_o.at[2 * k + o])
            )
    for c in outs:
        c.start()
    for c in outs:
        c.wait()


def vmem(limit=56 << 20):
    return pltpu.CompilerParams(vmem_limit_bytes=limit)


def body(
    queries,
    keys,
    values,
    query_gain,
    key_gain,
    residual,
    out_weight,
    mix_gain,
    ffn_gain,
    gate_in,
    value_in,
    conv_gate,
    conv_value,
    down_t,
):
    tok = queries.shape[0]
    hd = query_gain.shape[0]
    n_sp, n_tp = lax.axis_size("sp"), lax.axis_size("tp")
    n_x = n_tp // 2
    group = HEADS // KVH
    splits = n_tp // KVH
    part = tok // splits
    own = tok // n_tp
    model = residual.shape[1]
    units = gate_in.shape[1]
    tp, sp = lax.axis_index("tp"), lax.axis_index("sp")
    kv_head, piece = tp // splits, tp % splits
    x, core = tp // 2, tp % 2

    def send(array, change):
        return lax.ppermute(array, "tp", [(i, change(i)) for i in range(n_tp)])

    def other_core(array):
        return send(array, lambda i: i ^ 1)

    def up_x(array):
        return send(array, lambda i: (i + 2) % n_tp)

    def down_x(array):
        return send(array, lambda i: (i - 2) % n_tp)

    def far_x(array):
        return send(array, lambda i: (i + n_x) % n_tp)

    def gathered(mine, direct=False):
        size = mine.shape[0]
        half = size // 2
        a = up_x(mine)
        b = down_x(mine)
        near = other_core(mine)
        if direct:
            pieces = [(mine, tp), (near, tp ^ 1)]
            far = far_x(mine)
            for array, shift in ((a, n_x - 1), (b, 1), (far, n_x // 2)):
                base = ((x + shift) % n_x) * 2
                across = other_core(array)
                pieces += [(array, base + core), (across, base + 1 - core)]
            return [p[0] for p in pieces], [p[1] * size for p in pieces]
        c = up_x(a[:half])
        d = down_x(b[half:])
        low, high = ((x + n_x - 1) % n_x) * 2, ((x + 1) % n_x) * 2
        far = (tp + n_x) % n_tp
        found = [(mine, tp * size), (near, (tp ^ 1) * size)]
        for array, base in ((a, low), (b, high)):
            across = other_core(array)
            found.append((array, (base + core) * size))
            found.append((across, (base + 1 - core) * size))
        for array, shift in ((c, 0), (d, half)):
            found.append((array, far * size + shift))
            found.append((other_core(array), (far ^ 1) * size + shift))
        return [f[0] for f in found], [f[1] for f in found]

    row_np, col_np = rotary_parts(tok * n_sp, hd)
    row_np = row_np.reshape(n_sp, tok // GRID_W, 2 * hd)
    rows_all, cols_all = jnp.asarray(row_np), jnp.asarray(col_np)
    at = jnp.stack([piece, kv_head, sp, core, x]).astype(jnp.int32)
    packed_rows = 2 * part
    packed = pl.pallas_call(
        key_kernel,
        out_shape=jax.ShapeDtypeStruct((packed_rows, hd), BF16),
        grid_spec=pltpu.PrefetchScalarGridSpec(
            num_scalar_prefetch=1,
            grid=(1,),
            in_specs=[
                pl.BlockSpec((part, hd), lambda i, a: (a[0], a[1])),
                pl.BlockSpec((part, hd), lambda i, a: (a[0], a[1])),
                pl.BlockSpec((1, hd), lambda i, a: (0, 0)),
                pl.BlockSpec((1,) + row_np.shape[1:], lambda i, a: (a[2], 0, 0)),
                pl.BlockSpec(col_np.shape, lambda i, a: (0, 0)),
            ],
            out_specs=pl.BlockSpec((packed_rows, hd), lambda i, a: (0, 0)),
        ),
        name="key_prep",
    )(at, keys, values, key_gain[None], rows_all, cols_all)
    weights = jnp.concatenate([gate_in.T, value_in.T, down_t.T], axis=0)
    gate_rows = lax.all_gather(weights, "sp", axis=0, tiled=False)

    mine = pl.pallas_call(
        query_kernel,
        out_shape=jax.ShapeDtypeStruct((tok, hd), BF16),
        grid_spec=pltpu.PrefetchScalarGridSpec(
            num_scalar_prefetch=1,
            grid=(1,),
            in_specs=[
                pl.BlockSpec((tok, hd), lambda i, a: (0, 0)),
                pl.BlockSpec((1, hd), lambda i, a: (0, 0)),
                pl.BlockSpec((1,) + row_np.shape[1:], lambda i, a: (a[2], 0, 0)),
                pl.BlockSpec(col_np.shape, lambda i, a: (0, 0)),
            ],
            out_specs=pl.BlockSpec((tok, hd), lambda i, a: (0, 0)),
        ),
        name="query_prep",
    )(at, queries, query_gain[None], rows_all, cols_all)
    pair = send(mine, lambda i: i ^ 2)
    turned_q = [mine, other_core(mine), pair, other_core(pair)]
    rows = group * own

    out_pieces, out_at = gathered(out_weight, direct=True)

    packed, queries, out_weight = lax.optimization_barrier((packed, queries, out_weight))
    right = [(i, (i + 1) % n_sp) for i in range(n_sp)]
    left = [(i, (i - 1) % n_sp) for i in range(n_sp)]
    tail = 32
    shards = [packed]
    a = b = packed
    for s in range(1, n_sp // 2 + 1):
        a = lax.ppermute(a, "sp", right)
        shards.append(a)
        if len(shards) < n_sp:
            b = lax.ppermute(b, "sp", left)
            shards.append(b)
        if s == n_sp // 4:
            a, b, *turned_q = lax.optimization_barrier((a, b, *turned_q))
    a, *out_pieces = lax.optimization_barrier((a, *out_pieces))
    anywhere = pl.BlockSpec(memory_space=pl.ANY)
    keep, away = pl.pallas_call(
        functools.partial(attend_kernel, n_sp, group, own),
        out_shape=[jax.ShapeDtypeStruct((n_x, rows + tail, hd), BF16)] * 2,
        grid_spec=pltpu.PrefetchScalarGridSpec(
            num_scalar_prefetch=1,
            grid=(n_x,),
            in_specs=[anywhere] * group + [pl.BlockSpec((2 * part, hd), lambda i, a: (0, 0))] * n_sp,
            out_specs=[pl.BlockSpec((1, rows + tail, hd), lambda i, a: (lax.rem(i + n_x - a[4], n_x), 0, 0))] * 2,
            scratch_shapes=[pltpu.VMEM((group, tok, hd), BF16), pltpu.SemaphoreType.DMA((group,))],
        ),
        compiler_params=vmem(36 << 20),
        cost_estimate=pl.CostEstimate(
            flops=8 * group * tok * part * n_sp * hd,
            bytes_accessed=8 << 20,
            transcendentals=group * tok * part * n_sp,
        ),
        name="attend",
    )(at, *turned_q, *shards[:-1], a)
    merged = pl.pallas_call(
        functools.partial(merge_kernel, rows),
        out_shape=[jax.ShapeDtypeStruct((rows + tail, hd), BF16)] * n_x,
        compiler_params=vmem(16 << 20),
        name="merge",
    )(keep, other_core(away))
    seen = [merged[0], up_x(merged[1]), far_x(merged[2]), down_x(merged[3])]
    seen_at = [(x + n_x - k) % n_x for k in range(n_x)]
    whole = pl.BlockSpec(memory_space=pltpu.VMEM)
    stream, normed = pl.pallas_call(
        functools.partial(mix_kernel, group, n_x, len(out_pieces)),
        out_shape=[jax.ShapeDtypeStruct((own, model), BF16)] * 2,
        in_specs=[pl.BlockSpec(memory_space=pltpu.SMEM)] + [whole] * 3 + [anywhere] * (n_x + len(out_pieces)),
        scratch_shapes=[
            pltpu.VMEM((n_x, rows + tail, hd), BF16),
            pltpu.VMEM((own, HEADS * hd), BF16),
            pltpu.VMEM((HEADS * hd, model), BF16),
            pltpu.SemaphoreType.DMA((n_x,)),
            pltpu.SemaphoreType.DMA((len(out_pieces),)),
        ],
        compiler_params=vmem(20 << 20),
        cost_estimate=pl.CostEstimate(
            flops=2 * own * HEADS * hd * model, bytes_accessed=6 << 20, transcendentals=0
        ),
        name="mix",
    )(
        jnp.stack(out_at + seen_at).astype(jnp.int32),
        residual,
        mix_gain[None],
        ffn_gain[None],
        *seen,
        *out_pieces,
    )

    token_pieces, token_at = gathered(normed)
    first = last_row = None
    for p, r in zip(token_pieces, token_at):
        f = jnp.where(r == 0, p[:1], 0)
        e = jnp.where(r + p.shape[0] == tok, p[-1:], 0)
        first = f if first is None else first + f
        last_row = e if last_row is None else last_row + e
    before = lax.ppermute(last_row, "sp", [(i, i + 1) for i in range(n_sp - 1)])
    after = lax.ppermute(first, "sp", [(i + 1, i) for i in range(n_sp - 1)])
    halo = jnp.concatenate([before, after, jnp.zeros((14, model), BF16)], axis=0)
    block = 128
    blocks = -(-units // block)

    def by_block(taps):
        wide = jnp.pad(taps, ((0, 5), (0, blocks * block - units)))
        return jnp.transpose(wide.reshape(8, blocks, block), (1, 0, 2))

    taps = jnp.concatenate([by_block(conv_gate), by_block(conv_value)], axis=2)
    slots = []
    for k in range(n_x):
        to = ((x + k) % n_x) * 2
        slots += [(to + core) * own, (to + 1 - core) * own]
    where = jnp.stack(token_at + slots).astype(jnp.int32)
    keep, away = pl.pallas_call(
        functools.partial(ffn_kernel, len(token_pieces)),
        out_shape=[jax.ShapeDtypeStruct((n_x, own, model), BF16)] * 2,
        in_specs=[pl.BlockSpec(memory_space=pltpu.SMEM), whole, whole, anywhere] + [anywhere] * len(token_pieces),
        out_specs=[anywhere, anywhere],
        scratch_shapes=[
            pltpu.VMEM((tok + 16, model), BF16),
            pltpu.VMEM((n_sp, blocks * block, hd), BF16),
            pltpu.VMEM((n_sp, blocks * block, hd), BF16),
            pltpu.VMEM((n_sp, units, hd), BF16),
            pltpu.VMEM((tok + 16, 2 * block), F32),
            pltpu.VMEM((tok + 16, 2 * block), F32),
            pltpu.VMEM((tok, blocks * block), BF16),
            pltpu.VMEM((tok, model), BF16),
            pltpu.SemaphoreType.DMA((len(token_pieces),)),
            pltpu.SemaphoreType.DMA((blocks,)),
            pltpu.SemaphoreType.DMA((blocks,)),
            pltpu.SemaphoreType.DMA,
            pltpu.SemaphoreType.DMA((2 * n_x,)),
        ],
        compiler_params=vmem(56 << 20),
        cost_estimate=pl.CostEstimate(
            flops=6 * tok * units * model, bytes_accessed=16 << 20, transcendentals=tok * units
        ),
        name="ffn",
    )(where, halo, taps, gate_rows, *token_pieces)
    near = other_core(away)
    total = [keep[k].astype(F32) + near[k].astype(F32) for k in range(n_x)]
    one = up_x(total[1].astype(BF16))
    two = far_x(total[2].astype(BF16))
    three = down_x(total[3].astype(BF16))
    out = total[0] + one.astype(F32) + two.astype(F32) + three.astype(F32)
    return (stream.astype(F32) + out).astype(BF16)


def solution(mesh):
    return jax.shard_map(
        body,
        mesh=mesh,
        in_specs=(
            P(("grp", "sp"), "tp"),
            P(("grp", "sp"), None),
            P(("grp", "sp"), None),
            P(),
            P(),
            P(("grp", "sp", "tp"), None),
            P("tp", None),
            P(),
            P(),
            P("sp", "tp"),
            P("sp", "tp"),
            P(None, "tp"),
            P(None, "tp"),
            P("sp", "tp"),
        ),
        out_specs=P(("grp", "sp", "tp"), None),
        check_vma=False,
    )
```

```python
import functools
import numpy as np
import jax
import jax.numpy as jnp
from jax import lax
from jax.experimental import pallas as pl
from jax.experimental.pallas import tpu as pltpu
from jax.sharding import PartitionSpec as P

HEADS = 8
KVH = 2
GRID_W = 64
EPSILON = 1e-06
THETA = 10000.0
F32 = jnp.float32
BF16 = jnp.bfloat16
NT = (((1,), (1,)), ((), ()))


def rotary_parts(seq_total, head_dim):
    quarter = head_dim // 4
    inverse = THETA ** (-(2.0 * np.arange(quarter, dtype=np.float32)) / np.float32(head_dim // 2))
    inverse = inverse.astype(np.float32)
    rows = seq_total // GRID_W
    row_angle = (np.arange(rows) - rows // 2).astype(np.float32)[:, None] * inverse
    col_angle = (np.arange(GRID_W) - GRID_W // 2).astype(np.float32)[:, None] * inverse

    def lanes(angle, first):
        zero = np.zeros_like(angle)
        cos, sin = np.cos(angle.astype(np.float64)), np.sin(angle.astype(np.float64))
        cos, sin = [cos, cos], [-sin, sin]
        pad = [zero, zero]
        parts = (cos + pad if first else pad + cos) + (sin + pad if first else pad + sin)
        return np.concatenate(parts, axis=-1).astype(np.float32)

    return lanes(row_angle, True), lanes(col_angle, False)


def turned(raw, gain, cos, sin, factor):
    x = raw.astype(F32)
    head_dim = x.shape[-1]
    quarter = head_dim // 4
    normed = x * lax.rsqrt(jnp.mean(x * x, axis=-1, keepdims=True) + EPSILON) * gain
    lane = lax.broadcasted_iota(jnp.int32, x.shape, 1)
    other = jnp.where(
        (lane & quarter) == 0,
        pltpu.roll(normed, head_dim - quarter, 1),
        pltpu.roll(normed, quarter, 1),
    )
    return ((normed * cos + other * sin) * factor).astype(BF16)


def key_kernel(at_ref, k_ref, v_ref, gain_ref, row_ref, col_ref, out_ref):
    part, hd = k_ref.shape
    count = part // GRID_W
    for i in range(count):
        rows = pl.ds(i * GRID_W, GRID_W)
        table = row_ref[0, pl.ds(at_ref[0] * count + i, 1), :] + col_ref[...]
        out_ref[rows, :] = turned(k_ref[rows, :], gain_ref[...], table[:, :hd], table[:, hd:], 1.0)
    out_ref[pl.ds(part, part), :] = v_ref[...]


def query_kernel(at_ref, raw_ref, gain_ref, row_ref, col_ref, out_ref):
    hd = raw_ref.shape[1]
    for i in range(raw_ref.shape[0] // GRID_W):
        table = row_ref[0, pl.ds(i, 1), :] + col_ref[...]
        rows = pl.ds(i * GRID_W, GRID_W)
        out_ref[rows, :] = turned(
            raw_ref[rows, :], gain_ref[...], table[:, :hd], table[:, hd:], hd ** (-0.5)
        )


def as_row(col, eye):
    return jnp.sum(jnp.where(eye, col, 0.0), axis=0, keepdims=True)


def as_col(row, eye):
    return jnp.sum(jnp.where(eye, row, 0.0), axis=1, keepdims=True)


def square_eye(n):
    return lax.broadcasted_iota(jnp.int32, (n, n), 0) == lax.broadcasted_iota(jnp.int32, (n, n), 1)


def stats_rows(col, eye, tail):
    hd = eye.shape[0]
    rows = [as_row(col[b * hd : (b + 1) * hd], eye) for b in range(col.shape[0] // hd)]
    left = jnp.concatenate(rows + [jnp.zeros((8 - len(rows), hd), F32)], axis=0)
    high = left.astype(BF16).astype(F32)
    left = left - high
    mid = left.astype(BF16).astype(F32)
    return jnp.concatenate([high, mid, left - mid, jnp.zeros((tail - 24, hd), F32)], axis=0).astype(BF16)


def stats_col(block, eye, count):
    block = block.astype(F32)
    block = block[0:8] + block[8:16] + block[16:24]
    return jnp.concatenate([as_col(block[b : b + 1], eye) for b in range(count)], axis=0)


def attend_kernel(shards, heads, own, base, last, at_ref, *refs):
    q_in, refs = refs[:heads], refs[heads:]
    kv, refs = refs[:shards], refs[shards:]
    if last:
        before, refs = refs[:2], refs[2:]
        outs, (q_ref, sem) = refs[:2], refs[2:]
    else:
        out_ref, q_ref, sem = refs
    core, slot0 = at_ref[3], at_ref[0]
    step = pl.program_id(0) + base
    hd = q_ref.shape[2]
    half = hd // 2
    rows = heads * own
    part = kv[0].shape[0] // 2

    @pl.when(pl.program_id(0) == 0)
    def _():
        copies = []
        for k in range(heads):
            copies.append(pltpu.make_async_copy(q_in[k], q_ref.at[slot0 ^ k], sem.at[k]))
        for c in copies:
            c.start()
        for c in copies:
            c.wait()

    keys = jnp.concatenate([r[pl.ds(0, part), :] for r in kv], axis=0)
    vals = jnp.concatenate([r[pl.ds(part, part), :] for r in kv], axis=0)
    eye = square_eye(hd)
    todo = [(p, h) for p in range(2) for h in range(0, heads, 2)]
    size = 2 * own

    def score(p, h):
        start = pl.multiple_of((2 * step + (core ^ p)) * own, 32)
        q = jnp.concatenate([q_ref[h + i, pl.ds(start, own), :] for i in range(2)], axis=0)
        return lax.dot_general(q, keys, NT, preferred_element_type=F32)

    lse = [[], []]
    ahead = score(*todo[0])
    for i, (p, h) in enumerate(todo):
        s = ahead
        if i + 1 < len(todo):
            ahead = score(*todo[i + 1])
        here = pl.ds(h * own, size)
        there = pl.ds(rows + h * own, size)
        m = jnp.max(s, axis=1, keepdims=True)
        if last:
            early = step < pl.num_programs(0) // 2
            stats = jnp.where(early, before[0][0, p, there, :], before[1][0, p, there, :])
            m_old, den_old = stats[:, 0:1], stats[:, half : half + 1]
            m = jnp.maximum(m, m_old)
        e = jnp.exp(s - m)
        den = jnp.sum(e, axis=1, keepdims=True)
        acc = jnp.dot(e.astype(BF16), vals, preferred_element_type=F32)
        if last:
            fade = jnp.exp(m_old - m)
            den = den + den_old * fade
            acc = acc + jnp.where(early, before[0][0, p, here, :], before[1][0, p, here, :]) * fade
            outs[p][0, here, :] = (acc / den).astype(BF16)
            lse[p].append(m + jnp.log(den))
        else:
            out_ref[0, p, here, :] = acc
            lane = lax.broadcasted_iota(jnp.int32, (size, hd), 1)
            out_ref[0, p, there, :] = jnp.where(lane < half, m, den)
    if last:
        tail = outs[0].shape[1] - rows
        for p in range(2):
            outs[p][0, pl.ds(rows, tail), :] = stats_rows(jnp.concatenate(lse[p], axis=0), eye, tail)


def merge_kernel(rows, a_ref, b_ref, *out_refs):
    hd = a_ref.shape[2]
    tail = a_ref.shape[1] - rows
    eye = square_eye(hd)
    for k, out_ref in enumerate(out_refs):
        la = stats_col(a_ref[k, pl.ds(rows, tail), :], eye, rows // hd)
        lb = stats_col(b_ref[k, pl.ds(rows, tail), :], eye, rows // hd)
        top = jnp.maximum(la, lb)
        wa, wb = jnp.exp(la - top), jnp.exp(lb - top)
        total = wa + wb
        a = a_ref[k, pl.ds(0, rows), :].astype(F32)
        b = b_ref[k, pl.ds(0, rows), :].astype(F32)
        out_ref[pl.ds(0, rows), :] = (a * (wa / total) + b * (wb / total)).astype(BF16)
        out_ref[pl.ds(rows, tail), :] = stats_rows(top + jnp.log(total), eye, tail)


def normalised(x, gain):
    return x * lax.rsqrt(jnp.mean(x * x, axis=-1, keepdims=True) + EPSILON) * gain


def mix_kernel(group, chips, pieces, at_ref, res_ref, mg_ref, fg_ref, *refs):
    seen, refs = refs[:chips], refs[chips:]
    parts, refs = refs[:pieces], refs[pieces:]
    stream_ref, normed_ref, in_ref, att_ref, w_ref, sem_in, sem = refs
    arrive = []
    for i, one in enumerate(seen):
        arrive.append(pltpu.make_async_copy(one, in_ref.at[at_ref[pieces + i]], sem_in.at[i]))
    copies = []
    for i, part in enumerate(parts):
        size = part.shape[0]
        start = pl.multiple_of(at_ref[i], size)
        copies.append(pltpu.make_async_copy(part, w_ref.at[pl.ds(start, size), :], sem.at[i]))
    for c in arrive + copies:
        c.start()
    for c in arrive:
        c.wait()
    hd = in_ref.shape[2]
    toks = res_ref.shape[0]
    rows = group * toks
    tail = in_ref.shape[1] - rows
    splits = chips // KVH
    eye = square_eye(hd)
    for kv in range(KVH):
        cols = [stats_col(in_ref[kv * splits + j, pl.ds(rows, tail), :], eye, rows // hd) for j in range(splits)]
        top = functools.reduce(jnp.maximum, cols)
        w = [jnp.exp(x - top) for x in cols]
        total = functools.reduce(jnp.add, w)
        acc = None
        for j in range(splits):
            term = (w[j] / total) * in_ref[kv * splits + j, pl.ds(0, rows), :].astype(F32)
            acc = term if acc is None else acc + term
        acc = acc.astype(BF16)
        for h in range(group):
            c = (kv * group + h) * hd
            att_ref[:, c : c + hd] = acc[h * toks : (h + 1) * toks]
    for c in copies:
        c.wait()
    mix = jnp.dot(att_ref[...], w_ref[...], preferred_element_type=F32)
    stream = (res_ref[...].astype(F32) + normalised(mix, mg_ref[...])).astype(BF16)
    stream_ref[...] = stream
    normed_ref[...] = normalised(stream.astype(F32), fg_ref[...]).astype(BF16)


def gelu(v):
    return 0.5 * v * (1.0 + jnp.tanh(0.7978845608028654 * (v + 0.044715 * v * v * v)))


def ffn_kernel(pieces, at_ref, halo_ref, taps_ref, all_ref, *refs):
    toks_in, refs = refs[:pieces], refs[pieces:]
    keep_ref, send_ref, x_ref, g_ref, v_ref, d_ref, even_ref, odd_ref, h_ref, p_ref = refs[:10]
    sem_x, sem_g, sem_v, sem_d, sem_o = refs[10:]
    main = x_ref.shape[0] - halo_ref.shape[0]
    units = d_ref.shape[1]
    shards = d_ref.shape[0]
    block = taps_ref.shape[2] // 2
    blocks = taps_ref.shape[0]

    def token_copy(i):
        size = toks_in[i].shape[0]
        start = pl.multiple_of(at_ref[i], 16)
        return pltpu.make_async_copy(toks_in[i], x_ref.at[pl.ds(start, size), :], sem_x.at[i])

    def rows_copy(b, base, ref, sem):
        start = pl.multiple_of(b * block, block)
        return pltpu.make_async_copy(
            all_ref.at[:, pl.ds(base + start, block), :], ref.at[:, pl.ds(start, block), :], sem.at[b]
        )

    def gate_copy(b):
        return rows_copy(b, 0, g_ref, sem_g)

    def value_copy(b):
        return rows_copy(b, units, v_ref, sem_v)

    down = pltpu.make_async_copy(all_ref.at[:, pl.ds(2 * units, units), :], d_ref, sem_d)
    for i in range(pieces):
        token_copy(i).start()
    for b in range(blocks):
        gate_copy(b).start()
        value_copy(b).start()
    down.start()
    x_ref[pl.ds(main, halo_ref.shape[0]), :] = halo_ref[...]
    for i in range(pieces):
        token_copy(i).wait()

    def arrive(b):
        gate_copy(b).wait()
        value_copy(b).wait()

    def up(b, out_ref):
        rows = pl.ds(b * block, block)
        w = [
            jnp.concatenate([ref[s, rows, :] for s in range(shards)], axis=1) for ref in (g_ref, v_ref)
        ]
        w = jnp.concatenate(w, axis=0)
        y = lax.dot_general(x_ref[...], w, NT, preferred_element_type=F32)
        out_ref[...] = y.astype(BF16).astype(F32)

    def finish(b, in_ref):
        now = in_ref[pl.ds(0, main), :]
        row = lax.broadcasted_iota(jnp.int32, now.shape, 0)
        before = jnp.where(row == 0, in_ref[main : main + 1, :], pltpu.roll(now, 1, 0))
        after = jnp.where(row == main - 1, in_ref[main + 1 : main + 2, :], pltpu.roll(now, main - 1, 0))
        taps = taps_ref[b]
        mixed = taps[0:1] * before + taps[1:2] * now + taps[2:3] * after
        h_ref[:, pl.ds(b * block, block)] = (gelu(mixed[:, :block]) * mixed[:, block:]).astype(BF16)

    arrive(0)
    up(0, even_ref)

    def pair(i, unused):
        b = pl.multiple_of(2 * i, 2)
        arrive(b + 1)
        arrive(b + 2)
        up(b + 1, odd_ref)
        finish(b, even_ref)
        up(b + 2, even_ref)
        finish(b + 1, odd_ref)
        return unused

    lax.fori_loop(0, blocks // 2 - 1, pair, 0)
    arrive(blocks - 1)
    up(blocks - 1, odd_ref)
    finish(blocks - 2, even_ref)
    finish(blocks - 1, odd_ref)
    down.wait()

    def down_block(n, unused):
        w = jnp.concatenate([d_ref[4 * n + i] for i in range(4)], axis=1)
        y = jnp.dot(h_ref[:, :units], w, preferred_element_type=F32)
        p_ref[:, pl.ds(pl.multiple_of(n * 512, 512), 512)] = y.astype(BF16)
        return unused

    lax.fori_loop(0, shards // 4, down_block, 0)
    count, own = keep_ref.shape[0], keep_ref.shape[1]
    outs = []
    for k in range(count):
        for o, ref in enumerate((keep_ref, send_ref)):
            start = pl.multiple_of(at_ref[pieces + 2 * k + o], 16)
            outs.append(
                pltpu.make_async_copy(p_ref.at[pl.ds(start, own), :], ref.at[k], sem_o.at[2 * k + o])
            )
    for c in outs:
        c.start()
    for c in outs:
        c.wait()


def vmem(limit=56 << 20):
    return pltpu.CompilerParams(vmem_limit_bytes=limit)


def body(
    queries,
    keys,
    values,
    query_gain,
    key_gain,
    residual,
    out_weight,
    mix_gain,
    ffn_gain,
    gate_in,
    value_in,
    conv_gate,
    conv_value,
    down_t,
):
    tok = queries.shape[0]
    hd = query_gain.shape[0]
    n_sp, n_tp = lax.axis_size("sp"), lax.axis_size("tp")
    n_x = n_tp // 2
    group = HEADS // KVH
    splits = n_tp // KVH
    part = tok // splits
    own = tok // n_tp
    model = residual.shape[1]
    units = gate_in.shape[1]
    tp, sp = lax.axis_index("tp"), lax.axis_index("sp")
    kv_head, piece = tp // splits, tp % splits
    x, core = tp // 2, tp % 2

    def send(array, change):
        return lax.ppermute(array, "tp", [(i, change(i)) for i in range(n_tp)])

    def other_core(array):
        return send(array, lambda i: i ^ 1)

    def up_x(array):
        return send(array, lambda i: (i + 2) % n_tp)

    def down_x(array):
        return send(array, lambda i: (i - 2) % n_tp)

    def far_x(array):
        return send(array, lambda i: (i + n_x) % n_tp)

    def gathered(mine, direct=False):
        size = mine.shape[0]
        half = size // 2
        a = up_x(mine)
        b = down_x(mine)
        near = other_core(mine)
        if direct:
            pieces = [(mine, tp), (near, tp ^ 1)]
            far = far_x(mine)
            for array, shift in ((a, n_x - 1), (b, 1), (far, n_x // 2)):
                base = ((x + shift) % n_x) * 2
                across = other_core(array)
                pieces += [(array, base + core), (across, base + 1 - core)]
            return [p[0] for p in pieces], [p[1] * size for p in pieces]
        c = up_x(a[:half])
        d = down_x(b[half:])
        low, high = ((x + n_x - 1) % n_x) * 2, ((x + 1) % n_x) * 2
        far = (tp + n_x) % n_tp
        found = [(mine, tp * size), (near, (tp ^ 1) * size)]
        for array, base in ((a, low), (b, high)):
            across = other_core(array)
            found.append((array, (base + core) * size))
            found.append((across, (base + 1 - core) * size))
        for array, shift in ((c, 0), (d, half)):
            found.append((array, far * size + shift))
            found.append((other_core(array), (far ^ 1) * size + shift))
        return [f[0] for f in found], [f[1] for f in found]

    row_np, col_np = rotary_parts(tok * n_sp, hd)
    row_np = row_np.reshape(n_sp, tok // GRID_W, 2 * hd)
    rows_all, cols_all = jnp.asarray(row_np), jnp.asarray(col_np)
    at = jnp.stack([piece, kv_head, sp, core, x]).astype(jnp.int32)
    packed_rows = 2 * part
    packed = pl.pallas_call(
        key_kernel,
        out_shape=jax.ShapeDtypeStruct((packed_rows, hd), BF16),
        grid_spec=pltpu.PrefetchScalarGridSpec(
            num_scalar_prefetch=1,
            grid=(1,),
            in_specs=[
                pl.BlockSpec((part, hd), lambda i, a: (a[0], a[1])),
                pl.BlockSpec((part, hd), lambda i, a: (a[0], a[1])),
                pl.BlockSpec((1, hd), lambda i, a: (0, 0)),
                pl.BlockSpec((1,) + row_np.shape[1:], lambda i, a: (a[2], 0, 0)),
                pl.BlockSpec(col_np.shape, lambda i, a: (0, 0)),
            ],
            out_specs=pl.BlockSpec((packed_rows, hd), lambda i, a: (0, 0)),
        ),
        name="key_prep",
    )(at, keys, values, key_gain[None], rows_all, cols_all)
    weights = jnp.concatenate([gate_in.T, value_in.T, down_t.T], axis=0)
    gate_rows = lax.all_gather(weights, "sp", axis=0, tiled=False)

    mine = pl.pallas_call(
        query_kernel,
        out_shape=jax.ShapeDtypeStruct((tok, hd), BF16),
        grid_spec=pltpu.PrefetchScalarGridSpec(
            num_scalar_prefetch=1,
            grid=(1,),
            in_specs=[
                pl.BlockSpec((tok, hd), lambda i, a: (0, 0)),
                pl.BlockSpec((1, hd), lambda i, a: (0, 0)),
                pl.BlockSpec((1,) + row_np.shape[1:], lambda i, a: (a[2], 0, 0)),
                pl.BlockSpec(col_np.shape, lambda i, a: (0, 0)),
            ],
            out_specs=pl.BlockSpec((tok, hd), lambda i, a: (0, 0)),
        ),
        name="query_prep",
    )(at, queries, query_gain[None], rows_all, cols_all)
    pair = send(mine, lambda i: i ^ 2)
    turned_q = [mine, other_core(mine), pair, other_core(pair)]
    rows = group * own

    out_pieces, out_at = gathered(out_weight, direct=True)

    packed, queries, out_weight = lax.optimization_barrier((packed, queries, out_weight))
    right = [(i, (i + 1) % n_sp) for i in range(n_sp)]
    left = [(i, (i - 1) % n_sp) for i in range(n_sp)]
    tail = 32
    anywhere = pl.BlockSpec(memory_space=pl.ANY)

    def attend(here, base, steps, before):
        last = before is not None
        if last:
            shape = (n_x, rows + tail, hd)
            out_shape = [jax.ShapeDtypeStruct(shape, BF16)] * 2
            out_specs = [pl.BlockSpec((1,) + shape[1:], lambda i, a: (lax.rem(i + n_x - a[4], n_x), 0, 0))] * 2
        else:
            shape = (steps, 2, 2 * rows, hd)
            out_shape = jax.ShapeDtypeStruct(shape, F32)
            out_specs = pl.BlockSpec((1,) + shape[1:], lambda i, a: (i, 0, 0, 0))
        in_specs = [anywhere] * group + [pl.BlockSpec((2 * part, hd), lambda i, a: (0, 0))] * len(here)
        if last:
            kept = (1, 2, 2 * rows, hd)
            in_specs.append(pl.BlockSpec(kept, lambda i, a: (lax.min(i, n_x // 2 - 1), 0, 0, 0)))
            in_specs.append(pl.BlockSpec(kept, lambda i, a: (lax.max(i - n_x // 2, 0), 0, 0, 0)))
        share = group * tok * part * len(here) * steps // n_x
        return pl.pallas_call(
            functools.partial(attend_kernel, len(here), group, own, base, last),
            out_shape=out_shape,
            grid_spec=pltpu.PrefetchScalarGridSpec(
                num_scalar_prefetch=1,
                grid=(steps,),
                in_specs=in_specs,
                out_specs=out_specs,
                scratch_shapes=[pltpu.VMEM((group, tok, hd), BF16), pltpu.SemaphoreType.DMA((group,))],
            ),
            compiler_params=vmem(36 << 20),
            cost_estimate=pl.CostEstimate(
                flops=8 * share * hd, bytes_accessed=8 << 20, transcendentals=share
            ),
        )(at, *turned_q, *here, *(before or ()))

    shards = [packed]
    a = b = packed
    kept = []
    for s in range(1, n_sp // 2 + 1):
        a = lax.ppermute(a, "sp", right)
        shards.append(a)
        if len(shards) < n_sp:
            b = lax.ppermute(b, "sp", left)
            shards.append(b)
        if s == n_sp // 4:
            a, b, *turned_q = lax.optimization_barrier((a, b, *turned_q))
        if s in (n_sp // 4, n_sp // 4 + 1):
            kept.append(attend(shards[: n_sp // 2], len(kept) * (n_x // 2), n_x // 2, None))
        if s in (n_sp // 4 + 1, n_sp // 4 + 2):
            a, b, kept[s - n_sp // 4 - 1] = lax.optimization_barrier((a, b, kept[s - n_sp // 4 - 1]))
    a, *out_pieces = lax.optimization_barrier((a, *out_pieces))
    keep, away = attend(shards[n_sp // 2 : -1] + [a], 0, n_x, kept)
    merged = pl.pallas_call(
        functools.partial(merge_kernel, rows),
        out_shape=[jax.ShapeDtypeStruct((rows + tail, hd), BF16)] * n_x,
        compiler_params=vmem(16 << 20),
        name="merge",
    )(keep, other_core(away))
    seen = [merged[0], up_x(merged[1]), far_x(merged[2]), down_x(merged[3])]
    seen_at = [(x + n_x - k) % n_x for k in range(n_x)]
    whole = pl.BlockSpec(memory_space=pltpu.VMEM)
    stream, normed = pl.pallas_call(
        functools.partial(mix_kernel, group, n_x, len(out_pieces)),
        out_shape=[jax.ShapeDtypeStruct((own, model), BF16)] * 2,
        in_specs=[pl.BlockSpec(memory_space=pltpu.SMEM)] + [whole] * 3 + [anywhere] * (n_x + len(out_pieces)),
        scratch_shapes=[
            pltpu.VMEM((n_x, rows + tail, hd), BF16),
            pltpu.VMEM((own, HEADS * hd), BF16),
            pltpu.VMEM((HEADS * hd, model), BF16),
            pltpu.SemaphoreType.DMA((n_x,)),
            pltpu.SemaphoreType.DMA((len(out_pieces),)),
        ],
        compiler_params=vmem(20 << 20),
        cost_estimate=pl.CostEstimate(
            flops=2 * own * HEADS * hd * model, bytes_accessed=6 << 20, transcendentals=0
        ),
        name="mix",
    )(
        jnp.stack(out_at + seen_at).astype(jnp.int32),
        residual,
        mix_gain[None],
        ffn_gain[None],
        *seen,
        *out_pieces,
    )

    token_pieces, token_at = gathered(normed)
    first = last_row = None
    for p, r in zip(token_pieces, token_at):
        f = jnp.where(r == 0, p[:1], 0)
        e = jnp.where(r + p.shape[0] == tok, p[-1:], 0)
        first = f if first is None else first + f
        last_row = e if last_row is None else last_row + e
    before = lax.ppermute(last_row, "sp", [(i, i + 1) for i in range(n_sp - 1)])
    after = lax.ppermute(first, "sp", [(i + 1, i) for i in range(n_sp - 1)])
    halo = jnp.concatenate([before, after, jnp.zeros((14, model), BF16)], axis=0)
    block = 128
    blocks = -(-units // block)

    def by_block(taps):
        wide = jnp.pad(taps, ((0, 5), (0, blocks * block - units)))
        return jnp.transpose(wide.reshape(8, blocks, block), (1, 0, 2))

    taps = jnp.concatenate([by_block(conv_gate), by_block(conv_value)], axis=2)
    slots = []
    for k in range(n_x):
        to = ((x + k) % n_x) * 2
        slots += [(to + core) * own, (to + 1 - core) * own]
    where = jnp.stack(token_at + slots).astype(jnp.int32)
    keep, away = pl.pallas_call(
        functools.partial(ffn_kernel, len(token_pieces)),
        out_shape=[jax.ShapeDtypeStruct((n_x, own, model), BF16)] * 2,
        in_specs=[pl.BlockSpec(memory_space=pltpu.SMEM), whole, whole, anywhere] + [anywhere] * len(token_pieces),
        out_specs=[anywhere, anywhere],
        scratch_shapes=[
            pltpu.VMEM((tok + 16, model), BF16),
            pltpu.VMEM((n_sp, blocks * block, hd), BF16),
            pltpu.VMEM((n_sp, blocks * block, hd), BF16),
            pltpu.VMEM((n_sp, units, hd), BF16),
            pltpu.VMEM((tok + 16, 2 * block), F32),
            pltpu.VMEM((tok + 16, 2 * block), F32),
            pltpu.VMEM((tok, blocks * block), BF16),
            pltpu.VMEM((tok, model), BF16),
            pltpu.SemaphoreType.DMA((len(token_pieces),)),
            pltpu.SemaphoreType.DMA((blocks,)),
            pltpu.SemaphoreType.DMA((blocks,)),
            pltpu.SemaphoreType.DMA,
            pltpu.SemaphoreType.DMA((2 * n_x,)),
        ],
        compiler_params=vmem(56 << 20),
        cost_estimate=pl.CostEstimate(
            flops=6 * tok * units * model, bytes_accessed=16 << 20, transcendentals=tok * units
        ),
        name="ffn",
    )(where, halo, taps, gate_rows, *token_pieces)
    near = other_core(away)
    total = [keep[k].astype(F32) + near[k].astype(F32) for k in range(n_x)]
    one = up_x(total[1].astype(BF16))
    two = far_x(total[2].astype(BF16))
    three = down_x(total[3].astype(BF16))
    out = total[0] + one.astype(F32) + two.astype(F32) + three.astype(F32)
    return (stream.astype(F32) + out).astype(BF16)


def solution(mesh):
    return jax.shard_map(
        body,
        mesh=mesh,
        in_specs=(
            P(("grp", "sp"), "tp"),
            P(("grp", "sp"), None),
            P(("grp", "sp"), None),
            P(),
            P(),
            P(("grp", "sp", "tp"), None),
            P("tp", None),
            P(),
            P(),
            P("sp", "tp"),
            P("sp", "tp"),
            P(None, "tp"),
            P(None, "tp"),
            P("sp", "tp"),
        ),
        out_specs=P(("grp", "sp", "tp"), None),
        check_vma=False,
    )
```

```python
import functools
import numpy as np
import jax
import jax.numpy as jnp
from jax import lax
from jax.experimental import pallas as pl
from jax.experimental.pallas import tpu as pltpu
from jax.sharding import PartitionSpec as P

HEADS = 8
KVH = 2
GRID_W = 64
EPSILON = 1e-06
THETA = 10000.0
F32 = jnp.float32
BF16 = jnp.bfloat16
NT = (((1,), (1,)), ((), ()))


def rotary_parts(seq_total, head_dim):
    quarter = head_dim // 4
    inverse = THETA ** (-(2.0 * np.arange(quarter, dtype=np.float32)) / np.float32(head_dim // 2))
    inverse = inverse.astype(np.float32)
    rows = seq_total // GRID_W
    row_angle = (np.arange(rows) - rows // 2).astype(np.float32)[:, None] * inverse
    col_angle = (np.arange(GRID_W) - GRID_W // 2).astype(np.float32)[:, None] * inverse

    def lanes(angle, first):
        zero = np.zeros_like(angle)
        cos, sin = np.cos(angle.astype(np.float64)), np.sin(angle.astype(np.float64))
        cos, sin = [cos, cos], [-sin, sin]
        pad = [zero, zero]
        parts = (cos + pad if first else pad + cos) + (sin + pad if first else pad + sin)
        return np.concatenate(parts, axis=-1).astype(np.float32)

    return lanes(row_angle, True), lanes(col_angle, False)


def turned(raw, gain, cos, sin, factor):
    x = raw.astype(F32)
    head_dim = x.shape[-1]
    quarter = head_dim // 4
    normed = x * lax.rsqrt(jnp.mean(x * x, axis=-1, keepdims=True) + EPSILON) * gain
    lane = lax.broadcasted_iota(jnp.int32, x.shape, 1)
    other = jnp.where(
        (lane & quarter) == 0,
        pltpu.roll(normed, head_dim - quarter, 1),
        pltpu.roll(normed, quarter, 1),
    )
    return ((normed * cos + other * sin) * factor).astype(BF16)


def key_kernel(at_ref, k_ref, v_ref, gain_ref, row_ref, col_ref, out_ref):
    part, hd = k_ref.shape
    count = part // GRID_W
    for i in range(count):
        rows = pl.ds(i * GRID_W, GRID_W)
        table = row_ref[0, pl.ds(at_ref[0] * count + i, 1), :] + col_ref[...]
        out_ref[rows, :] = turned(k_ref[rows, :], gain_ref[...], table[:, :hd], table[:, hd:], 1.0)
    out_ref[pl.ds(part, part), :] = v_ref[...]


def query_kernel(at_ref, raw_ref, gain_ref, row_ref, col_ref, out_ref):
    hd = raw_ref.shape[1]
    for i in range(raw_ref.shape[0] // GRID_W):
        table = row_ref[0, pl.ds(i, 1), :] + col_ref[...]
        rows = pl.ds(i * GRID_W, GRID_W)
        out_ref[rows, :] = turned(
            raw_ref[rows, :], gain_ref[...], table[:, :hd], table[:, hd:], hd ** (-0.5)
        )


def as_row(col, eye):
    return jnp.sum(jnp.where(eye, col, 0.0), axis=0, keepdims=True)


def as_col(row, eye):
    return jnp.sum(jnp.where(eye, row, 0.0), axis=1, keepdims=True)


def square_eye(n):
    return lax.broadcasted_iota(jnp.int32, (n, n), 0) == lax.broadcasted_iota(jnp.int32, (n, n), 1)


def stats_rows(col, eye, tail):
    hd = eye.shape[0]
    rows = [as_row(col[b * hd : (b + 1) * hd], eye) for b in range(col.shape[0] // hd)]
    left = jnp.concatenate(rows + [jnp.zeros((8 - len(rows), hd), F32)], axis=0)
    high = left.astype(BF16).astype(F32)
    left = left - high
    mid = left.astype(BF16).astype(F32)
    return jnp.concatenate([high, mid, left - mid, jnp.zeros((tail - 24, hd), F32)], axis=0).astype(BF16)


def stats_col(block, eye, count):
    block = block.astype(F32)
    block = block[0:8] + block[8:16] + block[16:24]
    return jnp.concatenate([as_col(block[b : b + 1], eye) for b in range(count)], axis=0)


def attend_kernel(shards, heads, own, base, last, at_ref, *refs):
    q_in, refs = refs[:heads], refs[heads:]
    kv, refs = refs[:shards], refs[shards:]
    if last:
        before, refs = refs[:2], refs[2:]
        outs, (q_ref, sem) = refs[:2], refs[2:]
    else:
        out_ref, q_ref, sem = refs
    core, slot0 = at_ref[3], at_ref[0]
    step = pl.program_id(0) + base
    hd = q_ref.shape[2]
    half = hd // 2
    rows = heads * own
    part = kv[0].shape[0] // 2

    @pl.when(pl.program_id(0) == 0)
    def _():
        copies = []
        for k in range(heads):
            copies.append(pltpu.make_async_copy(q_in[k], q_ref.at[slot0 ^ k], sem.at[k]))
        for c in copies:
            c.start()
        for c in copies:
            c.wait()

    keys = jnp.concatenate([r[pl.ds(0, part), :] for r in kv], axis=0)
    vals = jnp.concatenate([r[pl.ds(part, part), :] for r in kv], axis=0)
    eye = square_eye(hd)
    todo = [(p, h) for p in range(2) for h in range(0, heads, 2)]
    size = 2 * own

    def score(p, h):
        start = pl.multiple_of((2 * step + (core ^ p)) * own, 32)
        q = jnp.concatenate([q_ref[h + i, pl.ds(start, own), :] for i in range(2)], axis=0)
        return lax.dot_general(q, keys, NT, preferred_element_type=F32)

    lse = [[], []]
    ahead = score(*todo[0])
    for i, (p, h) in enumerate(todo):
        s = ahead
        if i + 1 < len(todo):
            ahead = score(*todo[i + 1])
        here = pl.ds(h * own, size)
        there = pl.ds(rows + h * own, size)
        m = jnp.max(s, axis=1, keepdims=True)
        if last:
            early = step < pl.num_programs(0) // 2
            stats = jnp.where(early, before[0][0, p, there, :], before[1][0, p, there, :])
            m_old, den_old = stats[:, 0:1], stats[:, half : half + 1]
            m = jnp.maximum(m, m_old)
        e = jnp.exp(s - m)
        den = jnp.sum(e, axis=1, keepdims=True)
        acc = jnp.dot(e.astype(BF16), vals, preferred_element_type=F32)
        if last:
            fade = jnp.exp(m_old - m)
            den = den + den_old * fade
            acc = acc + jnp.where(early, before[0][0, p, here, :], before[1][0, p, here, :]) * fade
            outs[p][0, here, :] = (acc / den).astype(BF16)
            lse[p].append(m + jnp.log(den))
        else:
            out_ref[0, p, here, :] = acc
            lane = lax.broadcasted_iota(jnp.int32, (size, hd), 1)
            out_ref[0, p, there, :] = jnp.where(lane < half, m, den)
    if last:
        tail = outs[0].shape[1] - rows
        for p in range(2):
            outs[p][0, pl.ds(rows, tail), :] = stats_rows(jnp.concatenate(lse[p], axis=0), eye, tail)


def merge_kernel(rows, a_ref, b_ref, *out_refs):
    hd = a_ref.shape[2]
    tail = a_ref.shape[1] - rows
    eye = square_eye(hd)
    for k, out_ref in enumerate(out_refs):
        la = stats_col(a_ref[k, pl.ds(rows, tail), :], eye, rows // hd)
        lb = stats_col(b_ref[k, pl.ds(rows, tail), :], eye, rows // hd)
        top = jnp.maximum(la, lb)
        wa, wb = jnp.exp(la - top), jnp.exp(lb - top)
        total = wa + wb
        a = a_ref[k, pl.ds(0, rows), :].astype(F32)
        b = b_ref[k, pl.ds(0, rows), :].astype(F32)
        out_ref[pl.ds(0, rows), :] = (a * (wa / total) + b * (wb / total)).astype(BF16)
        out_ref[pl.ds(rows, tail), :] = stats_rows(top + jnp.log(total), eye, tail)


def normalised(x, gain):
    return x * lax.rsqrt(jnp.mean(x * x, axis=-1, keepdims=True) + EPSILON) * gain


def mix_kernel(group, chips, pieces, at_ref, res_ref, mg_ref, fg_ref, *refs):
    seen, refs = refs[:chips], refs[chips:]
    parts, refs = refs[:pieces], refs[pieces:]
    stream_ref, normed_ref, in_ref, att_ref, w_ref, sem_in, sem = refs
    arrive = []
    for i, one in enumerate(seen):
        arrive.append(pltpu.make_async_copy(one, in_ref.at[at_ref[pieces + i]], sem_in.at[i]))
    copies = []
    for i, part in enumerate(parts):
        size = part.shape[0]
        start = pl.multiple_of(at_ref[i], size)
        copies.append(pltpu.make_async_copy(part, w_ref.at[pl.ds(start, size), :], sem.at[i]))
    for c in arrive + copies:
        c.start()
    for c in arrive:
        c.wait()
    hd = in_ref.shape[2]
    toks = res_ref.shape[0]
    rows = group * toks
    tail = in_ref.shape[1] - rows
    splits = chips // KVH
    eye = square_eye(hd)
    for kv in range(KVH):
        cols = [stats_col(in_ref[kv * splits + j, pl.ds(rows, tail), :], eye, rows // hd) for j in range(splits)]
        top = functools.reduce(jnp.maximum, cols)
        w = [jnp.exp(x - top) for x in cols]
        total = functools.reduce(jnp.add, w)
        acc = None
        for j in range(splits):
            term = (w[j] / total) * in_ref[kv * splits + j, pl.ds(0, rows), :].astype(F32)
            acc = term if acc is None else acc + term
        acc = acc.astype(BF16)
        for h in range(group):
            c = (kv * group + h) * hd
            att_ref[:, c : c + hd] = acc[h * toks : (h + 1) * toks]
    for c in copies:
        c.wait()
    mix = jnp.dot(att_ref[...], w_ref[...], preferred_element_type=F32)
    stream = (res_ref[...].astype(F32) + normalised(mix, mg_ref[...])).astype(BF16)
    stream_ref[...] = stream
    normed_ref[...] = normalised(stream.astype(F32), fg_ref[...]).astype(BF16)


def gelu(v):
    return 0.5 * v * (1.0 + jnp.tanh(0.7978845608028654 * (v + 0.044715 * v * v * v)))


def ffn_kernel(pieces, at_ref, first_ref, last_ref, taps_ref, all_ref, *refs):
    toks_in, refs = refs[:pieces], refs[pieces:]
    keep_ref, send_ref, x_ref, g_ref, v_ref, d_ref, even_ref, odd_ref, h_ref, p_ref = refs[:10]
    sem_x, sem_g, sem_v, sem_d, sem_o = refs[10:]
    edge = 16
    main = x_ref.shape[0] - edge
    units = d_ref.shape[1]
    shards = d_ref.shape[0]
    block = taps_ref.shape[2] // 2
    blocks = taps_ref.shape[0]

    def token_copy(i):
        size = toks_in[i].shape[0]
        start = pl.multiple_of(at_ref[i], 16)
        return pltpu.make_async_copy(toks_in[i], x_ref.at[pl.ds(start, size), :], sem_x.at[i])

    def rows_copy(b, base, ref, sem):
        start = pl.multiple_of(b * block, block)
        return pltpu.make_async_copy(
            all_ref.at[:, pl.ds(base + start, block), :], ref.at[:, pl.ds(start, block), :], sem.at[b]
        )

    def gate_copy(b):
        return rows_copy(b, 0, g_ref, sem_g)

    def value_copy(b):
        return rows_copy(b, units, v_ref, sem_v)

    down = pltpu.make_async_copy(all_ref.at[:, pl.ds(2 * units, units), :], d_ref, sem_d)
    for i in range(pieces):
        token_copy(i).start()
    for b in range(blocks):
        gate_copy(b).start()
        value_copy(b).start()
    down.start()
    row = lax.broadcasted_iota(jnp.int32, (edge, x_ref.shape[1]), 0)
    halo = jnp.where(row == 0, first_ref[...].astype(F32), 0.0)
    halo = jnp.where(row == 1, last_ref[...].astype(F32), halo)
    x_ref[pl.ds(main, edge), :] = halo.astype(BF16)
    for i in range(pieces):
        token_copy(i).wait()

    def arrive(b):
        gate_copy(b).wait()
        value_copy(b).wait()

    def up(b, out_ref):
        rows = pl.ds(b * block, block)
        w = [
            jnp.concatenate([ref[s, rows, :] for s in range(shards)], axis=1) for ref in (g_ref, v_ref)
        ]
        w = jnp.concatenate(w, axis=0)
        y = lax.dot_general(x_ref[...], w, NT, preferred_element_type=F32)
        out_ref[...] = y.astype(BF16).astype(F32)

    def finish(b, in_ref):
        now = in_ref[pl.ds(0, main), :]
        row = lax.broadcasted_iota(jnp.int32, now.shape, 0)
        before = jnp.where(row == 0, in_ref[main : main + 1, :], pltpu.roll(now, 1, 0))
        after = jnp.where(row == main - 1, in_ref[main + 1 : main + 2, :], pltpu.roll(now, main - 1, 0))
        taps = taps_ref[b]
        mixed = taps[0:1] * before + taps[1:2] * now + taps[2:3] * after
        h_ref[:, pl.ds(b * block, block)] = (gelu(mixed[:, :block]) * mixed[:, block:]).astype(BF16)

    arrive(0)
    up(0, even_ref)

    def pair(i, unused):
        b = pl.multiple_of(2 * i, 2)
        arrive(b + 1)
        arrive(b + 2)
        up(b + 1, odd_ref)
        finish(b, even_ref)
        up(b + 2, even_ref)
        finish(b + 1, odd_ref)
        return unused

    lax.fori_loop(0, blocks // 2 - 1, pair, 0)
    arrive(blocks - 1)
    up(blocks - 1, odd_ref)
    finish(blocks - 2, even_ref)
    finish(blocks - 1, odd_ref)
    down.wait()

    def down_block(n, unused):
        w = jnp.concatenate([d_ref[4 * n + i] for i in range(4)], axis=1)
        y = jnp.dot(h_ref[:, :units], w, preferred_element_type=F32)
        p_ref[:, pl.ds(pl.multiple_of(n * 512, 512), 512)] = y.astype(BF16)
        return unused

    lax.fori_loop(0, shards // 4, down_block, 0)
    count, own = keep_ref.shape[0], keep_ref.shape[1]
    outs = []
    for k in range(count):
        for o, ref in enumerate((keep_ref, send_ref)):
            start = pl.multiple_of(at_ref[pieces + 2 * k + o], 16)
            outs.append(
                pltpu.make_async_copy(p_ref.at[pl.ds(start, own), :], ref.at[k], sem_o.at[2 * k + o])
            )
    for c in outs:
        c.start()
    for c in outs:
        c.wait()


def vmem(limit=56 << 20):
    return pltpu.CompilerParams(vmem_limit_bytes=limit)


def body(
    queries,
    keys,
    values,
    query_gain,
    key_gain,
    residual,
    out_weight,
    mix_gain,
    ffn_gain,
    gate_in,
    value_in,
    conv_gate,
    conv_value,
    down_t,
):
    tok = queries.shape[0]
    hd = query_gain.shape[0]
    n_sp, n_tp = lax.axis_size("sp"), lax.axis_size("tp")
    n_x = n_tp // 2
    group = HEADS // KVH
    splits = n_tp // KVH
    part = tok // splits
    own = tok // n_tp
    model = residual.shape[1]
    units = gate_in.shape[1]
    tp, sp = lax.axis_index("tp"), lax.axis_index("sp")
    kv_head, piece = tp // splits, tp % splits
    x, core = tp // 2, tp % 2

    def send(array, change):
        return lax.ppermute(array, "tp", [(i, change(i)) for i in range(n_tp)])

    def other_core(array):
        return send(array, lambda i: i ^ 1)

    def up_x(array):
        return send(array, lambda i: (i + 2) % n_tp)

    def down_x(array):
        return send(array, lambda i: (i - 2) % n_tp)

    def far_x(array):
        return send(array, lambda i: (i + n_x) % n_tp)

    def gathered(mine, direct=False):
        size = mine.shape[0]
        half = size // 2
        a = up_x(mine)
        b = down_x(mine)
        near = other_core(mine)
        if direct:
            pieces = [(mine, tp), (near, tp ^ 1)]
            far = far_x(mine)
            for array, shift in ((a, n_x - 1), (b, 1), (far, n_x // 2)):
                base = ((x + shift) % n_x) * 2
                across = other_core(array)
                pieces += [(array, base + core), (across, base + 1 - core)]
            return [p[0] for p in pieces], [p[1] * size for p in pieces]
        c = up_x(a[:half])
        d = down_x(b[half:])
        low, high = ((x + n_x - 1) % n_x) * 2, ((x + 1) % n_x) * 2
        far = (tp + n_x) % n_tp
        found = [(mine, tp * size), (near, (tp ^ 1) * size)]
        for array, base in ((a, low), (b, high)):
            across = other_core(array)
            found.append((array, (base + core) * size))
            found.append((across, (base + 1 - core) * size))
        for array, shift in ((c, 0), (d, half)):
            found.append((array, far * size + shift))
            found.append((other_core(array), (far ^ 1) * size + shift))
        return [f[0] for f in found], [f[1] for f in found]

    row_np, col_np = rotary_parts(tok * n_sp, hd)
    row_np = row_np.reshape(n_sp, tok // GRID_W, 2 * hd)
    rows_all, cols_all = jnp.asarray(row_np), jnp.asarray(col_np)
    at = jnp.stack([piece, kv_head, sp, core, x]).astype(jnp.int32)
    packed_rows = 2 * part
    packed = pl.pallas_call(
        key_kernel,
        out_shape=jax.ShapeDtypeStruct((packed_rows, hd), BF16),
        grid_spec=pltpu.PrefetchScalarGridSpec(
            num_scalar_prefetch=1,
            grid=(1,),
            in_specs=[
                pl.BlockSpec((part, hd), lambda i, a: (a[0], a[1])),
                pl.BlockSpec((part, hd), lambda i, a: (a[0], a[1])),
                pl.BlockSpec((1, hd), lambda i, a: (0, 0)),
                pl.BlockSpec((1,) + row_np.shape[1:], lambda i, a: (a[2], 0, 0)),
                pl.BlockSpec(col_np.shape, lambda i, a: (0, 0)),
            ],
            out_specs=pl.BlockSpec((packed_rows, hd), lambda i, a: (0, 0)),
        ),
        name="key_prep",
    )(at, keys, values, key_gain[None], rows_all, cols_all)
    weights = jnp.concatenate([gate_in.T, value_in.T, down_t.T], axis=0)
    gate_rows = lax.all_gather(weights, "sp", axis=0, tiled=False)

    mine = pl.pallas_call(
        query_kernel,
        out_shape=jax.ShapeDtypeStruct((tok, hd), BF16),
        grid_spec=pltpu.PrefetchScalarGridSpec(
            num_scalar_prefetch=1,
            grid=(1,),
            in_specs=[
                pl.BlockSpec((tok, hd), lambda i, a: (0, 0)),
                pl.BlockSpec((1, hd), lambda i, a: (0, 0)),
                pl.BlockSpec((1,) + row_np.shape[1:], lambda i, a: (a[2], 0, 0)),
                pl.BlockSpec(col_np.shape, lambda i, a: (0, 0)),
            ],
            out_specs=pl.BlockSpec((tok, hd), lambda i, a: (0, 0)),
        ),
        name="query_prep",
    )(at, queries, query_gain[None], rows_all, cols_all)
    pair = send(mine, lambda i: i ^ 2)
    turned_q = [mine, other_core(mine), pair, other_core(pair)]
    rows = group * own

    out_pieces, out_at = gathered(out_weight, direct=True)

    packed, queries, out_weight = lax.optimization_barrier((packed, queries, out_weight))
    right = [(i, (i + 1) % n_sp) for i in range(n_sp)]
    left = [(i, (i - 1) % n_sp) for i in range(n_sp)]
    tail = 32
    anywhere = pl.BlockSpec(memory_space=pl.ANY)

    def attend(here, base, steps, before):
        last = before is not None
        if last:
            shape = (n_x, rows + tail, hd)
            out_shape = [jax.ShapeDtypeStruct(shape, BF16)] * 2
            out_specs = [pl.BlockSpec((1,) + shape[1:], lambda i, a: (lax.rem(i + n_x - a[4], n_x), 0, 0))] * 2
        else:
            shape = (steps, 2, 2 * rows, hd)
            out_shape = jax.ShapeDtypeStruct(shape, F32)
            out_specs = pl.BlockSpec((1,) + shape[1:], lambda i, a: (i, 0, 0, 0))
        in_specs = [anywhere] * group + [pl.BlockSpec((2 * part, hd), lambda i, a: (0, 0))] * len(here)
        if last:
            kept = (1, 2, 2 * rows, hd)
            in_specs.append(pl.BlockSpec(kept, lambda i, a: (lax.min(i, n_x // 2 - 1), 0, 0, 0)))
            in_specs.append(pl.BlockSpec(kept, lambda i, a: (lax.max(i - n_x // 2, 0), 0, 0, 0)))
        share = group * tok * part * len(here) * steps // n_x
        return pl.pallas_call(
            functools.partial(attend_kernel, len(here), group, own, base, last),
            out_shape=out_shape,
            grid_spec=pltpu.PrefetchScalarGridSpec(
                num_scalar_prefetch=1,
                grid=(steps,),
                in_specs=in_specs,
                out_specs=out_specs,
                scratch_shapes=[pltpu.VMEM((group, tok, hd), BF16), pltpu.SemaphoreType.DMA((group,))],
            ),
            compiler_params=vmem(),
            cost_estimate=pl.CostEstimate(
                flops=8 * share * hd, bytes_accessed=8 << 20, transcendentals=share
            ),
        )(at, *turned_q, *here, *(before or ()))

    shards = [packed]
    a = b = packed
    kept = []
    for s in range(1, n_sp // 2 + 1):
        a = lax.ppermute(a, "sp", right)
        shards.append(a)
        if len(shards) < n_sp:
            b = lax.ppermute(b, "sp", left)
            shards.append(b)
        if s == n_sp // 4:
            a, b, *turned_q = lax.optimization_barrier((a, b, *turned_q))
        if s in (n_sp // 4, n_sp // 4 + 1):
            kept.append(attend(shards[: n_sp // 2], len(kept) * (n_x // 2), n_x // 2, None))
        if s in (n_sp // 4 + 1, n_sp // 4 + 2):
            a, b, kept[s - n_sp // 4 - 1] = lax.optimization_barrier((a, b, kept[s - n_sp // 4 - 1]))
    a, *out_pieces = lax.optimization_barrier((a, *out_pieces))
    keep, away = attend(shards[n_sp // 2 : -1] + [a], 0, n_x, kept)
    merged = pl.pallas_call(
        functools.partial(merge_kernel, rows),
        out_shape=[jax.ShapeDtypeStruct((rows + tail, hd), BF16)] * n_x,
        compiler_params=vmem(16 << 20),
        name="merge",
    )(keep, other_core(away))
    seen = [merged[0], up_x(merged[1]), far_x(merged[2]), down_x(merged[3])]
    seen_at = [(x + n_x - k) % n_x for k in range(n_x)]
    whole = pl.BlockSpec(memory_space=pltpu.VMEM)
    stream, normed = pl.pallas_call(
        functools.partial(mix_kernel, group, n_x, len(out_pieces)),
        out_shape=[jax.ShapeDtypeStruct((own, model), BF16)] * 2,
        in_specs=[pl.BlockSpec(memory_space=pltpu.SMEM)] + [whole] * 3 + [anywhere] * (n_x + len(out_pieces)),
        scratch_shapes=[
            pltpu.VMEM((n_x, rows + tail, hd), BF16),
            pltpu.VMEM((own, HEADS * hd), BF16),
            pltpu.VMEM((HEADS * hd, model), BF16),
            pltpu.SemaphoreType.DMA((n_x,)),
            pltpu.SemaphoreType.DMA((len(out_pieces),)),
        ],
        compiler_params=vmem(),
        cost_estimate=pl.CostEstimate(
            flops=2 * own * HEADS * hd * model, bytes_accessed=6 << 20, transcendentals=0
        ),
        name="mix",
    )(
        jnp.stack(out_at + seen_at).astype(jnp.int32),
        residual,
        mix_gain[None],
        ffn_gain[None],
        *seen,
        *out_pieces,
    )

    token_pieces, token_at = gathered(normed)
    first = last_row = None
    for p, r in zip(token_pieces, token_at):
        f = jnp.where(r == 0, p[:1], 0)
        e = jnp.where(r + p.shape[0] == tok, p[-1:], 0)
        first = f if first is None else first + f
        last_row = e if last_row is None else last_row + e
    before = lax.ppermute(last_row, "sp", [(i, i + 1) for i in range(n_sp - 1)])
    after = lax.ppermute(first, "sp", [(i + 1, i) for i in range(n_sp - 1)])
    block = 128
    blocks = -(-units // block)

    def by_block(taps):
        wide = jnp.pad(taps, ((0, 5), (0, blocks * block - units)))
        return jnp.transpose(wide.reshape(8, blocks, block), (1, 0, 2))

    taps = jnp.concatenate([by_block(conv_gate), by_block(conv_value)], axis=2)
    slots = []
    for k in range(n_x):
        to = ((x + k) % n_x) * 2
        slots += [(to + core) * own, (to + 1 - core) * own]
    where = jnp.stack(token_at + slots).astype(jnp.int32)
    keep, away = pl.pallas_call(
        functools.partial(ffn_kernel, len(token_pieces)),
        out_shape=[jax.ShapeDtypeStruct((n_x, own, model), BF16)] * 2,
        in_specs=[pl.BlockSpec(memory_space=pltpu.SMEM)]
        + [whole] * 3
        + [anywhere] * (1 + len(token_pieces)),
        out_specs=[anywhere, anywhere],
        scratch_shapes=[
            pltpu.VMEM((tok + 16, model), BF16),
            pltpu.VMEM((n_sp, blocks * block, hd), BF16),
            pltpu.VMEM((n_sp, blocks * block, hd), BF16),
            pltpu.VMEM((n_sp, units, hd), BF16),
            pltpu.VMEM((tok + 16, 2 * block), F32),
            pltpu.VMEM((tok + 16, 2 * block), F32),
            pltpu.VMEM((tok, blocks * block), BF16),
            pltpu.VMEM((tok, model), BF16),
            pltpu.SemaphoreType.DMA((len(token_pieces),)),
            pltpu.SemaphoreType.DMA((blocks,)),
            pltpu.SemaphoreType.DMA((blocks,)),
            pltpu.SemaphoreType.DMA,
            pltpu.SemaphoreType.DMA((2 * n_x,)),
        ],
        compiler_params=vmem(56 << 20),
        cost_estimate=pl.CostEstimate(
            flops=6 * tok * units * model, bytes_accessed=16 << 20, transcendentals=tok * units
        ),
        name="ffn",
    )(where, before, after, taps, gate_rows, *token_pieces)
    near = other_core(away)
    total = [keep[k].astype(F32) + near[k].astype(F32) for k in range(n_x)]
    one = up_x(total[1].astype(BF16))
    two = far_x(total[2].astype(BF16))
    three = down_x(total[3].astype(BF16))
    out = total[0] + one.astype(F32) + two.astype(F32) + three.astype(F32)
    return (stream.astype(F32) + out).astype(BF16)


def solution(mesh):
    return jax.shard_map(
        body,
        mesh=mesh,
        in_specs=(
            P(("grp", "sp"), "tp"),
            P(("grp", "sp"), None),
            P(("grp", "sp"), None),
            P(),
            P(),
            P(("grp", "sp", "tp"), None),
            P("tp", None),
            P(),
            P(),
            P("sp", "tp"),
            P("sp", "tp"),
            P(None, "tp"),
            P(None, "tp"),
            P("sp", "tp"),
        ),
        out_specs=P(("grp", "sp", "tp"), None),
        check_vma=False,
    )
```

```python
import functools
import numpy as np
import jax
import jax.numpy as jnp
from jax import lax
from jax.experimental import pallas as pl
from jax.experimental.pallas import tpu as pltpu
from jax.sharding import PartitionSpec as P

HEADS = 8
KVH = 2
GRID_W = 64
EPSILON = 1e-06
THETA = 10000.0
F32 = jnp.float32
BF16 = jnp.bfloat16
NT = (((1,), (1,)), ((), ()))


def rotary_parts(seq_total, head_dim):
    quarter = head_dim // 4
    inverse = THETA ** (-(2.0 * np.arange(quarter, dtype=np.float32)) / np.float32(head_dim // 2))
    inverse = inverse.astype(np.float32)
    rows = seq_total // GRID_W
    row_angle = (np.arange(rows) - rows // 2).astype(np.float32)[:, None] * inverse
    col_angle = (np.arange(GRID_W) - GRID_W // 2).astype(np.float32)[:, None] * inverse

    def lanes(angle, first):
        zero = np.zeros_like(angle)
        cos, sin = np.cos(angle.astype(np.float64)), np.sin(angle.astype(np.float64))
        cos, sin = [cos, cos], [-sin, sin]
        pad = [zero, zero]
        parts = (cos + pad if first else pad + cos) + (sin + pad if first else pad + sin)
        return np.concatenate(parts, axis=-1).astype(np.float32)

    return lanes(row_angle, True), lanes(col_angle, False)


def turned(raw, gain, cos, sin, factor):
    x = raw.astype(F32)
    head_dim = x.shape[-1]
    quarter = head_dim // 4
    normed = x * lax.rsqrt(jnp.mean(x * x, axis=-1, keepdims=True) + EPSILON) * gain
    lane = lax.broadcasted_iota(jnp.int32, x.shape, 1)
    other = jnp.where(
        (lane & quarter) == 0,
        pltpu.roll(normed, head_dim - quarter, 1),
        pltpu.roll(normed, quarter, 1),
    )
    return ((normed * cos + other * sin) * factor).astype(BF16)


def key_kernel(at_ref, k_ref, v_ref, gain_ref, row_ref, col_ref, out_ref):
    part, hd = k_ref.shape
    count = part // GRID_W
    for i in range(count):
        rows = pl.ds(i * GRID_W, GRID_W)
        table = row_ref[0, pl.ds(at_ref[0] * count + i, 1), :] + col_ref[...]
        out_ref[rows, :] = turned(k_ref[rows, :], gain_ref[...], table[:, :hd], table[:, hd:], 1.0)
    out_ref[pl.ds(part, part), :] = v_ref[...]


def query_kernel(at_ref, raw_ref, gain_ref, row_ref, col_ref, out_ref):
    hd = raw_ref.shape[1]
    for i in range(raw_ref.shape[0] // GRID_W):
        table = row_ref[0, pl.ds(i, 1), :] + col_ref[...]
        rows = pl.ds(i * GRID_W, GRID_W)
        out_ref[rows, :] = turned(
            raw_ref[rows, :], gain_ref[...], table[:, :hd], table[:, hd:], hd ** (-0.5)
        )


def as_row(col, eye):
    return jnp.sum(jnp.where(eye, col, 0.0), axis=0, keepdims=True)


def as_col(row, eye):
    return jnp.sum(jnp.where(eye, row, 0.0), axis=1, keepdims=True)


def square_eye(n):
    return lax.broadcasted_iota(jnp.int32, (n, n), 0) == lax.broadcasted_iota(jnp.int32, (n, n), 1)


def stats_rows(col, eye, tail):
    hd = eye.shape[0]
    rows = [as_row(col[b * hd : (b + 1) * hd], eye) for b in range(col.shape[0] // hd)]
    left = jnp.concatenate(rows + [jnp.zeros((8 - len(rows), hd), F32)], axis=0)
    high = left.astype(BF16).astype(F32)
    left = left - high
    mid = left.astype(BF16).astype(F32)
    return jnp.concatenate([high, mid, left - mid, jnp.zeros((tail - 24, hd), F32)], axis=0).astype(BF16)


def stats_col(block, eye, count):
    block = block.astype(F32)
    block = block[0:8] + block[8:16] + block[16:24]
    return jnp.concatenate([as_col(block[b : b + 1], eye) for b in range(count)], axis=0)


def attend_kernel(shards, heads, own, base, last, at_ref, *refs):
    q_in, refs = refs[:heads], refs[heads:]
    kv, refs = refs[:shards], refs[shards:]
    if last:
        before, refs = refs[:2], refs[2:]
        outs, (q_ref, sem) = refs[:2], refs[2:]
    else:
        out_ref, q_ref, sem = refs
    core, slot0 = at_ref[3], at_ref[0]
    step = pl.program_id(0) + base
    hd = q_ref.shape[2]
    half = hd // 2
    rows = heads * own
    part = kv[0].shape[0] // 2

    @pl.when(pl.program_id(0) == 0)
    def _():
        copies = []
        for k in range(heads):
            copies.append(pltpu.make_async_copy(q_in[k], q_ref.at[slot0 ^ k], sem.at[k]))
        for c in copies:
            c.start()
        for c in copies:
            c.wait()

    keys = jnp.concatenate([r[pl.ds(0, part), :] for r in kv], axis=0)
    vals = jnp.concatenate([r[pl.ds(part, part), :] for r in kv], axis=0)
    eye = square_eye(hd)
    todo = [(p, h) for p in range(2) for h in range(0, heads, 2)]
    size = 2 * own

    def score(p, h):
        start = pl.multiple_of((2 * step + (core ^ p)) * own, 32)
        q = jnp.concatenate([q_ref[h + i, pl.ds(start, own), :] for i in range(2)], axis=0)
        return lax.dot_general(q, keys, NT, preferred_element_type=F32)

    lse = [[], []]
    ahead = score(*todo[0])
    for i, (p, h) in enumerate(todo):
        s = ahead
        if i + 1 < len(todo):
            ahead = score(*todo[i + 1])
        here = pl.ds(h * own, size)
        there = pl.ds(rows + h * own, size)
        m = jnp.max(s, axis=1, keepdims=True)
        if last:
            early = step < pl.num_programs(0) // 2
            stats = jnp.where(early, before[0][0, p, there, :], before[1][0, p, there, :])
            m_old, den_old = stats[:, 0:1], stats[:, half : half + 1]
            m = jnp.maximum(m, m_old)
        e = jnp.exp(s - m)
        den = jnp.sum(e, axis=1, keepdims=True)
        acc = jnp.dot(e.astype(BF16), vals, preferred_element_type=F32)
        if last:
            fade = jnp.exp(m_old - m)
            den = den + den_old * fade
            acc = acc + jnp.where(early, before[0][0, p, here, :], before[1][0, p, here, :]) * fade
            outs[p][0, here, :] = (acc / den).astype(BF16)
            lse[p].append(m + jnp.log(den))
        else:
            out_ref[0, p, here, :] = acc
            lane = lax.broadcasted_iota(jnp.int32, (size, hd), 1)
            out_ref[0, p, there, :] = jnp.where(lane < half, m, den)
    if last:
        tail = outs[0].shape[1] - rows
        for p in range(2):
            outs[p][0, pl.ds(rows, tail), :] = stats_rows(jnp.concatenate(lse[p], axis=0), eye, tail)


def merge_kernel(rows, a_ref, b_ref, *out_refs):
    hd = a_ref.shape[2]
    tail = a_ref.shape[1] - rows
    eye = square_eye(hd)
    for k, out_ref in enumerate(out_refs):
        la = stats_col(a_ref[k, pl.ds(rows, tail), :], eye, rows // hd)
        lb = stats_col(b_ref[k, pl.ds(rows, tail), :], eye, rows // hd)
        top = jnp.maximum(la, lb)
        wa, wb = jnp.exp(la - top), jnp.exp(lb - top)
        total = wa + wb
        a = a_ref[k, pl.ds(0, rows), :].astype(F32)
        b = b_ref[k, pl.ds(0, rows), :].astype(F32)
        out_ref[pl.ds(0, rows), :] = (a * (wa / total) + b * (wb / total)).astype(BF16)
        out_ref[pl.ds(rows, tail), :] = stats_rows(top + jnp.log(total), eye, tail)


def normalised(x, gain):
    return x * lax.rsqrt(jnp.mean(x * x, axis=-1, keepdims=True) + EPSILON) * gain


def mix_kernel(group, chips, pieces, at_ref, res_ref, mg_ref, fg_ref, *refs):
    seen, refs = refs[:chips], refs[chips:]
    parts, refs = refs[:pieces], refs[pieces:]
    stream_ref, normed_ref, in_ref, att_ref, w_ref, sem_in, sem = refs
    arrive = []
    for i, one in enumerate(seen):
        arrive.append(pltpu.make_async_copy(one, in_ref.at[at_ref[pieces + i]], sem_in.at[i]))
    copies = []
    for i, part in enumerate(parts):
        size = part.shape[0]
        start = pl.multiple_of(at_ref[i], size)
        copies.append(pltpu.make_async_copy(part, w_ref.at[pl.ds(start, size), :], sem.at[i]))
    for c in arrive + copies:
        c.start()
    for c in arrive:
        c.wait()
    hd = in_ref.shape[2]
    toks = res_ref.shape[0]
    rows = group * toks
    tail = in_ref.shape[1] - rows
    splits = chips // KVH
    eye = square_eye(hd)
    for kv in range(KVH):
        cols = [stats_col(in_ref[kv * splits + j, pl.ds(rows, tail), :], eye, rows // hd) for j in range(splits)]
        top = functools.reduce(jnp.maximum, cols)
        w = [jnp.exp(x - top) for x in cols]
        total = functools.reduce(jnp.add, w)
        acc = None
        for j in range(splits):
            term = (w[j] / total) * in_ref[kv * splits + j, pl.ds(0, rows), :].astype(F32)
            acc = term if acc is None else acc + term
        acc = acc.astype(BF16)
        for h in range(group):
            c = (kv * group + h) * hd
            att_ref[:, c : c + hd] = acc[h * toks : (h + 1) * toks]
    for c in copies:
        c.wait()
    mix = jnp.dot(att_ref[...], w_ref[...], preferred_element_type=F32)
    stream = (res_ref[...].astype(F32) + normalised(mix, mg_ref[...])).astype(BF16)
    stream_ref[...] = stream
    normed_ref[...] = normalised(stream.astype(F32), fg_ref[...]).astype(BF16)


def gelu(v):
    return 0.5 * v * (1.0 + jnp.tanh(0.7978845608028654 * (v + 0.044715 * v * v * v)))


def ffn_kernel(pieces, at_ref, first_ref, last_ref, taps_ref, all_ref, *refs):
    toks_in, refs = refs[:pieces], refs[pieces:]
    keep_ref, send_ref, x_ref, g_ref, v_ref, d_ref, even_ref, odd_ref, h_ref, p_ref = refs[:10]
    sem_x, sem_g, sem_v, sem_d, sem_o = refs[10:]
    edge = 16
    main = x_ref.shape[0] - edge
    units = d_ref.shape[1]
    shards = d_ref.shape[0]
    block = taps_ref.shape[2] // 2
    blocks = taps_ref.shape[0]

    def token_copy(i):
        size = toks_in[i].shape[0]
        start = pl.multiple_of(at_ref[i], 16)
        return pltpu.make_async_copy(toks_in[i], x_ref.at[pl.ds(start, size), :], sem_x.at[i])

    def rows_copy(b, base, ref, sem):
        start = pl.multiple_of(b * block, block)
        return pltpu.make_async_copy(
            all_ref.at[:, pl.ds(base + start, block), :], ref.at[:, pl.ds(start, block), :], sem.at[b]
        )

    def gate_copy(b):
        return rows_copy(b, 0, g_ref, sem_g)

    def value_copy(b):
        return rows_copy(b, units, v_ref, sem_v)

    down = pltpu.make_async_copy(all_ref.at[:, pl.ds(2 * units, units), :], d_ref, sem_d)
    for i in range(pieces):
        token_copy(i).start()
    for b in range(blocks):
        gate_copy(b).start()
        value_copy(b).start()
    down.start()
    row = lax.broadcasted_iota(jnp.int32, (edge, x_ref.shape[1]), 0)
    halo = jnp.where(row == 0, first_ref[...].astype(F32), 0.0)
    halo = jnp.where(row == 1, last_ref[...].astype(F32), halo)
    x_ref[pl.ds(main, edge), :] = halo.astype(BF16)
    for i in range(pieces):
        token_copy(i).wait()

    def arrive(b):
        gate_copy(b).wait()
        value_copy(b).wait()

    def up(b, out_ref):
        rows = pl.ds(b * block, block)
        w = [
            jnp.concatenate([ref[s, rows, :] for s in range(shards)], axis=1) for ref in (g_ref, v_ref)
        ]
        w = jnp.concatenate(w, axis=0)
        y = lax.dot_general(x_ref[...], w, NT, preferred_element_type=F32)
        out_ref[...] = y.astype(BF16).astype(F32)

    def finish(b, in_ref):
        now = in_ref[pl.ds(0, main), :]
        row = lax.broadcasted_iota(jnp.int32, now.shape, 0)
        before = jnp.where(row == 0, in_ref[main : main + 1, :], pltpu.roll(now, 1, 0))
        after = jnp.where(row == main - 1, in_ref[main + 1 : main + 2, :], pltpu.roll(now, main - 1, 0))
        taps = taps_ref[b]
        mixed = taps[0:1] * before + taps[1:2] * now + taps[2:3] * after
        h_ref[:, pl.ds(b * block, block)] = (gelu(mixed[:, :block]) * mixed[:, block:]).astype(BF16)

    arrive(0)
    up(0, even_ref)

    def pair(i, unused):
        b = pl.multiple_of(2 * i, 2)
        arrive(b + 1)
        arrive(b + 2)
        up(b + 1, odd_ref)
        finish(b, even_ref)
        up(b + 2, even_ref)
        finish(b + 1, odd_ref)
        return unused

    lax.fori_loop(0, blocks // 2 - 1, pair, 0)
    arrive(blocks - 1)
    up(blocks - 1, odd_ref)
    finish(blocks - 2, even_ref)
    finish(blocks - 1, odd_ref)
    down.wait()

    def down_block(n, unused):
        w = jnp.concatenate([d_ref[4 * n + i] for i in range(4)], axis=1)
        y = jnp.dot(h_ref[:, :units], w, preferred_element_type=F32)
        p_ref[:, pl.ds(pl.multiple_of(n * 512, 512), 512)] = y.astype(BF16)
        return unused

    lax.fori_loop(0, shards // 4, down_block, 0)
    count, own = keep_ref.shape[0], keep_ref.shape[1]
    outs = []
    for k in range(count):
        for o, ref in enumerate((keep_ref, send_ref)):
            start = pl.multiple_of(at_ref[pieces + 2 * k + o], 16)
            outs.append(
                pltpu.make_async_copy(p_ref.at[pl.ds(start, own), :], ref.at[k], sem_o.at[2 * k + o])
            )
    for c in outs:
        c.start()
    for c in outs:
        c.wait()


def vmem(limit=56 << 20):
    return pltpu.CompilerParams(vmem_limit_bytes=limit)


def body(
    queries,
    keys,
    values,
    query_gain,
    key_gain,
    residual,
    out_weight,
    mix_gain,
    ffn_gain,
    gate_in,
    value_in,
    conv_gate,
    conv_value,
    down_t,
):
    tok = queries.shape[0]
    hd = query_gain.shape[0]
    n_sp, n_tp = lax.axis_size("sp"), lax.axis_size("tp")
    n_x = n_tp // 2
    group = HEADS // KVH
    splits = n_tp // KVH
    part = tok // splits
    own = tok // n_tp
    model = residual.shape[1]
    units = gate_in.shape[1]
    tp, sp = lax.axis_index("tp"), lax.axis_index("sp")
    kv_head, piece = tp // splits, tp % splits
    x, core = tp // 2, tp % 2

    def send(array, change):
        return lax.ppermute(array, "tp", [(i, change(i)) for i in range(n_tp)])

    def other_core(array):
        return send(array, lambda i: i ^ 1)

    def up_x(array):
        return send(array, lambda i: (i + 2) % n_tp)

    def down_x(array):
        return send(array, lambda i: (i - 2) % n_tp)

    def far_x(array):
        return send(array, lambda i: (i + n_x) % n_tp)

    def gathered(mine, direct=False):
        size = mine.shape[0]
        half = size // 2
        a = up_x(mine)
        b = down_x(mine)
        near = other_core(mine)
        if direct:
            pieces = [(mine, tp), (near, tp ^ 1)]
            far = far_x(mine)
            for array, shift in ((a, n_x - 1), (b, 1), (far, n_x // 2)):
                base = ((x + shift) % n_x) * 2
                across = other_core(array)
                pieces += [(array, base + core), (across, base + 1 - core)]
            return [p[0] for p in pieces], [p[1] * size for p in pieces]
        c = up_x(a[:half])
        d = down_x(b[half:])
        low, high = ((x + n_x - 1) % n_x) * 2, ((x + 1) % n_x) * 2
        far = (tp + n_x) % n_tp
        found = [(mine, tp * size), (near, (tp ^ 1) * size)]
        for array, base in ((a, low), (b, high)):
            across = other_core(array)
            found.append((array, (base + core) * size))
            found.append((across, (base + 1 - core) * size))
        for array, shift in ((c, 0), (d, half)):
            found.append((array, far * size + shift))
            found.append((other_core(array), (far ^ 1) * size + shift))
        return [f[0] for f in found], [f[1] for f in found]

    row_np, col_np = rotary_parts(tok * n_sp, hd)
    row_np = row_np.reshape(n_sp, tok // GRID_W, 2 * hd)
    rows_all, cols_all = jnp.asarray(row_np), jnp.asarray(col_np)
    at = jnp.stack([piece, kv_head, sp, core, x]).astype(jnp.int32)
    packed_rows = 2 * part
    packed = pl.pallas_call(
        key_kernel,
        out_shape=jax.ShapeDtypeStruct((packed_rows, hd), BF16),
        grid_spec=pltpu.PrefetchScalarGridSpec(
            num_scalar_prefetch=1,
            grid=(1,),
            in_specs=[
                pl.BlockSpec((part, hd), lambda i, a: (a[0], a[1])),
                pl.BlockSpec((part, hd), lambda i, a: (a[0], a[1])),
                pl.BlockSpec((1, hd), lambda i, a: (0, 0)),
                pl.BlockSpec((1,) + row_np.shape[1:], lambda i, a: (a[2], 0, 0)),
                pl.BlockSpec(col_np.shape, lambda i, a: (0, 0)),
            ],
            out_specs=pl.BlockSpec((packed_rows, hd), lambda i, a: (0, 0)),
        ),
        name="key_prep",
    )(at, keys, values, key_gain[None], rows_all, cols_all)
    weights = jnp.concatenate([gate_in.T, value_in.T, down_t.T], axis=0)
    gate_rows = lax.all_gather(weights, "sp", axis=0, tiled=False)

    mine = pl.pallas_call(
        query_kernel,
        out_shape=jax.ShapeDtypeStruct((tok, hd), BF16),
        grid_spec=pltpu.PrefetchScalarGridSpec(
            num_scalar_prefetch=1,
            grid=(1,),
            in_specs=[
                pl.BlockSpec((tok, hd), lambda i, a: (0, 0)),
                pl.BlockSpec((1, hd), lambda i, a: (0, 0)),
                pl.BlockSpec((1,) + row_np.shape[1:], lambda i, a: (a[2], 0, 0)),
                pl.BlockSpec(col_np.shape, lambda i, a: (0, 0)),
            ],
            out_specs=pl.BlockSpec((tok, hd), lambda i, a: (0, 0)),
        ),
        name="query_prep",
    )(at, queries, query_gain[None], rows_all, cols_all)
    pair = send(mine, lambda i: i ^ 2)
    turned_q = [mine, other_core(mine), pair, other_core(pair)]
    rows = group * own

    out_pieces, out_at = gathered(out_weight, direct=True)

    packed, queries, out_weight = lax.optimization_barrier((packed, queries, out_weight))
    right = [(i, (i + 1) % n_sp) for i in range(n_sp)]
    left = [(i, (i - 1) % n_sp) for i in range(n_sp)]
    tail = 32
    anywhere = pl.BlockSpec(memory_space=pl.ANY)

    def attend(here, base, steps, before):
        last = before is not None
        if last:
            shape = (n_x, rows + tail, hd)
            out_shape = [jax.ShapeDtypeStruct(shape, BF16)] * 2
            out_specs = [pl.BlockSpec((1,) + shape[1:], lambda i, a: (lax.rem(i + n_x - a[4], n_x), 0, 0))] * 2
        else:
            shape = (steps, 2, 2 * rows, hd)
            out_shape = jax.ShapeDtypeStruct(shape, F32)
            out_specs = pl.BlockSpec((1,) + shape[1:], lambda i, a: (i, 0, 0, 0))
        in_specs = [anywhere] * group + [pl.BlockSpec((2 * part, hd), lambda i, a: (0, 0))] * len(here)
        if last:
            kept = (1, 2, 2 * rows, hd)
            in_specs.append(pl.BlockSpec(kept, lambda i, a: (lax.min(i, n_x // 2 - 1), 0, 0, 0)))
            in_specs.append(pl.BlockSpec(kept, lambda i, a: (lax.max(i - n_x // 2, 0), 0, 0, 0)))
        share = group * tok * part * len(here) * steps // n_x
        return pl.pallas_call(
            functools.partial(attend_kernel, len(here), group, own, base, last),
            out_shape=out_shape,
            grid_spec=pltpu.PrefetchScalarGridSpec(
                num_scalar_prefetch=1,
                grid=(steps,),
                in_specs=in_specs,
                out_specs=out_specs,
                scratch_shapes=[pltpu.VMEM((group, tok, hd), BF16), pltpu.SemaphoreType.DMA((group,))],
            ),
            compiler_params=vmem(),
            cost_estimate=pl.CostEstimate(
                flops=8 * share * hd, bytes_accessed=8 << 20, transcendentals=share
            ),
        )(at, *turned_q, *here, *(before or ()))

    shards = [packed]
    a = b = packed
    kept = []
    for s in range(1, n_sp // 2 + 1):
        a = lax.ppermute(a, "sp", right)
        shards.append(a)
        if len(shards) < n_sp:
            b = lax.ppermute(b, "sp", left)
            shards.append(b)
        if s == n_sp // 4:
            a, b, *turned_q = lax.optimization_barrier((a, b, *turned_q))
        if s in (n_sp // 4, n_sp // 4 + 1):
            kept.append(attend(shards[: n_sp // 2], len(kept) * (n_x // 2), n_x // 2, None))
        if s in (n_sp // 4 + 1, n_sp // 4 + 2):
            a, b, kept[s - n_sp // 4 - 1] = lax.optimization_barrier((a, b, kept[s - n_sp // 4 - 1]))
    keep, away = attend(shards[n_sp // 2 : -1] + [a], 0, n_x, kept)
    merged = pl.pallas_call(
        functools.partial(merge_kernel, rows),
        out_shape=[jax.ShapeDtypeStruct((rows + tail, hd), BF16)] * n_x,
        compiler_params=vmem(16 << 20),
        name="merge",
    )(keep, other_core(away))
    one = up_x(merged[1])
    two = far_x(merged[2])
    three = down_x(merged[3])
    seen = [merged[0], one, two, three]
    seen_at = [(x + n_x - k) % n_x for k in range(n_x)]
    whole = pl.BlockSpec(memory_space=pltpu.VMEM)
    stream, normed = pl.pallas_call(
        functools.partial(mix_kernel, group, n_x, len(out_pieces)),
        out_shape=[jax.ShapeDtypeStruct((own, model), BF16)] * 2,
        in_specs=[pl.BlockSpec(memory_space=pltpu.SMEM)] + [whole] * 3 + [anywhere] * (n_x + len(out_pieces)),
        scratch_shapes=[
            pltpu.VMEM((n_x, rows + tail, hd), BF16),
            pltpu.VMEM((own, HEADS * hd), BF16),
            pltpu.VMEM((HEADS * hd, model), BF16),
            pltpu.SemaphoreType.DMA((n_x,)),
            pltpu.SemaphoreType.DMA((len(out_pieces),)),
        ],
        compiler_params=vmem(),
        cost_estimate=pl.CostEstimate(
            flops=2 * own * HEADS * hd * model, bytes_accessed=6 << 20, transcendentals=0
        ),
        name="mix",
    )(
        jnp.stack(out_at + seen_at).astype(jnp.int32),
        residual,
        mix_gain[None],
        ffn_gain[None],
        *seen,
        *out_pieces,
    )

    token_pieces, token_at = gathered(normed)
    first = last_row = None
    for p, r in zip(token_pieces, token_at):
        f = jnp.where(r == 0, p[:1], 0)
        e = jnp.where(r + p.shape[0] == tok, p[-1:], 0)
        first = f if first is None else first + f
        last_row = e if last_row is None else last_row + e
    before = lax.ppermute(last_row, "sp", [(i, i + 1) for i in range(n_sp - 1)])
    after = lax.ppermute(first, "sp", [(i + 1, i) for i in range(n_sp - 1)])
    block = 128
    blocks = -(-units // block)

    def by_block(taps):
        wide = jnp.pad(taps, ((0, 5), (0, blocks * block - units)))
        return jnp.transpose(wide.reshape(8, blocks, block), (1, 0, 2))

    taps = jnp.concatenate([by_block(conv_gate), by_block(conv_value)], axis=2)
    slots = []
    for k in range(n_x):
        to = ((x + k) % n_x) * 2
        slots += [(to + core) * own, (to + 1 - core) * own]
    where = jnp.stack(token_at + slots).astype(jnp.int32)
    keep, away = pl.pallas_call(
        functools.partial(ffn_kernel, len(token_pieces)),
        out_shape=[jax.ShapeDtypeStruct((n_x, own, model), BF16)] * 2,
        in_specs=[pl.BlockSpec(memory_space=pltpu.SMEM)]
        + [whole] * 3
        + [anywhere] * (1 + len(token_pieces)),
        out_specs=[anywhere, anywhere],
        scratch_shapes=[
            pltpu.VMEM((tok + 16, model), BF16),
            pltpu.VMEM((n_sp, blocks * block, hd), BF16),
            pltpu.VMEM((n_sp, blocks * block, hd), BF16),
            pltpu.VMEM((n_sp, units, hd), BF16),
            pltpu.VMEM((tok + 16, 2 * block), F32),
            pltpu.VMEM((tok + 16, 2 * block), F32),
            pltpu.VMEM((tok, blocks * block), BF16),
            pltpu.VMEM((tok, model), BF16),
            pltpu.SemaphoreType.DMA((len(token_pieces),)),
            pltpu.SemaphoreType.DMA((blocks,)),
            pltpu.SemaphoreType.DMA((blocks,)),
            pltpu.SemaphoreType.DMA,
            pltpu.SemaphoreType.DMA((2 * n_x,)),
        ],
        compiler_params=vmem(56 << 20),
        cost_estimate=pl.CostEstimate(
            flops=6 * tok * units * model, bytes_accessed=16 << 20, transcendentals=tok * units
        ),
        name="ffn",
    )(where, before, after, taps, gate_rows, *token_pieces)
    near = other_core(away)
    total = [keep[k].astype(F32) + near[k].astype(F32) for k in range(n_x)]
    half = own // 2
    low = up_x(total[2][:half].astype(BF16))
    high = down_x(total[2][half:].astype(BF16))
    direct_high = up_x(total[1][half:].astype(BF16))
    direct_low = down_x(total[3][:half].astype(BF16))
    low = up_x((total[1][:half] + low.astype(F32)).astype(BF16))
    high = down_x((total[3][half:] + high.astype(F32)).astype(BF16))
    ones = jnp.concatenate([low, high], axis=0).astype(F32)
    twos = jnp.concatenate([direct_low, direct_high], axis=0).astype(F32)
    return (stream.astype(F32) + total[0] + ones + twos).astype(BF16)


def solution(mesh):
    return jax.shard_map(
        body,
        mesh=mesh,
        in_specs=(
            P(("grp", "sp"), "tp"),
            P(("grp", "sp"), None),
            P(("grp", "sp"), None),
            P(),
            P(),
            P(("grp", "sp", "tp"), None),
            P("tp", None),
            P(),
            P(),
            P("sp", "tp"),
            P("sp", "tp"),
            P(None, "tp"),
            P(None, "tp"),
            P("sp", "tp"),
        ),
        out_specs=P(("grp", "sp", "tp"), None),
        check_vma=False,
    )
```

```python
import functools
import numpy as np
import jax
import jax.numpy as jnp
from jax import lax
from jax.experimental import pallas as pl
from jax.experimental.pallas import tpu as pltpu
from jax.sharding import PartitionSpec as P

HEADS = 8
KVH = 2
GRID_W = 64
EPSILON = 1e-06
THETA = 10000.0
F32 = jnp.float32
BF16 = jnp.bfloat16
NT = (((1,), (1,)), ((), ()))


def rotary_parts(seq_total, head_dim):
    quarter = head_dim // 4
    inverse = THETA ** (-(2.0 * np.arange(quarter, dtype=np.float32)) / np.float32(head_dim // 2))
    inverse = inverse.astype(np.float32)
    rows = seq_total // GRID_W
    row_angle = (np.arange(rows) - rows // 2).astype(np.float32)[:, None] * inverse
    col_angle = (np.arange(GRID_W) - GRID_W // 2).astype(np.float32)[:, None] * inverse

    def lanes(angle, first):
        zero = np.zeros_like(angle)
        cos, sin = np.cos(angle.astype(np.float64)), np.sin(angle.astype(np.float64))
        cos, sin = [cos, cos], [-sin, sin]
        pad = [zero, zero]
        parts = (cos + pad if first else pad + cos) + (sin + pad if first else pad + sin)
        return np.concatenate(parts, axis=-1).astype(np.float32)

    return lanes(row_angle, True), lanes(col_angle, False)


def turned(raw, gain, cos, sin, factor):
    x = raw.astype(F32)
    head_dim = x.shape[-1]
    quarter = head_dim // 4
    normed = x * lax.rsqrt(jnp.mean(x * x, axis=-1, keepdims=True) + EPSILON) * gain
    lane = lax.broadcasted_iota(jnp.int32, x.shape, 1)
    other = jnp.where(
        (lane & quarter) == 0,
        pltpu.roll(normed, head_dim - quarter, 1),
        pltpu.roll(normed, quarter, 1),
    )
    return ((normed * cos + other * sin) * factor).astype(BF16)


def key_kernel(at_ref, k_ref, v_ref, gain_ref, row_ref, col_ref, out_ref):
    part, hd = k_ref.shape
    count = part // GRID_W
    for i in range(count):
        rows = pl.ds(i * GRID_W, GRID_W)
        table = row_ref[0, pl.ds(at_ref[0] * count + i, 1), :] + col_ref[...]
        out_ref[rows, :] = turned(k_ref[rows, :], gain_ref[...], table[:, :hd], table[:, hd:], 1.0)
    out_ref[pl.ds(part, part), :] = v_ref[...]


def query_kernel(at_ref, raw_ref, gain_ref, row_ref, col_ref, out_ref):
    hd = raw_ref.shape[1]
    for i in range(raw_ref.shape[0] // GRID_W):
        table = row_ref[0, pl.ds(i, 1), :] + col_ref[...]
        rows = pl.ds(i * GRID_W, GRID_W)
        out_ref[rows, :] = turned(
            raw_ref[rows, :], gain_ref[...], table[:, :hd], table[:, hd:], hd ** (-0.5)
        )


def as_row(col, eye):
    return jnp.sum(jnp.where(eye, col, 0.0), axis=0, keepdims=True)


def as_col(row, eye):
    return jnp.sum(jnp.where(eye, row, 0.0), axis=1, keepdims=True)


def square_eye(n):
    return lax.broadcasted_iota(jnp.int32, (n, n), 0) == lax.broadcasted_iota(jnp.int32, (n, n), 1)


def stats_rows(col, eye, tail):
    hd = eye.shape[0]
    rows = [as_row(col[b * hd : (b + 1) * hd], eye) for b in range(col.shape[0] // hd)]
    left = jnp.concatenate(rows + [jnp.zeros((8 - len(rows), hd), F32)], axis=0)
    high = left.astype(BF16).astype(F32)
    left = left - high
    mid = left.astype(BF16).astype(F32)
    return jnp.concatenate([high, mid, left - mid, jnp.zeros((tail - 24, hd), F32)], axis=0).astype(BF16)


def stats_col(block, eye, count):
    block = block.astype(F32)
    block = block[0:8] + block[8:16] + block[16:24]
    return jnp.concatenate([as_col(block[b : b + 1], eye) for b in range(count)], axis=0)


def attend_kernel(shards, heads, own, base, last, at_ref, *refs):
    q_in, refs = refs[:heads], refs[heads:]
    kv, refs = refs[:shards], refs[shards:]
    if last:
        before, refs = refs[:2], refs[2:]
        outs, (q_ref, sem) = refs[:2], refs[2:]
    else:
        out_ref, q_ref, sem = refs
    core, slot0 = at_ref[3], at_ref[0]
    step = pl.program_id(0) + base
    hd = q_ref.shape[2]
    half = hd // 2
    rows = heads * own
    part = kv[0].shape[0] // 2

    @pl.when(pl.program_id(0) == 0)
    def _():
        copies = []
        for k in range(heads):
            copies.append(pltpu.make_async_copy(q_in[k], q_ref.at[slot0 ^ k], sem.at[k]))
        for c in copies:
            c.start()
        for c in copies:
            c.wait()

    keys = jnp.concatenate([r[pl.ds(0, part), :] for r in kv], axis=0)
    vals = jnp.concatenate([r[pl.ds(part, part), :] for r in kv], axis=0)
    eye = square_eye(hd)
    todo = [(p, h) for p in range(2) for h in range(0, heads, 2)]
    size = 2 * own

    def score(p, h):
        start = pl.multiple_of((2 * step + (core ^ p)) * own, 32)
        q = jnp.concatenate([q_ref[h + i, pl.ds(start, own), :] for i in range(2)], axis=0)
        return lax.dot_general(q, keys, NT, preferred_element_type=F32)

    lse = [[], []]
    ahead = score(*todo[0])
    for i, (p, h) in enumerate(todo):
        s = ahead
        if i + 1 < len(todo):
            ahead = score(*todo[i + 1])
        here = pl.ds(h * own, size)
        there = pl.ds(rows + h * own, size)
        m = jnp.max(s, axis=1, keepdims=True)
        if last:
            early = step < pl.num_programs(0) // 2
            stats = jnp.where(early, before[0][0, p, there, :], before[1][0, p, there, :])
            m_old, den_old = stats[:, 0:1], stats[:, half : half + 1]
            m = jnp.maximum(m, m_old)
        e = jnp.exp(s - m)
        den = jnp.sum(e, axis=1, keepdims=True)
        acc = jnp.dot(e.astype(BF16), vals, preferred_element_type=F32)
        if last:
            fade = jnp.exp(m_old - m)
            den = den + den_old * fade
            acc = acc + jnp.where(early, before[0][0, p, here, :], before[1][0, p, here, :]) * fade
            outs[p][0, here, :] = (acc / den).astype(BF16)
            lse[p].append(m + jnp.log(den))
        else:
            out_ref[0, p, here, :] = acc
            lane = lax.broadcasted_iota(jnp.int32, (size, hd), 1)
            out_ref[0, p, there, :] = jnp.where(lane < half, m, den)
    if last:
        tail = outs[0].shape[1] - rows
        for p in range(2):
            outs[p][0, pl.ds(rows, tail), :] = stats_rows(jnp.concatenate(lse[p], axis=0), eye, tail)


def merge_kernel(rows, a_ref, b_ref, *out_refs):
    hd = a_ref.shape[2]
    tail = a_ref.shape[1] - rows
    eye = square_eye(hd)
    for k, out_ref in enumerate(out_refs):
        la = stats_col(a_ref[k, pl.ds(rows, tail), :], eye, rows // hd)
        lb = stats_col(b_ref[k, pl.ds(rows, tail), :], eye, rows // hd)
        top = jnp.maximum(la, lb)
        wa, wb = jnp.exp(la - top), jnp.exp(lb - top)
        total = wa + wb
        a = a_ref[k, pl.ds(0, rows), :].astype(F32)
        b = b_ref[k, pl.ds(0, rows), :].astype(F32)
        out_ref[pl.ds(0, rows), :] = (a * (wa / total) + b * (wb / total)).astype(BF16)
        out_ref[pl.ds(rows, tail), :] = stats_rows(top + jnp.log(total), eye, tail)


def normalised(x, gain):
    return x * lax.rsqrt(jnp.mean(x * x, axis=-1, keepdims=True) + EPSILON) * gain


def mix_kernel(group, chips, pieces, at_ref, res_ref, mg_ref, fg_ref, *refs):
    seen, refs = refs[:chips], refs[chips:]
    parts, refs = refs[:pieces], refs[pieces:]
    stream_ref, normed_ref, in_ref, att_ref, w_ref, sem_in, sem = refs
    arrive = []
    for i, one in enumerate(seen):
        arrive.append(pltpu.make_async_copy(one, in_ref.at[at_ref[pieces + i]], sem_in.at[i]))
    copies = []
    for i, part in enumerate(parts):
        size = part.shape[0]
        start = pl.multiple_of(at_ref[i], size)
        copies.append(pltpu.make_async_copy(part, w_ref.at[pl.ds(start, size), :], sem.at[i]))
    for c in arrive + copies:
        c.start()
    for c in arrive:
        c.wait()
    hd = in_ref.shape[2]
    toks = res_ref.shape[0]
    rows = group * toks
    tail = in_ref.shape[1] - rows
    splits = chips // KVH
    eye = square_eye(hd)
    for kv in range(KVH):
        cols = [stats_col(in_ref[kv * splits + j, pl.ds(rows, tail), :], eye, rows // hd) for j in range(splits)]
        top = functools.reduce(jnp.maximum, cols)
        w = [jnp.exp(x - top) for x in cols]
        total = functools.reduce(jnp.add, w)
        acc = None
        for j in range(splits):
            term = (w[j] / total) * in_ref[kv * splits + j, pl.ds(0, rows), :].astype(F32)
            acc = term if acc is None else acc + term
        acc = acc.astype(BF16)
        for h in range(group):
            c = (kv * group + h) * hd
            att_ref[:, c : c + hd] = acc[h * toks : (h + 1) * toks]
    for c in copies:
        c.wait()
    mix = jnp.dot(att_ref[...], w_ref[...], preferred_element_type=F32)
    stream = (res_ref[...].astype(F32) + normalised(mix, mg_ref[...])).astype(BF16)
    stream_ref[...] = stream
    normed_ref[...] = normalised(stream.astype(F32), fg_ref[...]).astype(BF16)


def gelu(v):
    return 0.5 * v * (1.0 + jnp.tanh(0.7978845608028654 * (v + 0.044715 * v * v * v)))


def ffn_kernel(pieces, at_ref, first_ref, last_ref, taps_ref, all_ref, *refs):
    toks_in, refs = refs[:pieces], refs[pieces:]
    keep_ref, send_ref, x_ref, g_ref, v_ref, d_ref, even_ref, odd_ref, h_ref, p_ref = refs[:10]
    sem_x, sem_g, sem_v, sem_d, sem_o = refs[10:]
    edge = 16
    main = x_ref.shape[0] - edge
    units = d_ref.shape[1]
    shards = d_ref.shape[0]
    block = taps_ref.shape[2] // 2
    blocks = taps_ref.shape[0]

    def token_copy(i):
        size = toks_in[i].shape[0]
        start = pl.multiple_of(at_ref[i], 16)
        return pltpu.make_async_copy(toks_in[i], x_ref.at[pl.ds(start, size), :], sem_x.at[i])

    def rows_copy(b, base, ref, sem):
        start = pl.multiple_of(b * block, block)
        return pltpu.make_async_copy(
            all_ref.at[:, pl.ds(base + start, block), :], ref.at[:, pl.ds(start, block), :], sem.at[b]
        )

    def gate_copy(b):
        return rows_copy(b, 0, g_ref, sem_g)

    def value_copy(b):
        return rows_copy(b, units, v_ref, sem_v)

    down = pltpu.make_async_copy(all_ref.at[:, pl.ds(2 * units, units), :], d_ref, sem_d)
    for i in range(pieces):
        token_copy(i).start()
    gate_copy(0).start()
    value_copy(0).start()
    row = lax.broadcasted_iota(jnp.int32, (edge, x_ref.shape[1]), 0)
    halo = jnp.where(row == 0, first_ref[...].astype(F32), 0.0)
    halo = jnp.where(row == 1, last_ref[...].astype(F32), halo)
    x_ref[pl.ds(main, edge), :] = halo.astype(BF16)
    for i in range(pieces):
        token_copy(i).wait()

    def arrive(b):
        gate_copy(b).wait()
        value_copy(b).wait()

    def up(b, out_ref):
        rows = pl.ds(b * block, block)
        w = [
            jnp.concatenate([ref[s, rows, :] for s in range(shards)], axis=1) for ref in (g_ref, v_ref)
        ]
        w = jnp.concatenate(w, axis=0)
        y = lax.dot_general(x_ref[...], w, NT, preferred_element_type=F32)
        out_ref[...] = y.astype(BF16).astype(F32)

    def finish(b, in_ref):
        now = in_ref[pl.ds(0, main), :]
        row = lax.broadcasted_iota(jnp.int32, now.shape, 0)
        before = jnp.where(row == 0, in_ref[main : main + 1, :], pltpu.roll(now, 1, 0))
        after = jnp.where(row == main - 1, in_ref[main + 1 : main + 2, :], pltpu.roll(now, main - 1, 0))
        taps = taps_ref[b]
        mixed = taps[0:1] * before + taps[1:2] * now + taps[2:3] * after
        h_ref[:, pl.ds(b * block, block)] = (gelu(mixed[:, :block]) * mixed[:, block:]).astype(BF16)

    arrive(0)
    for b in range(1, blocks):
        gate_copy(b).start()
        value_copy(b).start()
    up(0, even_ref)

    def pair(i, unused):
        b = pl.multiple_of(2 * i, 2)
        arrive(b + 1)
        arrive(b + 2)
        up(b + 1, odd_ref)
        finish(b, even_ref)
        up(b + 2, even_ref)
        finish(b + 1, odd_ref)
        return unused

    lax.fori_loop(0, blocks // 2 - 1, pair, 0)
    arrive(blocks - 1)
    down.start()
    up(blocks - 1, odd_ref)
    finish(blocks - 2, even_ref)
    finish(blocks - 1, odd_ref)
    down.wait()

    wide = 512
    parts = x_ref.shape[1] // wide
    count, own = keep_ref.shape[0], keep_ref.shape[1]

    def out_copy(n, k, o):
        start = pl.multiple_of(at_ref[pieces + 2 * k + o], 16)
        cols = pl.ds(pl.multiple_of(n * wide, wide), wide)
        ref = (keep_ref, send_ref)[o]
        return pltpu.make_async_copy(
            p_ref.at[pl.ds(start, own), cols], ref.at[k, :, cols], sem_o.at[n, 2 * k + o]
        )

    def down_block(n, unused):
        w = jnp.concatenate([d_ref[4 * n + i] for i in range(4)], axis=1)
        y = jnp.dot(h_ref[:, :units], w, preferred_element_type=F32)
        p_ref[:, pl.ds(pl.multiple_of(n * wide, wide), wide)] = y.astype(BF16)
        for k in range(count):
            for o in range(2):
                out_copy(n, k, o).start()
        return unused

    lax.fori_loop(0, parts, down_block, 0)

    def out_wait(n, unused):
        for k in range(count):
            for o in range(2):
                out_copy(n, k, o).wait()
        return unused

    lax.fori_loop(0, parts, out_wait, 0)


def vmem(limit=56 << 20):
    return pltpu.CompilerParams(vmem_limit_bytes=limit)


def body(
    queries,
    keys,
    values,
    query_gain,
    key_gain,
    residual,
    out_weight,
    mix_gain,
    ffn_gain,
    gate_in,
    value_in,
    conv_gate,
    conv_value,
    down_t,
):
    tok = queries.shape[0]
    hd = query_gain.shape[0]
    n_sp, n_tp = lax.axis_size("sp"), lax.axis_size("tp")
    n_x = n_tp // 2
    group = HEADS // KVH
    splits = n_tp // KVH
    part = tok // splits
    own = tok // n_tp
    model = residual.shape[1]
    units = gate_in.shape[1]
    tp, sp = lax.axis_index("tp"), lax.axis_index("sp")
    kv_head, piece = tp // splits, tp % splits
    x, core = tp // 2, tp % 2

    def send(array, change):
        return lax.ppermute(array, "tp", [(i, change(i)) for i in range(n_tp)])

    def other_core(array):
        return send(array, lambda i: i ^ 1)

    def up_x(array):
        return send(array, lambda i: (i + 2) % n_tp)

    def down_x(array):
        return send(array, lambda i: (i - 2) % n_tp)

    def far_x(array):
        return send(array, lambda i: (i + n_x) % n_tp)

    def gathered(mine, direct=False):
        size = mine.shape[0]
        half = size // 2
        a = up_x(mine)
        b = down_x(mine)
        near = other_core(mine)
        if direct:
            pieces = [(mine, tp), (near, tp ^ 1)]
            far = far_x(mine)
            for array, shift in ((a, n_x - 1), (b, 1), (far, n_x // 2)):
                base = ((x + shift) % n_x) * 2
                across = other_core(array)
                pieces += [(array, base + core), (across, base + 1 - core)]
            return [p[0] for p in pieces], [p[1] * size for p in pieces]
        c = up_x(a[:half])
        d = down_x(b[half:])
        low, high = ((x + n_x - 1) % n_x) * 2, ((x + 1) % n_x) * 2
        far = (tp + n_x) % n_tp
        found = [(mine, tp * size), (near, (tp ^ 1) * size)]
        for array, base in ((a, low), (b, high)):
            across = other_core(array)
            found.append((array, (base + core) * size))
            found.append((across, (base + 1 - core) * size))
        for array, shift in ((c, 0), (d, half)):
            found.append((array, far * size + shift))
            found.append((other_core(array), (far ^ 1) * size + shift))
        return [f[0] for f in found], [f[1] for f in found]

    row_np, col_np = rotary_parts(tok * n_sp, hd)
    row_np = row_np.reshape(n_sp, tok // GRID_W, 2 * hd)
    rows_all, cols_all = jnp.asarray(row_np), jnp.asarray(col_np)
    at = jnp.stack([piece, kv_head, sp, core, x]).astype(jnp.int32)
    packed_rows = 2 * part
    packed = pl.pallas_call(
        key_kernel,
        out_shape=jax.ShapeDtypeStruct((packed_rows, hd), BF16),
        grid_spec=pltpu.PrefetchScalarGridSpec(
            num_scalar_prefetch=1,
            grid=(1,),
            in_specs=[
                pl.BlockSpec((part, hd), lambda i, a: (a[0], a[1])),
                pl.BlockSpec((part, hd), lambda i, a: (a[0], a[1])),
                pl.BlockSpec((1, hd), lambda i, a: (0, 0)),
                pl.BlockSpec((1,) + row_np.shape[1:], lambda i, a: (a[2], 0, 0)),
                pl.BlockSpec(col_np.shape, lambda i, a: (0, 0)),
            ],
            out_specs=pl.BlockSpec((packed_rows, hd), lambda i, a: (0, 0)),
        ),
        name="key_prep",
    )(at, keys, values, key_gain[None], rows_all, cols_all)
    weights = jnp.concatenate([gate_in.T, value_in.T, down_t.T], axis=0)
    gate_rows = lax.all_gather(weights, "sp", axis=0, tiled=False)

    mine = pl.pallas_call(
        query_kernel,
        out_shape=jax.ShapeDtypeStruct((tok, hd), BF16),
        grid_spec=pltpu.PrefetchScalarGridSpec(
            num_scalar_prefetch=1,
            grid=(1,),
            in_specs=[
                pl.BlockSpec((tok, hd), lambda i, a: (0, 0)),
                pl.BlockSpec((1, hd), lambda i, a: (0, 0)),
                pl.BlockSpec((1,) + row_np.shape[1:], lambda i, a: (a[2], 0, 0)),
                pl.BlockSpec(col_np.shape, lambda i, a: (0, 0)),
            ],
            out_specs=pl.BlockSpec((tok, hd), lambda i, a: (0, 0)),
        ),
        name="query_prep",
    )(at, queries, query_gain[None], rows_all, cols_all)
    pair = send(mine, lambda i: i ^ 2)
    turned_q = [mine, other_core(mine), pair, other_core(pair)]
    rows = group * own

    out_pieces, out_at = gathered(out_weight, direct=True)

    packed, queries, out_weight = lax.optimization_barrier((packed, queries, out_weight))
    right = [(i, (i + 1) % n_sp) for i in range(n_sp)]
    left = [(i, (i - 1) % n_sp) for i in range(n_sp)]
    tail = 32
    anywhere = pl.BlockSpec(memory_space=pl.ANY)

    def attend(here, base, steps, before):
        last = before is not None
        if last:
            shape = (n_x, rows + tail, hd)
            out_shape = [jax.ShapeDtypeStruct(shape, BF16)] * 2
            out_specs = [pl.BlockSpec((1,) + shape[1:], lambda i, a: (lax.rem(i + n_x - a[4], n_x), 0, 0))] * 2
        else:
            shape = (steps, 2, 2 * rows, hd)
            out_shape = jax.ShapeDtypeStruct(shape, F32)
            out_specs = pl.BlockSpec((1,) + shape[1:], lambda i, a: (i, 0, 0, 0))
        in_specs = [anywhere] * group + [pl.BlockSpec((2 * part, hd), lambda i, a: (0, 0))] * len(here)
        if last:
            kept = (1, 2, 2 * rows, hd)
            in_specs.append(pl.BlockSpec(kept, lambda i, a: (lax.min(i, n_x // 2 - 1), 0, 0, 0)))
            in_specs.append(pl.BlockSpec(kept, lambda i, a: (lax.max(i - n_x // 2, 0), 0, 0, 0)))
        share = group * tok * part * len(here) * steps // n_x
        return pl.pallas_call(
            functools.partial(attend_kernel, len(here), group, own, base, last),
            out_shape=out_shape,
            grid_spec=pltpu.PrefetchScalarGridSpec(
                num_scalar_prefetch=1,
                grid=(steps,),
                in_specs=in_specs,
                out_specs=out_specs,
                scratch_shapes=[pltpu.VMEM((group, tok, hd), BF16), pltpu.SemaphoreType.DMA((group,))],
            ),
            compiler_params=vmem(36 << 20),
            cost_estimate=pl.CostEstimate(
                flops=8 * share * hd, bytes_accessed=8 << 20, transcendentals=share
            ),
        )(at, *turned_q, *here, *(before or ()))

    shards = [packed]
    a = b = packed
    kept = []
    for s in range(1, n_sp // 2 + 1):
        a = lax.ppermute(a, "sp", right)
        shards.append(a)
        if len(shards) < n_sp:
            b = lax.ppermute(b, "sp", left)
            shards.append(b)
        if s == n_sp // 4:
            a, b, *turned_q = lax.optimization_barrier((a, b, *turned_q))
        if s in (n_sp // 4, n_sp // 4 + 1):
            kept.append(attend(shards[: n_sp // 2], len(kept) * (n_x // 2), n_x // 2, None))
        if s in (n_sp // 4 + 1, n_sp // 4 + 2):
            a, b, kept[s - n_sp // 4 - 1] = lax.optimization_barrier((a, b, kept[s - n_sp // 4 - 1]))
    keep, away = attend(shards[n_sp // 2 : -1] + [a], 0, n_x, kept)
    merged = pl.pallas_call(
        functools.partial(merge_kernel, rows),
        out_shape=[jax.ShapeDtypeStruct((rows + tail, hd), BF16)] * n_x,
        compiler_params=vmem(16 << 20),
        name="merge",
    )(keep, other_core(away))
    one = up_x(merged[1])
    two = far_x(merged[2])
    three = down_x(merged[3])
    seen = [merged[0], one, two, three]
    seen_at = [(x + n_x - k) % n_x for k in range(n_x)]
    whole = pl.BlockSpec(memory_space=pltpu.VMEM)
    stream, normed = pl.pallas_call(
        functools.partial(mix_kernel, group, n_x, len(out_pieces)),
        out_shape=[jax.ShapeDtypeStruct((own, model), BF16)] * 2,
        in_specs=[pl.BlockSpec(memory_space=pltpu.SMEM)] + [whole] * 3 + [anywhere] * (n_x + len(out_pieces)),
        scratch_shapes=[
            pltpu.VMEM((n_x, rows + tail, hd), BF16),
            pltpu.VMEM((own, HEADS * hd), BF16),
            pltpu.VMEM((HEADS * hd, model), BF16),
            pltpu.SemaphoreType.DMA((n_x,)),
            pltpu.SemaphoreType.DMA((len(out_pieces),)),
        ],
        compiler_params=vmem(),
        cost_estimate=pl.CostEstimate(
            flops=2 * own * HEADS * hd * model, bytes_accessed=6 << 20, transcendentals=0
        ),
        name="mix",
    )(
        jnp.stack(out_at + seen_at).astype(jnp.int32),
        residual,
        mix_gain[None],
        ffn_gain[None],
        *seen,
        *out_pieces,
    )

    token_pieces, token_at = gathered(normed)
    first = last_row = None
    for p, r in zip(token_pieces, token_at):
        f = jnp.where(r == 0, p[:1], 0)
        e = jnp.where(r + p.shape[0] == tok, p[-1:], 0)
        first = f if first is None else first + f
        last_row = e if last_row is None else last_row + e
    before = lax.ppermute(last_row, "sp", [(i, i + 1) for i in range(n_sp - 1)])
    after = lax.ppermute(first, "sp", [(i + 1, i) for i in range(n_sp - 1)])
    block = 128
    blocks = -(-units // block)

    def by_block(taps):
        wide = jnp.pad(taps, ((0, 5), (0, blocks * block - units)))
        return jnp.transpose(wide.reshape(8, blocks, block), (1, 0, 2))

    taps = jnp.concatenate([by_block(conv_gate), by_block(conv_value)], axis=2)
    slots = []
    for k in range(n_x):
        to = ((x + k) % n_x) * 2
        slots += [(to + core) * own, (to + 1 - core) * own]
    where = jnp.stack(token_at + slots).astype(jnp.int32)
    keep, away = pl.pallas_call(
        functools.partial(ffn_kernel, len(token_pieces)),
        out_shape=[jax.ShapeDtypeStruct((n_x, own, model), BF16)] * 2,
        in_specs=[pl.BlockSpec(memory_space=pltpu.SMEM)]
        + [whole] * 3
        + [anywhere] * (1 + len(token_pieces)),
        out_specs=[anywhere, anywhere],
        scratch_shapes=[
            pltpu.VMEM((tok + 16, model), BF16),
            pltpu.VMEM((n_sp, blocks * block, hd), BF16),
            pltpu.VMEM((n_sp, blocks * block, hd), BF16),
            pltpu.VMEM((n_sp, units, hd), BF16),
            pltpu.VMEM((tok + 16, 2 * block), F32),
            pltpu.VMEM((tok + 16, 2 * block), F32),
            pltpu.VMEM((tok, blocks * block), BF16),
            pltpu.VMEM((tok, model), BF16),
            pltpu.SemaphoreType.DMA((len(token_pieces),)),
            pltpu.SemaphoreType.DMA((blocks,)),
            pltpu.SemaphoreType.DMA((blocks,)),
            pltpu.SemaphoreType.DMA,
            pltpu.SemaphoreType.DMA((model // 512, 2 * n_x)),
        ],
        compiler_params=vmem(56 << 20),
        cost_estimate=pl.CostEstimate(
            flops=6 * tok * units * model, bytes_accessed=16 << 20, transcendentals=tok * units
        ),
        name="ffn",
    )(where, before, after, taps, gate_rows, *token_pieces)
    near = other_core(away)
    total = [keep[k].astype(F32) + near[k].astype(F32) for k in range(n_x)]
    half = own // 2
    low = up_x(total[2][:half].astype(BF16))
    high = down_x(total[2][half:].astype(BF16))
    direct_high = up_x(total[1][half:].astype(BF16))
    direct_low = down_x(total[3][:half].astype(BF16))
    low = up_x((total[1][:half] + low.astype(F32)).astype(BF16))
    high = down_x((total[3][half:] + high.astype(F32)).astype(BF16))
    ones = jnp.concatenate([low, high], axis=0).astype(F32)
    twos = jnp.concatenate([direct_low, direct_high], axis=0).astype(F32)
    return (stream.astype(F32) + total[0] + ones + twos).astype(BF16)


def solution(mesh):
    return jax.shard_map(
        body,
        mesh=mesh,
        in_specs=(
            P(("grp", "sp"), "tp"),
            P(("grp", "sp"), None),
            P(("grp", "sp"), None),
            P(),
            P(),
            P(("grp", "sp", "tp"), None),
            P("tp", None),
            P(),
            P(),
            P("sp", "tp"),
            P("sp", "tp"),
            P(None, "tp"),
            P(None, "tp"),
            P("sp", "tp"),
        ),
        out_specs=P(("grp", "sp", "tp"), None),
        check_vma=False,
    )
```

```python
import functools
import numpy as np
import jax
import jax.numpy as jnp
from jax import lax
from jax.experimental import pallas as pl
from jax.experimental.pallas import tpu as pltpu
from jax.sharding import PartitionSpec as P

HEADS = 8
KVH = 2
GRID_W = 64
EPSILON = 1e-06
THETA = 10000.0
F32 = jnp.float32
BF16 = jnp.bfloat16
NT = (((1,), (1,)), ((), ()))


def rotary_parts(seq_total, head_dim):
    quarter = head_dim // 4
    inverse = THETA ** (-(2.0 * np.arange(quarter, dtype=np.float32)) / np.float32(head_dim // 2))
    inverse = inverse.astype(np.float32)
    rows = seq_total // GRID_W
    row_angle = (np.arange(rows) - rows // 2).astype(np.float32)[:, None] * inverse
    col_angle = (np.arange(GRID_W) - GRID_W // 2).astype(np.float32)[:, None] * inverse

    def lanes(angle, first):
        zero = np.zeros_like(angle)
        cos, sin = np.cos(angle.astype(np.float64)), np.sin(angle.astype(np.float64))
        cos, sin = [cos, cos], [-sin, sin]
        pad = [zero, zero]
        parts = (cos + pad if first else pad + cos) + (sin + pad if first else pad + sin)
        return np.concatenate(parts, axis=-1).astype(np.float32)

    return lanes(row_angle, True), lanes(col_angle, False)


def turned(raw, gain, cos, sin, factor):
    x = raw.astype(F32)
    head_dim = x.shape[-1]
    quarter = head_dim // 4
    normed = x * lax.rsqrt(jnp.mean(x * x, axis=-1, keepdims=True) + EPSILON) * gain
    lane = lax.broadcasted_iota(jnp.int32, x.shape, 1)
    other = jnp.where(
        (lane & quarter) == 0,
        pltpu.roll(normed, head_dim - quarter, 1),
        pltpu.roll(normed, quarter, 1),
    )
    return ((normed * cos + other * sin) * factor).astype(BF16)


def key_kernel(at_ref, k_ref, v_ref, gain_ref, row_ref, col_ref, out_ref):
    part, hd = k_ref.shape
    count = part // GRID_W
    for i in range(count):
        rows = pl.ds(i * GRID_W, GRID_W)
        table = row_ref[0, pl.ds(at_ref[0] * count + i, 1), :] + col_ref[...]
        out_ref[rows, :] = turned(k_ref[rows, :], gain_ref[...], table[:, :hd], table[:, hd:], 1.0)
    out_ref[pl.ds(part, part), :] = v_ref[...]


def query_kernel(at_ref, raw_ref, gain_ref, row_ref, col_ref, out_ref):
    hd = raw_ref.shape[1]
    for i in range(raw_ref.shape[0] // GRID_W):
        table = row_ref[0, pl.ds(i, 1), :] + col_ref[...]
        rows = pl.ds(i * GRID_W, GRID_W)
        out_ref[rows, :] = turned(
            raw_ref[rows, :], gain_ref[...], table[:, :hd], table[:, hd:], hd ** (-0.5)
        )


def as_row(col, eye):
    return jnp.sum(jnp.where(eye, col, 0.0), axis=0, keepdims=True)


def as_col(row, eye):
    return jnp.sum(jnp.where(eye, row, 0.0), axis=1, keepdims=True)


def square_eye(n):
    return lax.broadcasted_iota(jnp.int32, (n, n), 0) == lax.broadcasted_iota(jnp.int32, (n, n), 1)


def stats_rows(col, eye, tail):
    hd = eye.shape[0]
    rows = [as_row(col[b * hd : (b + 1) * hd], eye) for b in range(col.shape[0] // hd)]
    left = jnp.concatenate(rows + [jnp.zeros((8 - len(rows), hd), F32)], axis=0)
    high = left.astype(BF16).astype(F32)
    left = left - high
    mid = left.astype(BF16).astype(F32)
    return jnp.concatenate([high, mid, left - mid, jnp.zeros((tail - 24, hd), F32)], axis=0).astype(BF16)


def stats_col(block, eye, count):
    block = block.astype(F32)
    block = block[0:8] + block[8:16] + block[16:24]
    return jnp.concatenate([as_col(block[b : b + 1], eye) for b in range(count)], axis=0)


def attend_kernel(shards, heads, own, base, last, at_ref, *refs):
    q_in, refs = refs[:heads], refs[heads:]
    kv, refs = refs[:shards], refs[shards:]
    if last:
        before, refs = refs[:2], refs[2:]
        outs, (q_ref, sem) = refs[:2], refs[2:]
    else:
        out_ref, q_ref, sem = refs
    core, slot0 = at_ref[3], at_ref[0]
    step = pl.program_id(0) + base
    hd = q_ref.shape[2]
    half = hd // 2
    rows = heads * own
    part = kv[0].shape[0] // 2

    @pl.when(pl.program_id(0) == 0)
    def _():
        copies = []
        for k in range(heads):
            copies.append(pltpu.make_async_copy(q_in[k], q_ref.at[slot0 ^ k], sem.at[k]))
        for c in copies:
            c.start()
        for c in copies:
            c.wait()

    keys = jnp.concatenate([r[pl.ds(0, part), :] for r in kv], axis=0)
    vals = jnp.concatenate([r[pl.ds(part, part), :] for r in kv], axis=0)
    eye = square_eye(hd)
    todo = [(p, h) for p in range(2) for h in range(0, heads, 2)]
    size = 2 * own

    def score(p, h):
        start = pl.multiple_of((2 * step + (core ^ p)) * own, 32)
        q = jnp.concatenate([q_ref[h + i, pl.ds(start, own), :] for i in range(2)], axis=0)
        return lax.dot_general(q, keys, NT, preferred_element_type=F32)

    lse = [[], []]
    ahead = score(*todo[0])
    for i, (p, h) in enumerate(todo):
        s = ahead
        if i + 1 < len(todo):
            ahead = score(*todo[i + 1])
        here = pl.ds(h * own, size)
        there = pl.ds(rows + h * own, size)
        m = jnp.max(s, axis=1, keepdims=True)
        if last:
            early = step < pl.num_programs(0) // 2
            stats = jnp.where(early, before[0][0, p, there, :], before[1][0, p, there, :])
            m_old, den_old = stats[:, 0:1], stats[:, half : half + 1]
            m = jnp.maximum(m, m_old)
        e = jnp.exp(s - m)
        den = jnp.sum(e, axis=1, keepdims=True)
        acc = jnp.dot(e.astype(BF16), vals, preferred_element_type=F32)
        if last:
            fade = jnp.exp(m_old - m)
            den = den + den_old * fade
            acc = acc + jnp.where(early, before[0][0, p, here, :], before[1][0, p, here, :]) * fade
            outs[p][0, here, :] = (acc / den).astype(BF16)
            lse[p].append(m + jnp.log(den))
        else:
            out_ref[0, p, here, :] = acc
            lane = lax.broadcasted_iota(jnp.int32, (size, hd), 1)
            out_ref[0, p, there, :] = jnp.where(lane < half, m, den)
    if last:
        tail = outs[0].shape[1] - rows
        for p in range(2):
            outs[p][0, pl.ds(rows, tail), :] = stats_rows(jnp.concatenate(lse[p], axis=0), eye, tail)


def merge_kernel(rows, a_ref, b_ref, *out_refs):
    hd = a_ref.shape[2]
    tail = a_ref.shape[1] - rows
    eye = square_eye(hd)
    for k, out_ref in enumerate(out_refs):
        la = stats_col(a_ref[k, pl.ds(rows, tail), :], eye, rows // hd)
        lb = stats_col(b_ref[k, pl.ds(rows, tail), :], eye, rows // hd)
        top = jnp.maximum(la, lb)
        wa, wb = jnp.exp(la - top), jnp.exp(lb - top)
        total = wa + wb
        a = a_ref[k, pl.ds(0, rows), :].astype(F32)
        b = b_ref[k, pl.ds(0, rows), :].astype(F32)
        out_ref[pl.ds(0, rows), :] = (a * (wa / total) + b * (wb / total)).astype(BF16)
        out_ref[pl.ds(rows, tail), :] = stats_rows(top + jnp.log(total), eye, tail)


def normalised(x, gain):
    return x * lax.rsqrt(jnp.mean(x * x, axis=-1, keepdims=True) + EPSILON) * gain


def mix_kernel(group, chips, pieces, at_ref, res_ref, mg_ref, fg_ref, *refs):
    seen, refs = refs[:chips], refs[chips:]
    parts, refs = refs[:pieces], refs[pieces:]
    stream_ref, normed_ref, in_ref, att_ref, w_ref, sem_in, sem = refs
    arrive = []
    for i, one in enumerate(seen):
        arrive.append(pltpu.make_async_copy(one, in_ref.at[at_ref[pieces + i]], sem_in.at[i]))
    copies = []
    for i, part in enumerate(parts):
        size = part.shape[0]
        start = pl.multiple_of(at_ref[i], size)
        copies.append(pltpu.make_async_copy(part, w_ref.at[pl.ds(start, size), :], sem.at[i]))
    for c in arrive + copies:
        c.start()
    for c in arrive:
        c.wait()
    hd = in_ref.shape[2]
    toks = res_ref.shape[0]
    rows = group * toks
    tail = in_ref.shape[1] - rows
    splits = chips // KVH
    eye = square_eye(hd)
    for kv in range(KVH):
        cols = [stats_col(in_ref[kv * splits + j, pl.ds(rows, tail), :], eye, rows // hd) for j in range(splits)]
        top = functools.reduce(jnp.maximum, cols)
        w = [jnp.exp(x - top) for x in cols]
        total = functools.reduce(jnp.add, w)
        acc = None
        for j in range(splits):
            term = (w[j] / total) * in_ref[kv * splits + j, pl.ds(0, rows), :].astype(F32)
            acc = term if acc is None else acc + term
        acc = acc.astype(BF16)
        for h in range(group):
            c = (kv * group + h) * hd
            att_ref[:, c : c + hd] = acc[h * toks : (h + 1) * toks]
    for c in copies:
        c.wait()
    mix = jnp.dot(att_ref[...], w_ref[...], preferred_element_type=F32)
    stream = (res_ref[...].astype(F32) + normalised(mix, mg_ref[...])).astype(BF16)
    stream_ref[...] = stream
    normed_ref[...] = normalised(stream.astype(F32), fg_ref[...]).astype(BF16)


def gelu(v):
    return 0.5 * v * (1.0 + jnp.tanh(0.7978845608028654 * (v + 0.044715 * v * v * v)))


def ffn_kernel(pieces, at_ref, first_ref, last_ref, taps_ref, all_ref, *refs):
    toks_in, refs = refs[:pieces], refs[pieces:]
    keep_ref, send_ref, x_ref, g_ref, v_ref, d_ref, even_ref, odd_ref, h_ref, p_ref = refs[:10]
    sem_x, sem_g, sem_v, sem_d, sem_o = refs[10:]
    edge = 16
    main = x_ref.shape[0] - edge
    units = d_ref.shape[1]
    shards = d_ref.shape[0]
    block = taps_ref.shape[2] // 2
    blocks = taps_ref.shape[0]

    def token_copy(i):
        size = toks_in[i].shape[0]
        start = pl.multiple_of(at_ref[i], 16)
        return pltpu.make_async_copy(toks_in[i], x_ref.at[pl.ds(start, size), :], sem_x.at[i])

    def rows_copy(b, base, ref, sem):
        start = pl.multiple_of(b * block, block)
        return pltpu.make_async_copy(
            all_ref.at[:, pl.ds(base + start, block), :], ref.at[:, pl.ds(start, block), :], sem.at[b]
        )

    def gate_copy(b):
        return rows_copy(b, 0, g_ref, sem_g)

    def value_copy(b):
        return rows_copy(b, units, v_ref, sem_v)

    down = pltpu.make_async_copy(all_ref.at[:, pl.ds(2 * units, units), :], d_ref, sem_d)
    for i in range(pieces):
        token_copy(i).start()
    gate_copy(0).start()
    value_copy(0).start()
    row = lax.broadcasted_iota(jnp.int32, (edge, x_ref.shape[1]), 0)
    halo = jnp.where(row == 0, first_ref[...].astype(F32), 0.0)
    halo = jnp.where(row == 1, last_ref[...].astype(F32), halo)
    x_ref[pl.ds(main, edge), :] = halo.astype(BF16)
    for i in range(pieces):
        token_copy(i).wait()

    def arrive(b):
        gate_copy(b).wait()
        value_copy(b).wait()

    def up(b, out_ref):
        rows = pl.ds(b * block, block)
        w = [
            jnp.concatenate([ref[s, rows, :] for s in range(shards)], axis=1) for ref in (g_ref, v_ref)
        ]
        w = jnp.concatenate(w, axis=0)
        y = lax.dot_general(x_ref[...], w, NT, preferred_element_type=F32)
        out_ref[...] = y.astype(BF16).astype(F32)

    def finish(b, in_ref):
        now = in_ref[pl.ds(0, main), :]
        row = lax.broadcasted_iota(jnp.int32, now.shape, 0)
        before = jnp.where(row == 0, in_ref[main : main + 1, :], pltpu.roll(now, 1, 0))
        after = jnp.where(row == main - 1, in_ref[main + 1 : main + 2, :], pltpu.roll(now, main - 1, 0))
        taps = taps_ref[b]
        mixed = taps[0:1] * before + taps[1:2] * now + taps[2:3] * after
        h_ref[:, pl.ds(b * block, block)] = (gelu(mixed[:, :block]) * mixed[:, block:]).astype(BF16)

    arrive(0)
    for b in range(1, blocks):
        gate_copy(b).start()
        value_copy(b).start()
    up(0, even_ref)

    def pair(i, unused):
        b = pl.multiple_of(2 * i, 2)
        arrive(b + 1)
        arrive(b + 2)
        up(b + 1, odd_ref)
        finish(b, even_ref)
        up(b + 2, even_ref)
        finish(b + 1, odd_ref)
        return unused

    lax.fori_loop(0, blocks // 2 - 1, pair, 0)
    arrive(blocks - 1)
    down.start()
    up(blocks - 1, odd_ref)
    finish(blocks - 2, even_ref)
    finish(blocks - 1, odd_ref)
    down.wait()

    wide = 512
    parts = x_ref.shape[1] // wide
    count, own = keep_ref.shape[0], keep_ref.shape[1]

    def out_copy(n, k, o):
        start = pl.multiple_of(at_ref[pieces + 2 * k + o], 16)
        cols = pl.ds(pl.multiple_of(n * wide, wide), wide)
        ref = (keep_ref, send_ref)[o]
        return pltpu.make_async_copy(
            p_ref.at[pl.ds(start, own), cols], ref.at[k, :, cols], sem_o.at[n, 2 * k + o]
        )

    def down_block(n, unused):
        w = jnp.concatenate([d_ref[4 * n + i] for i in range(4)], axis=1)
        y = jnp.dot(h_ref[:, :units], w, preferred_element_type=F32)
        p_ref[:, pl.ds(pl.multiple_of(n * wide, wide), wide)] = y.astype(BF16)
        for k in range(count):
            for o in range(2):
                out_copy(n, k, o).start()
        return unused

    lax.fori_loop(0, parts, down_block, 0)

    def out_wait(n, unused):
        for k in range(count):
            for o in range(2):
                out_copy(n, k, o).wait()
        return unused

    lax.fori_loop(0, parts, out_wait, 0)


def vmem(limit=56 << 20):
    return pltpu.CompilerParams(vmem_limit_bytes=limit)


def body(
    queries,
    keys,
    values,
    query_gain,
    key_gain,
    residual,
    out_weight,
    mix_gain,
    ffn_gain,
    gate_in,
    value_in,
    conv_gate,
    conv_value,
    down_t,
):
    tok = queries.shape[0]
    hd = query_gain.shape[0]
    n_sp, n_tp = lax.axis_size("sp"), lax.axis_size("tp")
    n_x = n_tp // 2
    group = HEADS // KVH
    splits = n_tp // KVH
    part = tok // splits
    own = tok // n_tp
    model = residual.shape[1]
    units = gate_in.shape[1]
    tp, sp = lax.axis_index("tp"), lax.axis_index("sp")
    kv_head, piece = tp // splits, tp % splits
    x, core = tp // 2, tp % 2

    def send(array, change):
        return lax.ppermute(array, "tp", [(i, change(i)) for i in range(n_tp)])

    def other_core(array):
        return send(array, lambda i: i ^ 1)

    def up_x(array):
        return send(array, lambda i: (i + 2) % n_tp)

    def down_x(array):
        return send(array, lambda i: (i - 2) % n_tp)

    def far_x(array):
        return send(array, lambda i: (i + n_x) % n_tp)

    def gathered(mine, direct=False):
        size = mine.shape[0]
        half = size // 2
        a = up_x(mine)
        b = down_x(mine)
        near = other_core(mine)
        if direct:
            pieces = [(mine, tp), (near, tp ^ 1)]
            far = far_x(mine)
            for array, shift in ((a, n_x - 1), (b, 1), (far, n_x // 2)):
                base = ((x + shift) % n_x) * 2
                across = other_core(array)
                pieces += [(array, base + core), (across, base + 1 - core)]
            return [p[0] for p in pieces], [p[1] * size for p in pieces]
        c = up_x(a[:half])
        d = down_x(b[half:])
        low, high = ((x + n_x - 1) % n_x) * 2, ((x + 1) % n_x) * 2
        far = (tp + n_x) % n_tp
        found = [(mine, tp * size), (near, (tp ^ 1) * size)]
        for array, base in ((a, low), (b, high)):
            across = other_core(array)
            found.append((array, (base + core) * size))
            found.append((across, (base + 1 - core) * size))
        both = jnp.concatenate([c, d], axis=0)
        found.append((both, far * size))
        found.append((other_core(both), (far ^ 1) * size))
        return [f[0] for f in found], [f[1] for f in found]

    row_np, col_np = rotary_parts(tok * n_sp, hd)
    row_np = row_np.reshape(n_sp, tok // GRID_W, 2 * hd)
    rows_all, cols_all = jnp.asarray(row_np), jnp.asarray(col_np)
    at = jnp.stack([piece, kv_head, sp, core, x]).astype(jnp.int32)
    packed_rows = 2 * part
    packed = pl.pallas_call(
        key_kernel,
        out_shape=jax.ShapeDtypeStruct((packed_rows, hd), BF16),
        grid_spec=pltpu.PrefetchScalarGridSpec(
            num_scalar_prefetch=1,
            grid=(1,),
            in_specs=[
                pl.BlockSpec((part, hd), lambda i, a: (a[0], a[1])),
                pl.BlockSpec((part, hd), lambda i, a: (a[0], a[1])),
                pl.BlockSpec((1, hd), lambda i, a: (0, 0)),
                pl.BlockSpec((1,) + row_np.shape[1:], lambda i, a: (a[2], 0, 0)),
                pl.BlockSpec(col_np.shape, lambda i, a: (0, 0)),
            ],
            out_specs=pl.BlockSpec((packed_rows, hd), lambda i, a: (0, 0)),
        ),
        name="key_prep",
    )(at, keys, values, key_gain[None], rows_all, cols_all)
    weights = jnp.concatenate([gate_in.T, value_in.T, down_t.T], axis=0)
    gate_rows = lax.all_gather(weights, "sp", axis=0, tiled=False)

    mine = pl.pallas_call(
        query_kernel,
        out_shape=jax.ShapeDtypeStruct((tok, hd), BF16),
        grid_spec=pltpu.PrefetchScalarGridSpec(
            num_scalar_prefetch=1,
            grid=(1,),
            in_specs=[
                pl.BlockSpec((tok, hd), lambda i, a: (0, 0)),
                pl.BlockSpec((1, hd), lambda i, a: (0, 0)),
                pl.BlockSpec((1,) + row_np.shape[1:], lambda i, a: (a[2], 0, 0)),
                pl.BlockSpec(col_np.shape, lambda i, a: (0, 0)),
            ],
            out_specs=pl.BlockSpec((tok, hd), lambda i, a: (0, 0)),
        ),
        name="query_prep",
    )(at, queries, query_gain[None], rows_all, cols_all)
    turned_q = [mine] + [send(mine, lambda i, k=k: i ^ k) for k in range(1, group)]
    rows = group * own

    out_pieces, out_at = gathered(out_weight, direct=True)

    packed, queries, out_weight = lax.optimization_barrier((packed, queries, out_weight))
    right = [(i, (i + 1) % n_sp) for i in range(n_sp)]
    left = [(i, (i - 1) % n_sp) for i in range(n_sp)]
    tail = 32
    anywhere = pl.BlockSpec(memory_space=pl.ANY)

    def attend(here, base, steps, before):
        last = before is not None
        if last:
            shape = (n_x, rows + tail, hd)
            out_shape = [jax.ShapeDtypeStruct(shape, BF16)] * 2
            out_specs = [pl.BlockSpec((1,) + shape[1:], lambda i, a: (lax.rem(i + n_x - a[4], n_x), 0, 0))] * 2
        else:
            shape = (steps, 2, 2 * rows, hd)
            out_shape = jax.ShapeDtypeStruct(shape, F32)
            out_specs = pl.BlockSpec((1,) + shape[1:], lambda i, a: (i, 0, 0, 0))
        in_specs = [anywhere] * group + [pl.BlockSpec((2 * part, hd), lambda i, a: (0, 0))] * len(here)
        if last:
            kept = (1, 2, 2 * rows, hd)
            in_specs.append(pl.BlockSpec(kept, lambda i, a: (lax.min(i, n_x // 2 - 1), 0, 0, 0)))
            in_specs.append(pl.BlockSpec(kept, lambda i, a: (lax.max(i - n_x // 2, 0), 0, 0, 0)))
        share = group * tok * part * len(here) * steps // n_x
        return pl.pallas_call(
            functools.partial(attend_kernel, len(here), group, own, base, last),
            out_shape=out_shape,
            grid_spec=pltpu.PrefetchScalarGridSpec(
                num_scalar_prefetch=1,
                grid=(steps,),
                in_specs=in_specs,
                out_specs=out_specs,
                scratch_shapes=[pltpu.VMEM((group, tok, hd), BF16), pltpu.SemaphoreType.DMA((group,))],
            ),
            compiler_params=vmem(36 << 20),
            cost_estimate=pl.CostEstimate(
                flops=8 * share * hd, bytes_accessed=8 << 20, transcendentals=share
            ),
        )(at, *turned_q, *here, *(before or ()))

    shards = [packed]
    a = b = packed
    kept = []
    for s in range(1, n_sp // 2 + 1):
        a = lax.ppermute(a, "sp", right)
        shards.append(a)
        if len(shards) < n_sp:
            b = lax.ppermute(b, "sp", left)
            shards.append(b)
        if s == n_sp // 4:
            a, b, *turned_q = lax.optimization_barrier((a, b, *turned_q))
        if s in (n_sp // 4, n_sp // 4 + 1):
            kept.append(attend(shards[: n_sp // 2], len(kept) * (n_x // 2), n_x // 2, None))
        if s in (n_sp // 4 + 1, n_sp // 4 + 2):
            a, b, kept[s - n_sp // 4 - 1] = lax.optimization_barrier((a, b, kept[s - n_sp // 4 - 1]))
    keep, away = attend(shards[n_sp // 2 : -1] + [a], 0, n_x, kept)
    merged = pl.pallas_call(
        functools.partial(merge_kernel, rows),
        out_shape=[jax.ShapeDtypeStruct((rows + tail, hd), BF16)] * n_x,
        compiler_params=vmem(16 << 20),
        name="merge",
    )(keep, other_core(away))
    one = up_x(merged[1])
    two = far_x(merged[2])
    three = down_x(merged[3])
    seen = [merged[0], one, two, three]
    seen_at = [(x + n_x - k) % n_x for k in range(n_x)]
    whole = pl.BlockSpec(memory_space=pltpu.VMEM)
    stream, normed = pl.pallas_call(
        functools.partial(mix_kernel, group, n_x, len(out_pieces)),
        out_shape=[jax.ShapeDtypeStruct((own, model), BF16)] * 2,
        in_specs=[pl.BlockSpec(memory_space=pltpu.SMEM)] + [whole] * 3 + [anywhere] * (n_x + len(out_pieces)),
        scratch_shapes=[
            pltpu.VMEM((n_x, rows + tail, hd), BF16),
            pltpu.VMEM((own, HEADS * hd), BF16),
            pltpu.VMEM((HEADS * hd, model), BF16),
            pltpu.SemaphoreType.DMA((n_x,)),
            pltpu.SemaphoreType.DMA((len(out_pieces),)),
        ],
        compiler_params=vmem(),
        cost_estimate=pl.CostEstimate(
            flops=2 * own * HEADS * hd * model, bytes_accessed=6 << 20, transcendentals=0
        ),
        name="mix",
    )(
        jnp.stack(out_at + seen_at).astype(jnp.int32),
        residual,
        mix_gain[None],
        ffn_gain[None],
        *seen,
        *out_pieces,
    )

    token_pieces, token_at = gathered(normed)
    first = last_row = None
    for p, r in zip(token_pieces, token_at):
        f = jnp.where(r == 0, p[:1], 0)
        e = jnp.where(r + p.shape[0] == tok, p[-1:], 0)
        first = f if first is None else first + f
        last_row = e if last_row is None else last_row + e
    before = lax.ppermute(last_row, "sp", [(i, i + 1) for i in range(n_sp - 1)])
    after = lax.ppermute(first, "sp", [(i + 1, i) for i in range(n_sp - 1)])
    block = 128
    blocks = -(-units // block)

    def by_block(taps):
        wide = jnp.pad(taps, ((0, 5), (0, blocks * block - units)))
        return jnp.transpose(wide.reshape(8, blocks, block), (1, 0, 2))

    taps = jnp.concatenate([by_block(conv_gate), by_block(conv_value)], axis=2)
    slots = []
    for k in range(n_x):
        to = ((x + k) % n_x) * 2
        slots += [(to + core) * own, (to + 1 - core) * own]
    where = jnp.stack(token_at + slots).astype(jnp.int32)
    keep, away = pl.pallas_call(
        functools.partial(ffn_kernel, len(token_pieces)),
        out_shape=[jax.ShapeDtypeStruct((n_x, own, model), BF16)] * 2,
        in_specs=[pl.BlockSpec(memory_space=pltpu.SMEM)]
        + [whole] * 3
        + [anywhere] * (1 + len(token_pieces)),
        out_specs=[anywhere, anywhere],
        scratch_shapes=[
            pltpu.VMEM((tok + 16, model), BF16),
            pltpu.VMEM((n_sp, blocks * block, hd), BF16),
            pltpu.VMEM((n_sp, blocks * block, hd), BF16),
            pltpu.VMEM((n_sp, units, hd), BF16),
            pltpu.VMEM((tok + 16, 2 * block), F32),
            pltpu.VMEM((tok + 16, 2 * block), F32),
            pltpu.VMEM((tok, blocks * block), BF16),
            pltpu.VMEM((tok, model), BF16),
            pltpu.SemaphoreType.DMA((len(token_pieces),)),
            pltpu.SemaphoreType.DMA((blocks,)),
            pltpu.SemaphoreType.DMA((blocks,)),
            pltpu.SemaphoreType.DMA,
            pltpu.SemaphoreType.DMA((model // 512, 2 * n_x)),
        ],
        compiler_params=vmem(56 << 20),
        cost_estimate=pl.CostEstimate(
            flops=6 * tok * units * model, bytes_accessed=16 << 20, transcendentals=tok * units
        ),
        name="ffn",
    )(where, before, after, taps, gate_rows, *token_pieces)
    near = other_core(away)
    total = [keep[k].astype(F32) + near[k].astype(F32) for k in range(n_x)]
    half = own // 2
    low = up_x(total[2][:half].astype(BF16))
    high = down_x(total[2][half:].astype(BF16))
    direct_high = up_x(total[1][half:].astype(BF16))
    direct_low = down_x(total[3][:half].astype(BF16))
    low = up_x((total[1][:half] + low.astype(F32)).astype(BF16))
    high = down_x((total[3][half:] + high.astype(F32)).astype(BF16))
    ones = jnp.concatenate([low, high], axis=0).astype(F32)
    twos = jnp.concatenate([direct_low, direct_high], axis=0).astype(F32)
    return (stream.astype(F32) + total[0] + ones + twos).astype(BF16)


def solution(mesh):
    return jax.shard_map(
        body,
        mesh=mesh,
        in_specs=(
            P(("grp", "sp"), "tp"),
            P(("grp", "sp"), None),
            P(("grp", "sp"), None),
            P(),
            P(),
            P(("grp", "sp", "tp"), None),
            P("tp", None),
            P(),
            P(),
            P("sp", "tp"),
            P("sp", "tp"),
            P(None, "tp"),
            P(None, "tp"),
            P("sp", "tp"),
        ),
        out_specs=P(("grp", "sp", "tp"), None),
        check_vma=False,
    )
```
